512 devices in a mesh: tp: 64 (over z, y), dp: 8 (over x, core).
Axes of the slice: x: 4, y: 8, z: 8, core: 2. Of those that a mesh axis runs over, the one named last changes fastest.
Arguments:
- tokens: bfloat16 [256, 4096], P(None, 'dp'), may hold values from -6 to 6
- lengths: int32 [256], P('dp'), may hold values from 1 to 4096, 262144 in all
- norm_gain: float32 [2, 4096], P(None, 'dp'), may hold values from 0.1 to 1.9
- w_in: bfloat16 [2, 4096, 2048], P(None, 'dp', 'tp'), may hold values from -0.09375 to 0.09375
- log_step: float32 [2, 128], P(None, 'tp'), may hold values from -4.6 to -0.7
- eig_re: float32 [2, 128, 64], P(None, 'tp'), may hold values from -2 to -0.05
- eig_im: float32 [2, 128, 64], P(None, 'tp'), may hold values from 0 to 8
- in_mat: float32 [2, 2, 128, 64, 16], P(None, None, 'tp'), may hold values from -2.5 to 2.5
- output_matrices: float32 [2, 2, 128, 16, 64], P(None, None, 'tp'), may hold values from -1.25 to 1.25
- skip: float32 [2, 2048], P(None, 'tp'), may hold values from -4 to 4
- w_glu: bfloat16 [2, 2048, 4096], P(None, 'tp', 'dp'), may hold values from -0.75 to 0.75
- w_gate: bfloat16 [2, 2048, 4096], P(None, 'tp', 'dp'), may hold values from -0.125 to 0.125
- state: float32 [2, 2, 256, 8192], P(None, None, 'dp', 'tp'), may hold values from -6 to 6
Outputs:
- mixed: bfloat16 [256, 4096], P(None, 'dp')
- new_state: float32 [2, 2, 256, 8192], P(None, None, 'dp', 'tp')
The draws below stay inside these ranges and needn't reach their ends.
Inputs may be any that keep to these rules, and one draw needn't show every extreme that they name: `lengths`: each sequence's number of past positions; the largest is exactly 4096 and all add up to 262144.
All inputs are finite; a program needn't handle non-finite values.
Results may differ from the reference program's by a relative error of at most 0.0095.
Values may be sent and summed in bfloat16 or wider, within the bound.
A program may use at most 64 MiB of HBM per device.

```python
import math
import jax
import jax.numpy as jnp
import numpy as np
from jax import lax

D = 4096
GROUPS = 128
GROUP = 16
STATES = 64
S5W = 2048
LAYERS = 2
BATCH = 256
LEN_MAX = 4096
LEN_MEAN = 1024
BLOCK_LEN = 256


def spiked(array, stream_key, source, target, shards_of, factor):
    owner, partner = [(jnp.arange(array.shape[dim]) // (array.shape[dim] // shards_of)).reshape([-1 if axis == dim else 1 for axis in range(array.ndim)]) for dim in (source, target)]
    chosen = jax.random.permutation(stream_key, shards_of)[partner]
    strong = (owner == chosen) | (owner == (partner + shards_of // 2) % shards_of)
    return jnp.where(strong, factor * array, array)


def block_levels(own_key, dims, pieces, low, top_value):
    def one(position, shards_of):
        draws = jax.random.uniform(jax.random.fold_in(jax.random.fold_in(own_key, 6), position), (shards_of,), jnp.float32, low / len(pieces), top_value / len(pieces))
        return jnp.repeat(jnp.exp(draws), dims[position] // shards_of).reshape((-1,) + (1,) * (len(dims) - position - 1))

    level = one(*pieces[0])
    for cut in pieces[1:]:
        level = level * one(*cut)
    return level


def profile(number_of, total, reach, lean):
    loads = [(1 << 20) // math.isqrt(grade ** lean) + 1 for grade in range(2, number_of + 1)]
    rest, holding = total - reach - (number_of - 1), [1] * (number_of - 1)
    while rest > 0:
        candidates = [i for i in range(number_of - 1) if holding[i] < reach]
        mass, remaining = sum([loads[i] for i in candidates]), rest
        for i in candidates:
            extra = min(reach - holding[i], max(1, remaining * loads[i] // mass), rest)
            holding[i] = holding[i] + extra
            rest = rest - extra
    return np.array([reach] + holding)


def ragged(rng, amount, total, reach, skew):
    if amount == 2:
        one = jax.random.randint(rng, (), max(1, total - reach), min(reach, total - 1) + 1)
        return jnp.stack([one, total - one])
    sizes = jnp.asarray(profile(amount, total, reach, skew), jnp.int32)
    couples = (amount - 1) // 2
    giver, sink = sizes[1:1 + 2 * couples:2], sizes[2:2 + 2 * couples:2]
    slack = jnp.minimum(giver - 1, reach - sink)
    moved = jax.random.randint(jax.random.fold_in(rng, 1), (couples,), 0, 1 << 20) % (slack + 1)
    sizes = sizes.at[1:1 + 2 * couples:2].set(giver - moved).at[2:2 + 2 * couples:2].set(sink + moved)
    return sizes[jax.random.permutation(jax.random.fold_in(rng, 2), amount)]


def scatter_about(rng, extent, spread, limit, split=(), kind=jnp.bfloat16):
    result = spread * jax.random.normal(rng, extent, jnp.float32)
    if split:
        result = result * block_levels(rng, extent, split, -0.22, 0.18)
    return jnp.clip(result, -limit, limit).astype(kind)


def noise_with(key, dims, deviation, most, pieces, heavy, kind=jnp.bfloat16):
    entries = deviation * jax.random.normal(key, dims, jnp.float32)
    if pieces:
        entries = entries * block_levels(key, dims, pieces, -0.22, 0.18)
    return jnp.clip(spiked(entries, jax.random.fold_in(key, 3), *heavy), -most, most).astype(kind)


def setup_inputs(seed: int = 0) -> dict:
    arg_keys = jax.random.split(jax.random.key(seed), 14)
    return {
        "tokens": scatter_about(arg_keys[0], (BATCH, D), 1.0, 6.0, ((1, 8),)),
        "lengths": ragged(arg_keys[1], BATCH, BATCH * LEN_MEAN, LEN_MAX, 2).astype(jnp.int32),
        "norm_gain": jnp.clip(1.0 + 0.18 * jax.random.normal(arg_keys[2], (LAYERS, D), jnp.float32), 0.1, 1.9),
        "w_in": scatter_about(arg_keys[3], (LAYERS, D, S5W), D ** -0.5, 0.09375, ((1, 8), (2, 64))),
        "log_step": jnp.clip(-4.6 + 3.8999999 * jax.random.uniform(arg_keys[4], (LAYERS, GROUPS), jnp.float32) ** block_levels(arg_keys[4], (LAYERS, GROUPS), ((1, 64),), -0.2, 0.2), -4.6, -0.7),
        "eig_re": jnp.clip(-2.0 + 1.95 * jax.random.uniform(arg_keys[5], (LAYERS, GROUPS, STATES), jnp.float32) ** block_levels(arg_keys[5], (LAYERS, GROUPS, STATES), ((1, 64),), -0.2, 0.2), -2.0, -0.05),
        "eig_im": jnp.clip(8.0 * jax.random.uniform(arg_keys[6], (LAYERS, GROUPS, STATES), jnp.float32) ** block_levels(arg_keys[6], (LAYERS, GROUPS, STATES), ((1, 64),), -0.2, 0.2), 0.0, 8.0),
        "in_mat": scatter_about(arg_keys[7], (LAYERS, 2, GROUPS, STATES, GROUP), 0.177, 2.5, ((2, 64),), jnp.float32),
        "output_matrices": scatter_about(arg_keys[8], (LAYERS, 2, GROUPS, GROUP, STATES), 0.088, 1.25, ((2, 64),), jnp.float32),
        "skip": scatter_about(arg_keys[9], (LAYERS, S5W), 1.0, 4.0, ((1, 64),), jnp.float32),
        "w_glu": noise_with(arg_keys[10], (LAYERS, S5W, D), (S5W // 4) ** -0.5, 0.75, ((1, 64), (2, 8)), (1, 2, 64, 4.0)),
        "w_gate": scatter_about(arg_keys[11], (LAYERS, S5W, D), S5W ** -0.5, 0.125, ((1, 64), (2, 8))),
        "state": scatter_about(arg_keys[12], (LAYERS, 2, BATCH, GROUPS * STATES), 0.5, 6.0, ((2, 8), (3, 64)), jnp.float32),
    }


NORM_EPS = 1e-06
FULL_PRECISION = lax.Precision.HIGHEST

def position_factor(lengths):
    blocks = (lengths // BLOCK_LEN).astype(jnp.float32)
    return 2.0 / (1.0 + blocks * (4.0 * BLOCK_LEN / LEN_MAX))

def recurrent_step(driven_state, state_pair, factor, log_step, eig_re, eig_im, in_mat, output_matrices, skip):
    step_size = jnp.exp(log_step)[None, :, None] * factor[:, None, None]
    magnitude = jnp.exp(eig_re[None] * step_size)
    turned = eig_im[None] * step_size
    decay_re = magnitude * jnp.cos(turned)
    decay_im = magnitude * jnp.sin(turned)
    modulus = eig_re * eig_re + eig_im * eig_im
    weight_re = ((decay_re - 1.0) * eig_re + decay_im * eig_im) / modulus
    weight_im = (decay_im * eig_re - (decay_re - 1.0) * eig_im) / modulus
    drive_re = jnp.einsum('bgc,gpc->bgp', driven_state, in_mat[0], precision=FULL_PRECISION)
    drive_im = jnp.einsum('bgc,gpc->bgp', driven_state, in_mat[1], precision=FULL_PRECISION)
    state_real = decay_re * state_pair[0] - decay_im * state_pair[1] + weight_re * drive_re - weight_im * drive_im
    state_imaginary = decay_re * state_pair[1] + decay_im * state_pair[0] + weight_re * drive_im + weight_im * drive_re
    readout_value = jnp.einsum('szv,zuv->szu', state_real, output_matrices[0], precision=FULL_PRECISION) - jnp.einsum('szv,zuv->szu', state_imaginary, output_matrices[1], precision=FULL_PRECISION) + skip * driven_state
    return (jax.nn.gelu(readout_value), state_real, state_imaginary)

def reference(tokens, lengths, norm_gain, w_in, log_step, eig_re, eig_im, in_mat, output_matrices, skip, w_glu, w_gate, state):
    factor = position_factor(lengths)
    current = tokens.astype(jnp.float32)
    rounded = tokens
    new_states = []
    for layer_index in range(LAYERS):
        squares = lax.optimization_barrier(jnp.sum(current * current, axis=1))
        scaled = (current * norm_gain[layer_index]).astype(jnp.bfloat16)
        partial_value = jnp.dot(scaled, w_in[layer_index], preferred_element_type=jnp.float32)
        driven_state = (partial_value * lax.rsqrt(squares / D + NORM_EPS)[:, None]).astype(jnp.bfloat16)
        driven_state = driven_state.astype(jnp.float32).reshape(BATCH, GROUPS, GROUP)
        state_pair = state[layer_index].reshape(2, BATCH, GROUPS, STATES)
        readout_value, state_real, state_imaginary = recurrent_step(driven_state, state_pair, factor, log_step[layer_index], eig_re[layer_index], eig_im[layer_index], in_mat[layer_index], output_matrices[layer_index], skip[layer_index].reshape(GROUPS, GROUP))
        readout_value = readout_value.reshape(BATCH, GROUPS * GROUP).astype(jnp.bfloat16)
        new_states.append(jnp.stack([state_real, state_imaginary]).reshape(2, BATCH, GROUPS * STATES))
        linear = jnp.dot(readout_value, w_glu[layer_index], preferred_element_type=jnp.float32)
        gate_sum = jnp.dot(readout_value, w_gate[layer_index], preferred_element_type=jnp.float32)
        rounded = (current + linear * jax.nn.sigmoid(gate_sum)).astype(jnp.bfloat16)
        current = rounded.astype(jnp.float32)
    return (rounded, jnp.stack(new_states))
```

```python
import jax
import jax.numpy as jnp
from jax import lax
from jax.experimental import pallas as pl
from jax.experimental.pallas import tpu as pltpu
from jax.sharding import PartitionSpec as P

D = 4096
LEN_MAX = 4096
BLOCK_LEN = 256
NORM_EPS = 1e-06
MESH = pl.DeviceIdType.MESH
F32 = jnp.float32
BF16 = jnp.bfloat16

(PH1, ST1A, RES0, PH2, ST1B, ST1W, PH3, PH4, RES1, PH5, PH6, PH7, PH8, PH9A, PH9B, GAIN) = range(16)
NEAR = 16
PAIR = NEAR + 9
COUNT = PAIR + 12


def roll(x, amount):
    amount = amount % 128
    return x if amount == 0 else pltpu.roll(x, amount, 1)


def groups4(rows):
    return lax.broadcasted_iota(jnp.int32, (rows, 128), 1) // 32


def low_half(rows):
    return lax.broadcasted_iota(jnp.int32, (rows, 128), 1) < 64


def pick4(parts, group):
    out = parts[3]
    for i in (2, 1, 0):
        out = jnp.where(group == i, parts[i], out)
    return out


def split2(x):
    hi = x.astype(BF16)
    lo = (x - hi.astype(F32)).astype(BF16)
    return hi, lo


def kernel(
    tok_h, len_h, gain_h, win_h, ls_h, er_h, ei_h, im_h, om_h, skip_h, glu_h, gate_h, st_h,
    mixed_ref, ns_ref,
    tok, lens, gain, win, ls, er, ei, im, om, skip, glu, gate, st,
    s1, r1, ws, w, wis, pk, wi, gb, rz, rz1, s2, r2, s3, r3, r4, m0, s5, r5, s7, r7, oa, ob,
    lsem, ss, rs,
):
    tp = lax.axis_index("tp")
    d = lax.axis_index("dp")
    z = tp // 8
    y = lax.rem(tp, 8)
    x = d // 2
    core = lax.rem(d, 2)

    def at_y(k):
        return {"tp": z * 8 + lax.rem(y + k, 8), "dp": d}

    def at_z(k):
        return {"tp": lax.rem(z + k, 8) * 8 + y, "dp": d}

    def at_d(k):
        return {"tp": tp, "dp": lax.rem(d + k, 8)}

    def send(src, dst, sem, dev, rsem=None):
        pltpu.make_async_remote_copy(
            src_ref=src,
            dst_ref=dst,
            send_sem=ss.at[sem],
            recv_sem=rs.at[sem if rsem is None else rsem],
            device_id=dev,
            device_id_type=MESH,
        ).start()

    def wait_recv(ref, sem):
        pltpu.make_async_copy(ref, ref, rs.at[sem]).wait()

    def wait_sent(ref, sem):
        pltpu.make_async_copy(ref, ref, ss.at[sem]).wait()

    hbm = (tok_h, win_h, gain_h, glu_h, gate_h, len_h, ls_h, er_h, ei_h, im_h, om_h, skip_h, st_h)
    vmem = (tok, win, gain, glu, gate, lens, ls, er, ei, im, om, skip, st)
    loads = [pltpu.make_async_copy(a, b, lsem.at[i]) for i, (a, b) in enumerate(zip(hbm, vmem))]
    for copy in loads:
        copy.start()

    barrier = pltpu.get_barrier_semaphore()
    for k in range(1, 8):
        for dev in (at_d(k), at_y(k), at_z(k)):
            pl.semaphore_signal(barrier, inc=1, device_id=dev, device_id_type=MESH)
    for k in range(8):
        @pl.when(jnp.logical_not(jnp.logical_and(z == k, d == z)))
        def _(k=k):
            pl.semaphore_signal(
                barrier, inc=1, device_id={"tp": k * 8 + y, "dp": z}, device_id_type=MESH
            )

    group8 = groups4(8)
    low16 = low_half(16)
    low32 = low_half(32)

    for i in range(3):
        loads[i].wait()
    for dd in range(8):
        t = tok[32 * dd : 32 * dd + 32, :].astype(F32)
        scaled = (t * gain[0:1, :]).astype(BF16)
        part = jnp.dot(scaled, win[0], preferred_element_type=F32)
        sq = jnp.sum(t * t, axis=1, keepdims=True)
        s1[dd, 0:8, :] = jnp.concatenate([part[8 * i : 8 * i + 8, :] for i in range(4)], axis=1)
        s1[dd, 8:16, :] = pick4(
            [jnp.broadcast_to(sq[8 * i : 8 * i + 8, :], (8, 128)) for i in range(4)], group8
        )
    r1[pl.ds(d, 1)] = s1[pl.ds(d, 1)]

    loads[3].wait()
    loads[4].wait()

    def pack_projection(layer):
        for q in range(4):
            g = glu[layer, :, 128 * q : 128 * q + 128].astype(F32)
            t = gate[layer, :, 128 * q : 128 * q + 128].astype(F32)
            ws[layer, 2 * q] = jnp.where(low32, g, roll(t, 64)).astype(BF16)
            ws[layer, 2 * q + 1] = jnp.where(low32, roll(g, 64), t).astype(BF16)
        w[layer, pl.ds(d, 1), pl.ds(y, 1)] = ws[layer, pl.ds(y, 1)][None]

    pack_projection(0)

    half = lax.rem(y, 2)
    column = pl.ds(pl.multiple_of((y // 2) * 128, 128), 128)
    for dd in range(8):
        t = tok[32 * dd : 32 * dd + 32, column].astype(F32)
        t = jnp.where(half == 1, roll(t, 64), t)
        rz[dd] = jnp.where(low16, t[0:16], roll(t[16:32], 64)).astype(BF16)

    @pl.when(d == z)
    def _():
        rz[8] = rz[pl.ds(d, 1)][0]

    pl.semaphore_wait(barrier, 29 - jnp.where(d == z, 1, 0))

    for k in range(1, 8):
        to = lax.rem(d + k, 8)
        send(s1.at[to], r1.at[d], PH1, at_d(k))
    for k in range(1, 8):
        to = lax.rem(y + k, 8)
        send(ws.at[0, to], w.at[0, d, y], ST1A, at_y(k))

    @pl.when(d == z)
    def _():
        for k in range(1, 8):
            send(rz.at[lax.rem(d + k, 8)], rz.at[8], RES0, at_d(k))

    for i in range(5, 13):
        loads[i].wait()
    eye = lax.broadcasted_iota(jnp.int32, (32, 32), 0) == lax.broadcasted_iota(jnp.int32, (32, 32), 1)
    blocks = (lens[...] // BLOCK_LEN).astype(F32)
    blocks = jnp.sum(jnp.where(eye, jnp.broadcast_to(blocks, (32, 32)), 0.0), axis=1, keepdims=True)
    factor = 2.0 / (1.0 + blocks * (4.0 * BLOCK_LEN / LEN_MAX))

    def constants(layer):
        def row(ref):
            return jnp.concatenate([ref[layer, 0:1, :], ref[layer, 1:2, :]], axis=1)

        e_re, e_im = row(er), row(ei)
        rate = jnp.exp(ls[layer : layer + 1, :])
        rate = jnp.concatenate(
            [jnp.broadcast_to(rate[:, 0:1], (1, 64)), jnp.broadcast_to(rate[:, 1:2], (1, 64))], axis=1
        )
        step = rate * factor
        magnitude = jnp.exp(e_re * step)
        turned = e_im * step
        a_re = magnitude * jnp.cos(turned)
        a_im = magnitude * jnp.sin(turned)
        modulus = e_re * e_re + e_im * e_im
        b_re = ((a_re - 1.0) * e_re + a_im * e_im) / modulus
        b_im = (a_im * e_re - (a_re - 1.0) * e_im) / modulus
        u, v = st[layer, 0], st[layer, 1]
        k_re = a_re * u - a_im * v
        k_im = a_re * v + a_im * u
        rows = []
        for c in range(2):
            for g in range(2):
                slab = im[layer, c, g]
                zero = jnp.zeros((64, 16), F32)
                one = jnp.concatenate([slab, zero] if g == 0 else [zero, slab], axis=1)
                rows.append(jnp.concatenate([one] * 4, axis=1))
        hi, lo = split2(jnp.concatenate(rows, axis=0))
        in_cat = jnp.concatenate([hi, lo], axis=1)
        cols = []
        for c in range(2):
            zero = jnp.zeros((16, 64), F32)
            top = jnp.concatenate([om[layer, c, 0], zero], axis=1)
            low = jnp.concatenate([zero, om[layer, c, 1]], axis=1)
            both = jnp.concatenate([top, low], axis=0)
            cols.append(both if c == 0 else -both)
        both = jnp.concatenate(cols, axis=1)
        hi, lo = split2(jnp.concatenate([both] * 4, axis=0))
        out_cat = jnp.concatenate([hi, lo, hi], axis=1)
        direct = jnp.concatenate([skip[layer : layer + 1, :]] * 4, axis=1)
        return k_re, k_im, b_re, b_im, in_cat, out_cat, direct

    def recurrence(layer, consts, total):
        k_re, k_im, b_re, b_im, in_cat, out_cat, direct = consts
        driven = (total[0:8] * lax.rsqrt(total[8:16] / D + NORM_EPS)).astype(BF16).astype(F32)
        spread = jnp.concatenate([jnp.where(group8 == i, driven, 0.0) for i in range(4)], axis=0)
        spread = spread.astype(BF16)
        drive = lax.dot_general(
            jnp.concatenate([spread, spread], axis=1), in_cat, (((1,), (1,)), ((), ())),
            preferred_element_type=F32,
        )
        d_re, d_im = drive[:, 0:128], drive[:, 128:256]
        n_re = k_re + b_re * d_re - b_im * d_im
        n_im = k_im + b_re * d_im + b_im * d_re
        ns_ref[layer, 0] = n_re
        ns_ref[layer, 1] = n_im
        hi, lo = split2(jnp.concatenate([n_re, n_im], axis=1))
        full = lax.dot_general(
            jnp.concatenate([hi, hi, lo], axis=1), out_cat, (((1,), (1,)), ((), ())),
            preferred_element_type=F32,
        )
        value = pick4([full[8 * i : 8 * i + 8] for i in range(4)], group8) + direct * driven
        inner = 0.7978845608028654 * (value + 0.044715 * (value * value * value))
        return (value * (0.5 * (1.0 + jnp.tanh(inner)))).astype(BF16).astype(F32)

    def gather_readout(layer, value, sem):
        s2[layer] = value
        r2[layer, pl.ds(y, 1)] = value[None]
        for k in range(1, 8):
            send(s2.at[layer], r2.at[layer, y], sem, at_y(k))

    def unpack_readout(layer):
        tiles = []
        for i in range(4):
            tiles.append(
                jnp.concatenate(
                    [
                        pick4([roll(r2[layer, 4 * q + j], 32 * (j - i)) for j in range(4)], group8)
                        for q in range(2)
                    ],
                    axis=1,
                )
            )
        return jnp.concatenate(tiles, axis=0).astype(BF16)

    def near(kind, ref_of):
        mine = ref_of(d)
        for r in range(1, 4):
            to = lax.rem(x + r, 4) * 2 + core
            send(mine, mine, NEAR + 3 * kind + r - 1, {"tp": tp, "dp": to})
        send(mine, mine, PAIR + 4 * kind, {"tp": tp, "dp": x * 2 + 1 - core})

    def relay(kind, ref_of):
        for r in range(1, 4):
            ref = ref_of(lax.rem(x + 4 - r, 4) * 2 + core)
            wait_recv(ref, NEAR + 3 * kind + r - 1)
            send(ref, ref, PAIR + 4 * kind + r, {"tp": tp, "dp": x * 2 + 1 - core})

    def wait_pair(kind, ref_of):
        for r in range(4):
            wait_recv(ref_of(lax.rem(x + 4 - r, 4) * 2 + 1 - core), PAIR + 4 * kind + r)

    def near_sent(kind, ref):
        for r in range(3):
            wait_sent(ref, NEAR + 3 * kind + r)
        for r in range(4):
            wait_sent(ref, PAIR + 4 * kind + r)

    def w0(k):
        return w.at[0, k]

    def w1(k):
        return w.at[1, k]

    def wi_of(k):
        return wi.at[k]

    consts0 = constants(0)

    wait_recv(r1.at[pl.ds(0, 7)], PH1)
    value = recurrence(0, consts0, jnp.sum(r1[...], axis=0))
    gather_readout(0, value, PH2)

    wait_recv(w.at[0, 0, pl.ds(0, 7)], ST1A)
    near(0, w0)

    pack_projection(1)
    for dest in range(8):
        rows = win[1, 64 * dest : 64 * dest + 64, :].astype(F32)
        wis[dest] = jnp.concatenate([rows[16 * j : 16 * j + 16, :] for j in range(4)], axis=1).astype(BF16)
    pk[pl.ds(y, 1)] = wis[pl.ds(y, 1)]
    for k in range(1, 8):
        to = lax.rem(y + k, 8)
        send(wis.at[to], pk.at[y], ST1W, at_y(k))
    for k in range(1, 8):
        to = lax.rem(y + k, 8)
        send(ws.at[1, to], w.at[1, d, y], ST1B, at_y(k))
    own_gain = gain[1:2, column]
    gb[pl.ds(d, 1)] = jnp.where(half == 1, roll(own_gain, 64), own_gain)[None]
    for k in range(1, 8):
        send(gb.at[d], gb.at[d], GAIN, at_d(k))

    wait_recv(r2.at[0, pl.ds(0, 7)], PH2)
    piece = unpack_readout(0)
    relay(0, w0)
    wait_pair(0, w0)
    for k in range(8):
        s3[k] = jnp.dot(
            piece, w[0, k].reshape(256, 128), preferred_element_type=F32
        ).astype(BF16)
    for k in range(1, 8):
        send(s3.at[lax.rem(z + k, 8)], r3.at[z], PH3, at_z(k))
    r3[pl.ds(z, 1)] = s3[pl.ds(z, 1)]

    wait_recv(pk.at[pl.ds(0, 7)], ST1W)
    group16 = groups4(16)
    for j in range(4):
        cols = []
        for q in range(2):
            cols.append(
                pick4([roll(pk[4 * q + g].astype(F32), 32 * (g - j)) for g in range(4)], group16)
            )
        wi[pl.ds(d, 1), 16 * j : 16 * j + 16, :] = jnp.concatenate(cols, axis=1).astype(BF16)[None]
    near(2, wi_of)
    wait_recv(w.at[1, 0, pl.ds(0, 7)], ST1B)
    near(1, w1)

    @pl.when(d != z)
    def _():
        wait_recv(rz.at[8], RES0)

    def gated(parts, residual):
        top, low = parts[0:16], parts[16:32]
        linear = jnp.where(low16, top, roll(low, 64))
        gate_sum = jnp.where(low16, roll(top, 64), low)
        return (residual + linear * (1.0 / (1.0 + jnp.exp(-gate_sum)))).astype(BF16)

    residual0 = rz[8].astype(F32)
    wait_recv(r3.at[pl.ds(0, 7)], PH3)
    own = gated(jnp.sum(r3[...].astype(F32), axis=0), residual0)
    m0[...] = own
    r4[pl.ds(z, 1)] = own[None]
    for k in range(1, 8):
        send(m0, r4.at[z], PH4, at_z(k))

    @pl.when(d != z)
    def _():
        send(m0, rz1, RES1, {"tp": d * 8 + y, "dp": z})

    @pl.when(d == z)
    def _():
        rz1[...] = own

    relay(2, wi_of)
    relay(1, w1)
    consts1 = constants(1)
    wait_recv(gb.at[pl.ds(0, 7)], GAIN)
    low1 = low_half(1)
    gains = [jnp.where(low1, gb[2 * q], roll(gb[2 * q + 1], 64)) for q in range(4)]
    wait_pair(2, wi_of)

    wait_recv(r4.at[pl.ds(0, 7)], PH4)
    tiles = []
    sq = jnp.zeros((32, 1), F32)
    for q in range(4):
        a, b = r4[2 * q].astype(F32), r4[2 * q + 1].astype(F32)
        cur = jnp.concatenate(
            [jnp.where(low16, a, roll(b, 64)), jnp.where(low16, roll(a, 64), b)], axis=0
        )
        sq = sq + jnp.sum(cur * cur, axis=1, keepdims=True)
        tiles.append((cur * gains[q]).astype(BF16))
    part = jnp.dot(
        jnp.concatenate(tiles, axis=1), wi[...].reshape(512, 256), preferred_element_type=F32
    )
    squares = pick4([jnp.broadcast_to(sq[8 * i : 8 * i + 8, :], (8, 128)) for i in range(4)], group8)
    for q in range(2):
        rows = [part[8 * i : 8 * i + 8, 128 * q : 128 * q + 128] for i in range(4)]
        for j in range(4):
            s5[4 * q + j, 0:8, :] = pick4([roll(rows[i], 32 * (i - j)) for i in range(4)], group8)
            s5[4 * q + j, 8:16, :] = squares
    for k in range(1, 8):
        send(s5.at[lax.rem(y + k, 8)], r5.at[y], PH5, at_y(k))
    r5[pl.ds(y, 1)] = s5[pl.ds(y, 1)]
    wait_recv(r5.at[pl.ds(0, 7)], PH5)
    value = recurrence(1, consts1, jnp.sum(r5[...], axis=0))
    gather_readout(1, value, PH6)
    wait_pair(1, w1)

    @pl.when(d != z)
    def _():
        wait_recv(rz1, RES1)

    wait_recv(r2.at[1, pl.ds(0, 7)], PH6)
    piece = unpack_readout(1)
    for k in range(8):
        s7[k] = jnp.dot(
            piece, w[1, k].reshape(256, 128), preferred_element_type=F32
        ).astype(BF16)
    for k in range(8):
        @pl.when(jnp.logical_not(jnp.logical_and(d == k, d == z)))
        def _(k=k):
            send(s7.at[k], r7.at[z], PH7, {"tp": d * 8 + y, "dp": k})

    @pl.when(d == z)
    def _():
        r7[pl.ds(z, 1)] = s7[pl.ds(z, 1)]
        wait_recv(r7.at[pl.ds(0, 7)], PH7)

    @pl.when(d != z)
    def _():
        wait_recv(r7, PH7)

    own = gated(jnp.sum(r7[...].astype(F32), axis=0), rz1[...].astype(F32))

    odd = lax.rem(y + z, 2)

    @pl.when(odd == 0)
    def _():
        oa[pl.ds(y, 1), pl.ds(z // 2, 1)] = own[None, None]
        for k in range(1, 8):
            send(oa.at[y, z // 2], oa.at[y, z // 2], PH8, at_z(k))

    @pl.when(odd == 1)
    def _():
        ob[pl.ds(z, 1), pl.ds(y // 2, 1)] = own[None, None]
        for k in range(1, 8):
            send(ob.at[z, y // 2], ob.at[z, y // 2], PH8, at_y(k))

    wait_recv(r4.at[pl.ds(0, 7)], PH8)
    for k in range(1, 8):
        send(oa.at[y], oa.at[y], PH9A, at_y(k))
        send(ob.at[z], ob.at[z], PH9B, at_z(k))
    wait_recv(oa.at[pl.ds(0, 7)], PH9A)
    wait_recv(ob.at[pl.ds(0, 7)], PH9B)
    for zz in range(8):
        for q in range(4):
            a, b = [
                (oa[yy, zz // 2] if (yy + zz) % 2 == 0 else ob[zz, yy // 2]).astype(F32)
                for yy in (2 * q, 2 * q + 1)
            ]
            mixed_ref[32 * zz : 32 * zz + 32, 128 * q : 128 * q + 128] = jnp.concatenate(
                [jnp.where(low16, a, roll(b, 64)), jnp.where(low16, roll(a, 64), b)], axis=0
            ).astype(BF16)

    wait_sent(s1.at[pl.ds(0, 7)], PH1)
    wait_sent(ws.at[0, pl.ds(0, 7)], ST1A)
    wait_sent(ws.at[1, pl.ds(0, 7)], ST1B)
    wait_sent(wis.at[pl.ds(0, 7)], ST1W)
    wait_sent(gb.at[pl.ds(0, 7)], GAIN)
    wait_sent(r2.at[0, pl.ds(0, 7)], PH2)
    wait_sent(r2.at[1, pl.ds(0, 7)], PH6)
    wait_sent(s3.at[pl.ds(0, 7)], PH3)
    wait_sent(r4.at[pl.ds(0, 7)], PH4)
    wait_sent(s5.at[pl.ds(0, 7)], PH5)
    wait_sent(r4.at[pl.ds(0, 7)], PH8)
    wait_sent(oa.at[pl.ds(0, 7)], PH9A)
    wait_sent(ob.at[pl.ds(0, 7)], PH9B)
    near_sent(0, w.at[0, 0])
    near_sent(1, w.at[1, 0])
    near_sent(2, wi.at[0])

    @pl.when(d == z)
    def _():
        wait_sent(rz.at[pl.ds(0, 7)], RES0)
        wait_sent(s7.at[pl.ds(0, 7)], PH7)

    @pl.when(d != z)
    def _():
        wait_sent(m0, RES1)
        wait_sent(s7, PH7)


def body(tokens, lengths, norm_gain, w_in, log_step, eig_re, eig_im, in_mat, output_matrices, skip,
         w_glu, w_gate, state):
    args = (tokens, lengths.reshape(1, 32), norm_gain, w_in, log_step, eig_re, eig_im, in_mat,
            output_matrices, skip, w_glu, w_gate, state)
    return pl.pallas_call(
        kernel,
        name="decode",
        out_shape=(
            jax.ShapeDtypeStruct((256, 512), BF16),
            jax.ShapeDtypeStruct((2, 2, 32, 128), F32),
        ),
        in_specs=[pl.BlockSpec(memory_space=pl.ANY)] * 13,
        out_specs=(pl.BlockSpec(memory_space=pltpu.VMEM),) * 2,
        scratch_shapes=[pltpu.VMEM(a.shape, a.dtype) for a in args]
        + [
            pltpu.VMEM((8, 16, 128), F32),
            pltpu.VMEM((8, 16, 128), F32),
            pltpu.VMEM((2, 8, 32, 128), BF16),
            pltpu.VMEM((2, 8, 8, 32, 128), BF16),
            pltpu.VMEM((8, 16, 128), BF16),
            pltpu.VMEM((8, 16, 128), BF16),
            pltpu.VMEM((8, 64, 256), BF16),
            pltpu.VMEM((8, 1, 128), F32),
            pltpu.VMEM((9, 16, 128), BF16),
            pltpu.VMEM((16, 128), BF16),
            pltpu.VMEM((2, 8, 128), F32),
            pltpu.VMEM((2, 8, 8, 128), F32),
            pltpu.VMEM((8, 32, 128), BF16),
            pltpu.VMEM((8, 32, 128), BF16),
            pltpu.VMEM((8, 16, 128), BF16),
            pltpu.VMEM((16, 128), BF16),
            pltpu.VMEM((8, 16, 128), F32),
            pltpu.VMEM((8, 16, 128), F32),
            pltpu.VMEM((8, 32, 128), BF16),
            pltpu.VMEM((8, 32, 128), BF16),
            pltpu.VMEM((8, 4, 16, 128), BF16),
            pltpu.VMEM((8, 4, 16, 128), BF16),
            pltpu.SemaphoreType.DMA((13,)),
            pltpu.SemaphoreType.DMA((COUNT,)),
            pltpu.SemaphoreType.DMA((COUNT,)),
        ],
        compiler_params=pltpu.CompilerParams(collective_id=0, has_side_effects=True),
    )(*args)


def solution(mesh):
    placed = (
        P(None, "dp"),
        P("dp"),
        P(None, "dp"),
        P(None, "dp", "tp"),
        P(None, "tp"),
        P(None, "tp", None),
        P(None, "tp", None),
        P(None, None, "tp", None, None),
        P(None, None, "tp", None, None),
        P(None, "tp"),
        P(None, "tp", "dp"),
        P(None, "tp", "dp"),
        P(None, None, "dp", "tp"),
    )
    return jax.shard_map(
        body,
        mesh=mesh,
        in_specs=placed,
        out_specs=(P(None, "dp"), P(None, None, "dp", "tp")),
        check_vma=False,
    )
```

```python
import jax
import jax.numpy as jnp
from jax import lax
from jax.experimental import pallas as pl
from jax.experimental.pallas import tpu as pltpu
from jax.sharding import PartitionSpec as P

D = 4096
LEN_MAX = 4096
BLOCK_LEN = 256
NORM_EPS = 1e-06
MESH = pl.DeviceIdType.MESH
NT = (((1,), (1,)), ((), ()))
F32 = jnp.float32
BF16 = jnp.bfloat16

(PH1, RES0, PH2, ST1B, ST1W, PH3, PH4, RES1, PH5, PH6, PH7, PH9A, PH9B, GAIN) = range(14)
NEAR = 14
PAIR = NEAR + 9
FAR = PAIR + 12
LASTZ = FAR + 7
LASTY = LASTZ + 7
COUNT = LASTY + 7
NEAREST = (1, 7, 2, 6, 3, 5, 4)
FARTHEST = (4, 3, 5, 2, 6, 1, 7)


def roll(x, amount):
    amount = amount % 128
    return x if amount == 0 else pltpu.roll(x, amount, 1)


def groups4(rows):
    return lax.broadcasted_iota(jnp.int32, (rows, 128), 1) // 32


def low_half(rows):
    return lax.broadcasted_iota(jnp.int32, (rows, 128), 1) < 64


def pick4(parts, group):
    out = parts[3]
    for i in (2, 1, 0):
        out = jnp.where(group == i, parts[i], out)
    return out


def split2(x):
    hi = x.astype(BF16)
    lo = (x - hi.astype(F32)).astype(BF16)
    return hi, lo


def kernel(
    tok_h, len_h, gain_h, win_h, ls_h, er_h, ei_h, im_h, om_h, skip_h, glu_h, gate_h, st_h,
    mixed_ref, ns_ref,
    tok, lens, gain, win, ls, er, ei, im, om, skip, glu, gate, st,
    s1, r1, ws, w, wis, pk, wi, gb, rz, rz1, s2, r2, s3, r3, r4, m0, s5, r5, s7, r7, oa, ob,
    lsem, ss, rs,
):
    tp = lax.axis_index("tp")
    d = lax.axis_index("dp")
    z = tp // 8
    y = lax.rem(tp, 8)
    x = d // 2
    core = lax.rem(d, 2)

    def at_y(k):
        return {"tp": z * 8 + lax.rem(y + k, 8), "dp": d}

    def at_z(k):
        return {"tp": lax.rem(z + k, 8) * 8 + y, "dp": d}

    def at_d(k):
        return {"tp": tp, "dp": lax.rem(d + k, 8)}

    def send(src, dst, sem, dev, rsem=None):
        pltpu.make_async_remote_copy(
            src_ref=src,
            dst_ref=dst,
            send_sem=ss.at[sem],
            recv_sem=rs.at[sem if rsem is None else rsem],
            device_id=dev,
            device_id_type=MESH,
        ).start()

    def wait_recv(ref, sem):
        with jax.named_scope(f"recv{sem}"):
            pltpu.make_async_copy(ref, ref, rs.at[sem]).wait()

    def wait_sent(ref, sem):
        pltpu.make_async_copy(ref, ref, ss.at[sem]).wait()

    def pass_on(k):
        block = w.at[0, d, lax.rem(y + 8 - k, 8)]
        if k:
            wait_recv(block, FAR + k - 1)
        for r in range(1, 4):
            to = lax.rem(x + r, 4) * 2 + core
            send(block, block, NEAR + r - 1, {"tp": tp, "dp": to})

    hbm = (tok_h, win_h, gain_h, glu_h, gate_h, len_h, ls_h, er_h, ei_h, im_h, om_h, skip_h, st_h)
    vmem = (tok, win, gain, glu, gate, lens, ls, er, ei, im, om, skip, st)
    loads = [pltpu.make_async_copy(a, b, lsem.at[i]) for i, (a, b) in enumerate(zip(hbm, vmem))]
    for copy in loads[:3]:
        copy.start()

    barrier = pltpu.get_barrier_semaphore()
    for at in (at_y, at_z, at_d):
        for k in FARTHEST:
            pl.semaphore_signal(barrier, inc=1, device_id=at(k), device_id_type=MESH)
    for copy in loads[3:]:
        copy.start()

    def fold_low(t):
        return jnp.where(low16, t[0:16], roll(t[16:32], 64))

    def fold_high(t):
        return jnp.where(low16, roll(t[0:16], 64), t[16:32])

    def unfold(a, b):
        return jnp.concatenate(
            [jnp.where(low16, a, roll(b, 64)), jnp.where(low16, roll(a, 64), b)], axis=0
        )

    group8 = groups4(8)
    low16 = low_half(16)
    low32 = low_half(32)
    low128 = low_half(128)

    with jax.named_scope("load0"):
        for i in range(3):
            loads[i].wait()
    for dd in range(8):
        t = tok[32 * dd : 32 * dd + 32, :].astype(F32)
        scaled = (t * gain[0:1, :]).astype(BF16)
        part = lax.dot_general(scaled, win[0], NT, preferred_element_type=F32)
        sq = jnp.sum(t * t, axis=1, keepdims=True)
        packed = jnp.concatenate([part[8 * i : 8 * i + 8, :] for i in range(4)], axis=1)
        spread = pick4([jnp.broadcast_to(sq[8 * i : 8 * i + 8, :], (8, 128)) for i in range(4)], group8)
        s1[dd] = jnp.concatenate([packed, spread], axis=0).astype(BF16)
    r1[pl.ds(d, 1)] = s1[pl.ds(d, 1)]

    loads[3].wait()
    loads[4].wait()

    def pack_projection(layer):
        for q in range(4):
            g = glu[layer, :, 128 * q : 128 * q + 128].astype(F32)
            t = gate[layer, :, 128 * q : 128 * q + 128].astype(F32)
            ws[layer, 2 * q] = jnp.where(low32, g, roll(t, 64)).astype(BF16)
            ws[layer, 2 * q + 1] = jnp.where(low32, roll(g, 64), t).astype(BF16)
        w[layer, pl.ds(d, 1), pl.ds(y, 1)] = ws[layer, pl.ds(y, 1)][None]

    pack_projection(0)

    half = lax.rem(y, 2)
    column = pl.ds(pl.multiple_of((y // 2) * 128, 128), 128)
    for dd in range(8):
        t = tok[32 * dd : 32 * dd + 32, column].astype(F32)
        t = jnp.where(half == 1, roll(t, 64), t)
        rz[dd] = fold_low(t).astype(BF16)

    @pl.when(d == z)
    def _():
        rz[8] = rz[pl.ds(d, 1)][0]

    with jax.named_scope("entry"):
        pl.semaphore_wait(barrier, 21)

    for k in FARTHEST:
        to = lax.rem(d + k, 8)
        send(s1.at[to], r1.at[d], PH1, at_d(k))
    for k in FARTHEST:
        to = lax.rem(y + k, 8)
        send(ws.at[0, to], w.at[0, d, y], FAR + k - 1, at_y(k))
    pass_on(0)

    @pl.when(d == z)
    def _():
        for k in FARTHEST:
            send(rz.at[lax.rem(d + k, 8)], rz.at[8], RES0, at_d(k))

    for i in range(5, 13):
        loads[i].wait()
    eye = lax.broadcasted_iota(jnp.int32, (32, 32), 0) == lax.broadcasted_iota(jnp.int32, (32, 32), 1)
    blocks = (lens[...] // BLOCK_LEN).astype(F32)
    blocks = jnp.sum(jnp.where(eye, jnp.broadcast_to(blocks, (32, 32)), 0.0), axis=1, keepdims=True)
    factor = 2.0 / (1.0 + blocks * (4.0 * BLOCK_LEN / LEN_MAX))

    def by_group(slabs, sign):
        zero = jnp.zeros((16, 64), F32)
        cols = []
        for c in range(2):
            top = jnp.concatenate([slabs[2 * c], zero], axis=1)
            low = jnp.concatenate([zero, slabs[2 * c + 1]], axis=1)
            both = jnp.concatenate([top, low], axis=0)
            cols.append(both if c == 0 else sign * both)
        return jnp.concatenate([jnp.concatenate(cols, axis=1)] * 4, axis=0)

    def constants(layer):
        def row(ref):
            return jnp.concatenate([ref[layer, 0:1, :], ref[layer, 1:2, :]], axis=1)

        e_re, e_im = row(er), row(ei)
        rate = jnp.exp(ls[layer : layer + 1, :])
        rate = jnp.concatenate(
            [jnp.broadcast_to(rate[:, 0:1], (1, 64)), jnp.broadcast_to(rate[:, 1:2], (1, 64))], axis=1
        )
        step = rate * factor
        magnitude = jnp.exp(e_re * step)
        turned = e_im * step
        a_re = magnitude * jnp.cos(turned)
        a_im = magnitude * jnp.sin(turned)
        modulus = e_re * e_re + e_im * e_im
        b_re = ((a_re - 1.0) * e_re + a_im * e_im) / modulus
        b_im = (a_im * e_re - (a_re - 1.0) * e_im) / modulus
        u, v = st[layer, 0], st[layer, 1]
        k_re = a_re * u - a_im * v
        k_im = a_re * v + a_im * u
        hi, lo = split2(by_group([im[layer, c, g] for c in range(2) for g in range(2)], 1.0))
        in_cat = jnp.concatenate([hi, lo], axis=0)
        hi, lo = split2(by_group([om[layer, c, g] for c in range(2) for g in range(2)], -1.0))
        out_cat = jnp.concatenate([hi, lo, hi], axis=1)
        direct = jnp.concatenate([skip[layer : layer + 1, :]] * 4, axis=1)
        return k_re, k_im, b_re, b_im, in_cat, out_cat, direct

    def recurrence(layer, consts, total):
        k_re, k_im, b_re, b_im, in_cat, out_cat, direct = consts
        driven = (total[0:8] * lax.rsqrt(total[8:16] / D + NORM_EPS)).astype(BF16).astype(F32)
        spread = jnp.concatenate([jnp.where(group8 == i, driven, 0.0) for i in range(4)], axis=0)
        spread = spread.astype(BF16)
        drive = lax.dot_general(
            jnp.concatenate([spread, spread], axis=1), in_cat, (((1,), (0,)), ((), ())),
            preferred_element_type=F32,
        )
        d_re, d_im = drive[:, 0:128], drive[:, 128:256]
        n_re = k_re + b_re * d_re - b_im * d_im
        n_im = k_im + b_re * d_im + b_im * d_re
        ns_ref[layer, 0] = n_re
        ns_ref[layer, 1] = n_im
        hi, lo = split2(jnp.concatenate([n_re, n_im], axis=1))
        full = lax.dot_general(
            jnp.concatenate([hi, hi, lo], axis=1), out_cat, NT, preferred_element_type=F32
        )
        value = pick4([full[8 * i : 8 * i + 8] for i in range(4)], group8) + direct * driven
        inner = 0.7978845608028654 * (value + 0.044715 * (value * value * value))
        return (value * (0.5 * (1.0 + jnp.tanh(inner)))).astype(BF16)

    def gather_readout(layer, value, sem):
        s2[layer] = value
        r2[layer, pl.ds(y, 1)] = value[None]
        for k in FARTHEST:
            send(s2.at[layer], r2.at[layer, y], sem, at_y(k))

    def unpack_readout(layer):
        got = [r2[layer, j].astype(F32) for j in range(8)]
        tiles = []
        for i in range(4):
            tiles.append(
                jnp.concatenate(
                    [
                        pick4([roll(got[4 * q + j], 32 * (j - i)) for j in range(4)], group8)
                        for q in range(2)
                    ],
                    axis=1,
                )
            )
        return jnp.concatenate(tiles, axis=0).astype(BF16)

    def near(kind, ref_of):
        mine = ref_of(d)
        for r in range(1, 4):
            to = lax.rem(x + r, 4) * 2 + core
            send(mine, mine, NEAR + 3 * kind + r - 1, {"tp": tp, "dp": to})
        to_pair(kind, ref_of)

    def to_pair(kind, ref_of):
        send(ref_of(d), ref_of(d), PAIR + 4 * kind, {"tp": tp, "dp": x * 2 + 1 - core})

    def relay(kind, ref_of):
        for r in range(1, 4):
            ref = ref_of(lax.rem(x + 4 - r, 4) * 2 + core)
            wait_recv(ref, NEAR + 3 * kind + r - 1)
            send(ref, ref, PAIR + 4 * kind + r, {"tp": tp, "dp": x * 2 + 1 - core})

    def wait_pair(kind, ref_of):
        for r in range(4):
            wait_recv(ref_of(lax.rem(x + 4 - r, 4) * 2 + 1 - core), PAIR + 4 * kind + r)

    def near_sent(kind, ref):
        for r in range(3):
            wait_sent(ref, NEAR + 3 * kind + r)
        for r in range(4):
            wait_sent(ref, PAIR + 4 * kind + r)

    def w0(k):
        return w.at[0, k]

    def w1(k):
        return w.at[1, k]

    def wi_of(k):
        return wi.at[k]

    consts0 = constants(0)

    for k in NEAREST[:4]:
        pass_on(k)
    wait_recv(r1.at[pl.ds(0, 7)], PH1)
    value = recurrence(0, consts0, jnp.sum(r1[...].astype(F32), axis=0))
    gather_readout(0, value, PH2)
    for k in NEAREST[4:]:
        pass_on(k)
    to_pair(0, w0)

    pack_projection(1)
    for q in range(4):
        t = win[1, :, 128 * q : 128 * q + 128].astype(F32)
        wis[2 * q] = fold_low(t).astype(BF16)
        wis[2 * q + 1] = fold_high(t).astype(BF16)
    pk[pl.ds(y, 1)] = wis[pl.ds(y, 1)]
    for k in FARTHEST:
        to = lax.rem(y + k, 8)
        send(wis.at[to], pk.at[y], ST1W, at_y(k))
    for k in FARTHEST:
        to = lax.rem(y + k, 8)
        send(ws.at[1, to], w.at[1, d, y], ST1B, at_y(k))
    own_gain = gain[1:2, column]
    gb[pl.ds(d, 1)] = jnp.where(half == 1, roll(own_gain, 64), own_gain)[None]
    for k in FARTHEST:
        send(gb.at[d], gb.at[d], GAIN, at_d(k))

    relay(0, w0)
    wait_recv(r2.at[0, pl.ds(0, 7)], PH2)
    piece = unpack_readout(0)
    wait_pair(0, w0)
    for k in range(8):
        s3[k] = jnp.dot(
            piece, w[0, k].reshape(256, 128), preferred_element_type=F32
        ).astype(BF16)
    for k in FARTHEST:
        send(s3.at[lax.rem(z + k, 8)], r3.at[z], PH3, at_z(k))
    r3[pl.ds(z, 1)] = s3[pl.ds(z, 1)]

    wait_recv(pk.at[pl.ds(0, 7)], ST1W)
    for j in range(4):
        rows = unfold(pk[j].astype(F32), pk[4 + j].astype(F32)).astype(BF16)
        wi[pl.ds(d, 1), 32 * j : 32 * j + 32, :] = rows[None]
    near(2, wi_of)
    wait_recv(w.at[1, 0, pl.ds(0, 7)], ST1B)
    near(1, w1)

    @pl.when(d != z)
    def _():
        wait_recv(rz.at[8], RES0)

    def gated(parts, residual):
        linear, gate_sum = fold_low(parts), fold_high(parts)
        return (residual + linear * (1.0 / (1.0 + jnp.exp(-gate_sum)))).astype(BF16)

    residual0 = rz[8].astype(F32)
    wait_recv(r3.at[pl.ds(0, 7)], PH3)
    own = gated(jnp.sum(r3[...].astype(F32), axis=0), residual0)
    m0[...] = own
    r4[pl.ds(z, 1)] = own[None]
    for k in FARTHEST:
        send(m0, r4.at[z], PH4, at_z(k))

    alone = jnp.logical_and(z == 0, d == 0)

    @pl.when(jnp.logical_not(alone))
    def _():
        send(m0, rz1, RES1, {"tp": lax.rem(d + z, 8) * 8 + y, "dp": z})

    @pl.when(alone)
    def _():
        rz1[...] = own

    relay(2, wi_of)
    relay(1, w1)
    consts1 = constants(1)
    wait_recv(gb.at[pl.ds(0, 7)], GAIN)
    low1 = low_half(1)
    gains = [jnp.where(low1, gb[2 * q], roll(gb[2 * q + 1], 64)) for q in range(4)]
    wait_pair(2, wi_of)
    cols = []
    for q in range(4):
        a, b = wi[2 * q].astype(F32), wi[2 * q + 1].astype(F32)
        cols.append(
            jnp.concatenate(
                [jnp.where(low128, a, roll(b, 64)), jnp.where(low128, roll(a, 64), b)], axis=0
            ).astype(BF16)
        )
    win_t = jnp.concatenate(cols, axis=1)

    wait_recv(r4.at[pl.ds(0, 7)], PH4)
    tiles = []
    sq = jnp.zeros((32, 1), F32)
    for q in range(4):
        cur = unfold(r4[2 * q].astype(F32), r4[2 * q + 1].astype(F32))
        sq = sq + jnp.sum(cur * cur, axis=1, keepdims=True)
        tiles.append((cur * gains[q]).astype(BF16))
    part = lax.dot_general(jnp.concatenate(tiles, axis=1), win_t, NT, preferred_element_type=F32)
    squares = pick4([jnp.broadcast_to(sq[8 * i : 8 * i + 8, :], (8, 128)) for i in range(4)], group8)
    for q in range(2):
        rows = [part[8 * i : 8 * i + 8, 128 * q : 128 * q + 128] for i in range(4)]
        for j in range(4):
            packed = pick4([roll(rows[i], 32 * (i - j)) for i in range(4)], group8)
            s5[4 * q + j] = jnp.concatenate([packed, squares], axis=0).astype(BF16)
    for k in FARTHEST:
        send(s5.at[lax.rem(y + k, 8)], r5.at[y], PH5, at_y(k))
    r5[pl.ds(y, 1)] = s5[pl.ds(y, 1)]
    wait_recv(r5.at[pl.ds(0, 7)], PH5)
    value = recurrence(1, consts1, jnp.sum(r5[...].astype(F32), axis=0))
    gather_readout(1, value, PH6)
    wait_pair(1, w1)

    @pl.when(jnp.logical_or(z != 0, d != 0))
    def _():
        wait_recv(rz1, RES1)

    wait_recv(r2.at[1, pl.ds(0, 7)], PH6)
    piece = unpack_readout(1)
    for k in range(8):
        s7[k] = jnp.dot(
            piece, w[1, k].reshape(256, 128), preferred_element_type=F32
        ).astype(BF16)
    keeps = z == lax.rem(2 * d, 8)
    for k in (0, *FARTHEST):
        to = lax.rem(d + k, 8)
        dev = {"tp": lax.rem(d + to, 8) * 8 + y, "dp": to}
        if k:
            send(s7.at[to], r7.at[z], PH7, dev)
        else:

            @pl.when(jnp.logical_not(keeps))
            def _(to=to, dev=dev):
                send(s7.at[to], r7.at[z], PH7, dev)

    wait_sent(s1.at[pl.ds(0, 7)], PH1)
    for k in range(7):
        wait_sent(ws.at[0, 0], FAR + k)
    wait_sent(ws.at[1, pl.ds(0, 7)], ST1B)
    wait_sent(wis.at[pl.ds(0, 7)], ST1W)
    wait_sent(gb.at[pl.ds(0, 7)], GAIN)
    wait_sent(r2.at[0, pl.ds(0, 7)], PH2)
    wait_sent(r2.at[1, pl.ds(0, 7)], PH6)
    wait_sent(s3.at[pl.ds(0, 7)], PH3)
    wait_sent(r4.at[pl.ds(0, 7)], PH4)
    wait_sent(s5.at[pl.ds(0, 7)], PH5)
    near_sent(0, w.at[0, 0])
    near_sent(1, w.at[1, 0])
    near_sent(2, wi.at[0])

    @pl.when(d == z)
    def _():
        wait_sent(rz.at[pl.ds(0, 7)], RES0)

    @pl.when(jnp.logical_or(z != 0, d != 0))
    def _():
        wait_sent(m0, RES1)

    @pl.when(keeps)
    def _():
        r7[pl.ds(z, 1)] = s7[pl.ds(d, 1)]
        wait_recv(r7.at[pl.ds(0, 7)], PH7)

    @pl.when(jnp.logical_not(keeps))
    def _():
        wait_recv(r7, PH7)

    own = gated(jnp.sum(r7[...].astype(F32), axis=0), rz1[...].astype(F32))

    odd = lax.rem(y + z, 2)

    def forward_a(zz):
        for k in FARTHEST:
            send(oa.at[y, zz // 2], oa.at[y, zz // 2], PH9A, at_y(k))

    def forward_b(yy):
        for k in FARTHEST:
            send(ob.at[z, yy // 2], ob.at[z, yy // 2], PH9B, at_z(k))

    def from_z(k):
        zz = lax.rem(z + 8 - k, 8)
        wait_recv(oa.at[y, zz // 2], LASTZ + k - 1)
        forward_a(zz)

    def from_y(k):
        yy = lax.rem(y + 8 - k, 8)
        wait_recv(ob.at[z, yy // 2], LASTY + k - 1)
        forward_b(yy)

    @pl.when(odd == 0)
    def _():
        oa[pl.ds(y, 1), pl.ds(z // 2, 1)] = own[None, None]
        for k in FARTHEST:
            send(oa.at[y, z // 2], oa.at[y, z // 2], LASTZ + k - 1, at_z(k))
        forward_a(z)
        for k in NEAREST:
            (from_z if k % 2 == 0 else from_y)(k)

    @pl.when(odd == 1)
    def _():
        ob[pl.ds(z, 1), pl.ds(y // 2, 1)] = own[None, None]
        for k in FARTHEST:
            send(ob.at[z, y // 2], ob.at[z, y // 2], LASTY + k - 1, at_y(k))
        forward_b(y)
        for k in NEAREST:
            (from_y if k % 2 == 0 else from_z)(k)

    wait_recv(oa.at[pl.ds(0, 7)], PH9A)
    wait_recv(ob.at[pl.ds(0, 7)], PH9B)
    for zz in range(8):
        rows = pl.ds(pl.multiple_of(lax.rem(zz + 8 - d, 8) * 32, 32), 32)
        for q in range(4):
            a, b = [
                (oa[yy, zz // 2] if (yy + zz) % 2 == 0 else ob[zz, yy // 2]).astype(F32)
                for yy in (2 * q, 2 * q + 1)
            ]
            mixed_ref[rows, 128 * q : 128 * q + 128] = unfold(a, b).astype(BF16)

    wait_sent(oa.at[pl.ds(0, 7)], PH9A)
    wait_sent(ob.at[pl.ds(0, 7)], PH9B)
    @pl.when(odd == 0)
    def _():
        for k in range(7):
            wait_sent(m0, LASTZ + k)

    @pl.when(odd == 1)
    def _():
        for k in range(7):
            wait_sent(m0, LASTY + k)

    @pl.when(keeps)
    def _():
        wait_sent(s7.at[pl.ds(0, 7)], PH7)

    @pl.when(jnp.logical_not(keeps))
    def _():
        wait_sent(s7, PH7)


def body(tokens, lengths, norm_gain, w_in, log_step, eig_re, eig_im, in_mat, output_matrices, skip,
         w_glu, w_gate, state):
    args = (tokens, lengths.reshape(1, 32), norm_gain, w_in.swapaxes(1, 2), log_step, eig_re, eig_im,
            in_mat.swapaxes(3, 4), output_matrices, skip, w_glu, w_gate, state)
    return pl.pallas_call(
        kernel,
        name="decode",
        out_shape=(pltpu.VMEM((256, 512), BF16), pltpu.VMEM((2, 2, 32, 128), F32)),
        in_specs=[pl.BlockSpec(memory_space=pl.ANY)] * 13,
        out_specs=(pl.BlockSpec(memory_space=pltpu.VMEM),) * 2,
        scratch_shapes=[pltpu.VMEM(a.shape, a.dtype) for a in args]
        + [
            pltpu.VMEM((8, 16, 128), BF16),
            pltpu.VMEM((8, 16, 128), BF16),
            pltpu.VMEM((2, 8, 32, 128), BF16),
            pltpu.VMEM((2, 8, 8, 32, 128), BF16),
            pltpu.VMEM((8, 16, 128), BF16),
            pltpu.VMEM((8, 16, 128), BF16),
            pltpu.VMEM((8, 128, 128), BF16),
            pltpu.VMEM((8, 1, 128), F32),
            pltpu.VMEM((9, 16, 128), BF16),
            pltpu.VMEM((16, 128), BF16),
            pltpu.VMEM((2, 8, 128), BF16),
            pltpu.VMEM((2, 8, 8, 128), BF16),
            pltpu.VMEM((8, 32, 128), BF16),
            pltpu.VMEM((8, 32, 128), BF16),
            pltpu.VMEM((8, 16, 128), BF16),
            pltpu.VMEM((16, 128), BF16),
            pltpu.VMEM((8, 16, 128), BF16),
            pltpu.VMEM((8, 16, 128), BF16),
            pltpu.VMEM((8, 32, 128), BF16),
            pltpu.VMEM((8, 32, 128), BF16),
            pltpu.VMEM((8, 4, 16, 128), BF16),
            pltpu.VMEM((8, 4, 16, 128), BF16),
            pltpu.SemaphoreType.DMA((13,)),
            pltpu.SemaphoreType.DMA((COUNT,)),
            pltpu.SemaphoreType.DMA((COUNT,)),
        ],
        compiler_params=pltpu.CompilerParams(collective_id=0, has_side_effects=True),
    )(*args)


def solution(mesh):
    placed = (
        P(None, "dp"),
        P("dp"),
        P(None, "dp"),
        P(None, "dp", "tp"),
        P(None, "tp"),
        P(None, "tp", None),
        P(None, "tp", None),
        P(None, None, "tp", None, None),
        P(None, None, "tp", None, None),
        P(None, "tp"),
        P(None, "tp", "dp"),
        P(None, "tp", "dp"),
        P(None, None, "dp", "tp"),
    )
    return jax.shard_map(
        body,
        mesh=mesh,
        in_specs=placed,
        out_specs=(P(None, "dp"), P(None, None, "dp", "tp")),
        check_vma=False,
    )
```

```python
import jax
import jax.numpy as jnp
from jax import lax
from jax.experimental import pallas as pl
from jax.experimental.pallas import tpu as pltpu
from jax.sharding import PartitionSpec as P

D = 4096
LEN_MAX = 4096
BLOCK_LEN = 256
NORM_EPS = 1e-06
MESH = pl.DeviceIdType.MESH
NT = (((1,), (1,)), ((), ()))
F32 = jnp.float32
BF16 = jnp.bfloat16

(PH1, RES0, PH2, ST1N, ST1S, STWN, STWS, PH3, PH4, RES1, PH5, PH6, PH7, PH9A, PH9B, GAIN, STATE, COUNTS, NEW) = range(19)
NEAR = 20
FARN = NEAR + 9
FARS = FARN + 8
LASTZ = FARS + 8
LASTY = LASTZ + 8
COUNT = LASTY + 8
NEAREST = (1, 7, 2, 6, 3, 5, 4)
FARTHEST = (4, 3, 5, 2, 6, 1, 7)


def roll(x, amount):
    amount = amount % 128
    return x if amount == 0 else pltpu.roll(x, amount, 1)


def groups4(rows):
    return lax.broadcasted_iota(jnp.int32, (rows, 128), 1) // 32


def low_half(rows):
    return lax.broadcasted_iota(jnp.int32, (rows, 128), 1) < 64


def pick4(parts, group):
    out = parts[3]
    for i in (2, 1, 0):
        out = jnp.where(group == i, parts[i], out)
    return out


def split2(x):
    hi = x.astype(BF16)
    lo = (x - hi.astype(F32)).astype(BF16)
    return hi, lo


def kernel(
    tok_h, len_h, gain_h, win_h, ls_h, er_h, ei_h, im_h, om_h, skip_h, glu_h, gate_h, st_h,
    mixed_ref, ns_ref,
    tok, lens, gain, win, ls, er, ei, im, om, skip, glu, gate, st,
    s1, r1, ws, w, wis, pk, wi, gb, rz, rz1, s2, r2, s3, r3, r4, m0, s5, r5, s7, r7, oa, ob,
    counts, st2, nsend, nrecv,
    lsem, ss, rs,
):
    tp = lax.axis_index("tp")
    d = lax.axis_index("dp")
    z = tp // 8
    y = lax.rem(tp, 8)
    x = d // 2
    core = lax.rem(d, 2)
    one = 2 * x + 1

    def at_y(k, dp=None):
        return {"tp": z * 8 + lax.rem(y + k, 8), "dp": one if dp is None else dp}

    def at_z(k, dp=None):
        return {"tp": lax.rem(z + k, 8) * 8 + y, "dp": one if dp is None else dp}

    def at_x(k, c=1):
        return {"tp": tp, "dp": 2 * lax.rem(x + k, 4) + c}

    def send(src, dst, sem, dev):
        pltpu.make_async_remote_copy(
            src_ref=src,
            dst_ref=dst,
            send_sem=ss.at[sem],
            recv_sem=rs.at[sem],
            device_id=dev,
            device_id_type=MESH,
        ).start()

    def wait_recv(ref, sem):
        with jax.named_scope(f"recv{sem}"):
            pltpu.make_async_copy(ref, ref, rs.at[sem]).wait()

    def wait_sent(ref, sem):
        pltpu.make_async_copy(ref, ref, ss.at[sem]).wait()

    def fold_low(t):
        n = t.shape[0] // 2
        return jnp.where(low_half(n), t[0:n], roll(t[n : 2 * n], 64))

    def fold_high(t):
        n = t.shape[0] // 2
        return jnp.where(low_half(n), roll(t[0:n], 64), t[n : 2 * n])

    def unfold(a, b):
        low = low_half(a.shape[0])
        return jnp.concatenate([jnp.where(low, a, roll(b, 64)), jnp.where(low, roll(a, 64), b)], axis=0)

    hbm = (tok_h, win_h, gain_h, glu_h, gate_h, len_h, st_h, ls_h, er_h, ei_h, im_h, om_h, skip_h)
    vmem = (tok, win, gain, glu, gate, lens, st, ls, er, ei, im, om, skip)
    loads = [pltpu.make_async_copy(a, b, lsem.at[i]) for i, (a, b) in enumerate(zip(hbm, vmem))]
    for copy in loads[:3]:
        copy.start()

    barrier = pltpu.get_barrier_semaphore()

    def greet(dev):
        pl.semaphore_signal(barrier, inc=1, device_id=dev, device_id_type=MESH)

    @pl.when(core == 1)
    def _():
        for k in FARTHEST:
            greet(at_y(k, 2 * x))
            greet(at_y(k))
            greet(at_z(k))
        for k in (2, 3, 1):
            greet(at_x(k, 0))
            greet(at_x(k))
        greet(at_x(0, 0))

    @pl.when(core == 0)
    def _():
        greet(at_x(0))

    for copy in loads[3:]:
        copy.start()
    group8 = groups4(8)

    def rows4(t):
        return pick4([jnp.broadcast_to(t[8 * i : 8 * i + 8], (8, 128)) for i in range(4)], group8)

    with jax.named_scope("load0"):
        for i in range(3):
            loads[i].wait()
    for xx in range(4):
        t = tok[64 * xx : 64 * xx + 64, :].astype(F32)
        scaled = (t * gain[0:1, :]).astype(BF16)
        part = lax.dot_general(scaled, win[0], NT, preferred_element_type=F32)
        sq = jnp.sum(t * t, axis=1, keepdims=True)
        packed = [
            jnp.concatenate([part[32 * h + 8 * i : 32 * h + 8 * i + 8, :] for i in range(4)], axis=1)
            for h in range(2)
        ]
        spread = [rows4(sq[32 * h : 32 * h + 32]) for h in range(2)]
        s1[xx] = jnp.concatenate(packed + spread, axis=0).astype(BF16)

    loads[3].wait()
    loads[4].wait()
    low32 = low_half(32)

    def pack_projection(layer):
        for q in range(4):
            g = glu[layer, :, 128 * q : 128 * q + 128].astype(F32)
            t = gate[layer, :, 128 * q : 128 * q + 128].astype(F32)
            ws[layer, 2 * q] = jnp.where(low32, g, roll(t, 64)).astype(BF16)
            ws[layer, 2 * q + 1] = jnp.where(low32, roll(g, 64), t).astype(BF16)

    pack_projection(0)

    half = lax.rem(y, 2)
    column = pl.ds(pl.multiple_of((y // 2) * 128, 128), 128)

    def pack_residual():
        for xx in range(4):
            t = tok[64 * xx : 64 * xx + 64, column].astype(F32)
            rz[xx] = fold_low(jnp.where(half == 1, roll(t, 64), t)).astype(BF16)

    def pack_input_weights():
        for q in range(4):
            t = win[1, :, 128 * q : 128 * q + 128].astype(F32)
            wis[2 * q] = fold_low(t).astype(BF16)
            wis[2 * q + 1] = fold_high(t).astype(BF16)

    def pack_gain():
        t = gain[1:2, column]
        return jnp.where(half == 1, roll(t, 64), t)[None]

    def assemble(g):
        for m in range(4):
            rows = pl.ds(pl.multiple_of((lax.rem(2 * m + g + 8 - 2 * x, 8) // 2) * 64, 64), 64)
            for q in range(4):
                a, b = (oa[2 * q, m], ob[2 * m, q]) if g == 0 else (ob[2 * m + 1, q], oa[2 * q + 1, m])
                mixed_ref[rows, 128 * q : 128 * q + 128] = unfold(a.astype(F32), b.astype(F32)).astype(BF16)

    @pl.when(core == 0)
    def _():
        with jax.named_scope("entry"):
            pl.semaphore_wait(barrier, 11)
        for k in (2, 3, 1, 0):
            send(s1.at[lax.rem(x + k, 4)], r1.at[d], PH1, at_x(k))
        for k in (0, *FARTHEST):
            send(ws.at[0, lax.rem(y + k, 8)], w.at[0, x, y, 0], FARS + k, at_y(k))
        loads[5].wait()
        counts[0] = (lens[...] // BLOCK_LEN).astype(F32)
        send(counts.at[0], counts.at[0], COUNTS, at_x(0))
        loads[6].wait()
        send(st, st2, STATE, at_x(0))

        @pl.when(d == z)
        def _():
            pack_residual()
            for k in range(4):
                send(rz.at[lax.rem(x + k, 4)], rz.at[4], RES0, at_x(k))

        pack_input_weights()
        for k in (0, *FARTHEST):
            send(wis.at[lax.rem(y + k, 8)], pk.at[0, y], STWS, at_y(k))
        gb[pl.ds(d, 1)] = pack_gain()
        for k in range(4):
            send(gb.at[d], gb.at[d], GAIN, at_x(k))
        pack_projection(1)
        for k in (0, *FARTHEST):
            send(ws.at[1, lax.rem(y + k, 8)], w.at[1, x, y, 0], ST1S, at_y(k))
        for i in range(7, 13):
            loads[i].wait()

        wait_sent(s1, PH1)
        for k in range(8):
            wait_sent(ws.at[0, 0], FARS + k)
        wait_sent(counts.at[0], COUNTS)
        wait_sent(st, STATE)

        @pl.when(d == z)
        def _():
            wait_sent(rz.at[pl.ds(0, 4)], RES0)

        wait_sent(wis, STWS)
        wait_sent(gb.at[pl.ds(0, 4)], GAIN)
        wait_sent(ws.at[1], ST1S)

        wait_recv(nrecv, NEW)
        ns_ref[...] = nrecv[...]
        wait_recv(oa.at[pl.ds(0, 4)], PH9A)
        wait_recv(ob.at[pl.ds(0, 4)], PH9B)
        assemble(0)

    @pl.when(core == 1)
    def _():
        r1[pl.ds(d, 1)] = s1[pl.ds(x, 1)]
        w[0, pl.ds(x, 1), pl.ds(y, 1), 1] = ws[0, pl.ds(y, 1)][None]

        @pl.when(d == z)
        def _():
            pack_residual()
            rz[4] = rz[pl.ds(x, 1)][0]

        with jax.named_scope("entry"):
            pl.semaphore_wait(barrier, 18)
        for k in (2, 3, 1):
            send(s1.at[lax.rem(x + k, 4)], r1.at[d], PH1, at_x(k))
        for k in FARTHEST:
            send(ws.at[0, lax.rem(y + k, 8)], w.at[0, x, y, 1], FARN + k, at_y(k))

        def pass_on(k):
            yy = lax.rem(y + 8 - k, 8)
            block = w.at[0, x, yy]
            if k:
                wait_recv(w.at[0, x, yy, 1], FARN + k)
            wait_recv(w.at[0, x, yy, 0], FARS + k)
            for r in (2, 3, 1):
                send(block, block, NEAR + r - 1, at_x(r))

        @pl.when(d == z)
        def _():
            for k in (2, 3, 1):
                send(rz.at[lax.rem(x + k, 4)], rz.at[4], RES0, at_x(k))

        loads[5].wait()
        counts[1] = (lens[...] // BLOCK_LEN).astype(F32)
        for i in range(6, 13):
            loads[i].wait()
        wait_recv(counts.at[0], COUNTS)
        wait_recv(st2, STATE)
        eye = lax.broadcasted_iota(jnp.int32, (32, 32), 0) == lax.broadcasted_iota(jnp.int32, (32, 32), 1)
        blocks = jnp.concatenate(
            [
                jnp.sum(jnp.where(eye, jnp.broadcast_to(counts[h], (32, 32)), 0.0), axis=1, keepdims=True)
                for h in range(2)
            ],
            axis=0,
        )
        factor = 2.0 / (1.0 + blocks * (4.0 * BLOCK_LEN / LEN_MAX))

        def by_group(slabs, sign):
            zero = jnp.zeros((16, 64), F32)
            cols = []
            for c in range(2):
                top = jnp.concatenate([slabs[2 * c], zero], axis=1)
                low = jnp.concatenate([zero, slabs[2 * c + 1]], axis=1)
                both = jnp.concatenate([top, low], axis=0)
                cols.append(both if c == 0 else sign * both)
            return jnp.concatenate([jnp.concatenate(cols, axis=1)] * 4, axis=0)

        def constants(layer):
            def row(ref):
                return jnp.concatenate([ref[layer, 0:1, :], ref[layer, 1:2, :]], axis=1)

            e_re, e_im = row(er), row(ei)
            rate = jnp.exp(ls[layer : layer + 1, :])
            rate = jnp.concatenate(
                [jnp.broadcast_to(rate[:, 0:1], (1, 64)), jnp.broadcast_to(rate[:, 1:2], (1, 64))], axis=1
            )
            step = rate * factor
            magnitude = jnp.exp(e_re * step)
            turned = e_im * step
            a_re = magnitude * jnp.cos(turned)
            a_im = magnitude * jnp.sin(turned)
            modulus = e_re * e_re + e_im * e_im
            b_re = ((a_re - 1.0) * e_re + a_im * e_im) / modulus
            b_im = (a_im * e_re - (a_re - 1.0) * e_im) / modulus
            u = jnp.concatenate([st2[layer, 0], st[layer, 0]], axis=0)
            v = jnp.concatenate([st2[layer, 1], st[layer, 1]], axis=0)
            k_re = a_re * u - a_im * v
            k_im = a_re * v + a_im * u
            hi, lo = split2(by_group([im[layer, c, g] for c in range(2) for g in range(2)], 1.0))
            in_cat = jnp.concatenate([hi, lo], axis=0)
            hi, lo = split2(by_group([om[layer, c, g] for c in range(2) for g in range(2)], -1.0))
            out_cat = jnp.concatenate([hi, lo, hi], axis=1)
            direct = jnp.concatenate([skip[layer : layer + 1, :]] * 4, axis=1)
            return k_re, k_im, b_re, b_im, in_cat, out_cat, direct

        def recurrence(layer, consts, total):
            k_re, k_im, b_re, b_im, in_cat, out_cat, direct = consts
            driven = (total[0:16] * lax.rsqrt(total[16:32] / D + NORM_EPS)).astype(BF16).astype(F32)
            spread = jnp.concatenate(
                [jnp.where(group8 == i, driven[8 * h : 8 * h + 8], 0.0) for h in range(2) for i in range(4)],
                axis=0,
            ).astype(BF16)
            drive = lax.dot_general(
                jnp.concatenate([spread, spread], axis=1), in_cat, (((1,), (0,)), ((), ())),
                preferred_element_type=F32,
            )
            d_re, d_im = drive[:, 0:128], drive[:, 128:256]
            n_re = k_re + b_re * d_re - b_im * d_im
            n_im = k_im + b_re * d_im + b_im * d_re
            for part, new in ((0, n_re), (1, n_im)):
                nsend[layer, part] = new[0:32]
                ns_ref[layer, part] = new[32:64]
            hi, lo = split2(jnp.concatenate([n_re, n_im], axis=1))
            full = lax.dot_general(
                jnp.concatenate([hi, hi, lo], axis=1), out_cat, NT, preferred_element_type=F32
            )
            value = jnp.concatenate([rows4(full[32 * h : 32 * h + 32]) for h in range(2)], axis=0)
            value = value + direct * driven
            inner = 0.7978845608028654 * (value + 0.044715 * (value * value * value))
            return (value * (0.5 * (1.0 + jnp.tanh(inner)))).astype(BF16)

        def gather_readout(layer, value, sem):
            s2[layer] = value
            r2[layer, pl.ds(y, 1)] = value[None]
            for k in FARTHEST:
                send(s2.at[layer], r2.at[layer, y], sem, at_y(k))

        def unpack_readout(layer):
            got = [r2[layer, j].astype(F32) for j in range(8)]
            tiles = []
            for h in range(2):
                for i in range(4):
                    cols = []
                    for q in range(2):
                        parts = [got[4 * q + j][8 * h : 8 * h + 8] for j in range(4)]
                        cols.append(pick4([roll(parts[j], 32 * (j - i)) for j in range(4)], group8))
                    tiles.append(jnp.concatenate(cols, axis=1))
            return jnp.concatenate(tiles, axis=0).astype(BF16)

        def project(layer, piece, k):
            return jnp.dot(
                piece, w[layer, k // 2, :, k % 2].reshape(256, 128), preferred_element_type=F32
            ).astype(BF16)

        def near(kind, block):
            for r in (2, 3, 1):
                send(block, block, NEAR + 3 * kind + r - 1, at_x(r))

        def wait_near(kind, ref):
            for r in range(1, 4):
                wait_recv(ref, NEAR + 3 * kind + r - 1)

        pass_on(0)
        consts0 = constants(0)
        for k in NEAREST[:4]:
            pass_on(k)
        wait_recv(r1.at[pl.ds(0, 7)], PH1)
        value = recurrence(0, consts0, jnp.sum(r1[...].astype(F32), axis=0))
        gather_readout(0, value, PH2)
        for k in NEAREST[4:]:
            pass_on(k)

        pack_input_weights()
        pk[1, pl.ds(y, 1)] = wis[pl.ds(y, 1)]
        for k in FARTHEST:
            send(wis.at[lax.rem(y + k, 8)], pk.at[1, y], STWN, at_y(k))
        gb[pl.ds(d, 1)] = pack_gain()
        for k in range(1, 4):
            send(gb.at[d], gb.at[d], GAIN, at_x(k))
        pack_projection(1)
        w[1, pl.ds(x, 1), pl.ds(y, 1), 1] = ws[1, pl.ds(y, 1)][None]
        for k in FARTHEST:
            send(ws.at[1, lax.rem(y + k, 8)], w.at[1, x, y, 1], ST1N, at_y(k))

        wait_recv(r2.at[0, pl.ds(0, 7)], PH2)
        piece = unpack_readout(0)
        wait_near(0, w.at[0, 0])
        for k in range(8):
            s3[k] = project(0, piece, k)
        for k in FARTHEST:
            send(s3.at[lax.rem(z + k, 8)], r3.at[z], PH3, at_z(k))
        r3[pl.ds(z, 1)] = s3[pl.ds(z, 1)]

        wait_recv(pk.at[1, pl.ds(0, 7)], STWN)
        wait_recv(pk.at[0], STWS)
        for h in range(2):
            for j in range(4):
                rows = unfold(pk[h, j].astype(F32), pk[h, 4 + j].astype(F32)).astype(BF16)
                wi[pl.ds(x, 1), h, 32 * j : 32 * j + 32, :] = rows[None]
        near(2, wi.at[x])
        wait_recv(w.at[1, 0, pl.ds(0, 7), 1], ST1N)
        wait_recv(w.at[1, 0, pl.ds(0, 8), 0], ST1S)
        near(1, w.at[1, x])
        send(nsend.at[0], nrecv.at[0], NEW, at_x(0, 0))

        @pl.when(d != z)
        def _():
            wait_recv(rz.at[4], RES0)

        def gated(parts, residual):
            linear, gate_sum = fold_low(parts), fold_high(parts)
            return (residual + linear * (1.0 / (1.0 + jnp.exp(-gate_sum)))).astype(BF16)

        residual0 = rz[4].astype(F32)
        wait_recv(r3.at[pl.ds(0, 7)], PH3)
        own = gated(jnp.sum(r3[...].astype(F32), axis=0), residual0)
        m0[...] = own
        r4[pl.ds(z, 1)] = own[None]
        for k in FARTHEST:
            send(m0, r4.at[z], PH4, at_z(k))

        alone = jnp.logical_and(x == 0, z < 2)

        @pl.when(jnp.logical_not(alone))
        def _():
            send(m0, rz1, RES1, {"tp": lax.rem(2 * x + z, 8) * 8 + y, "dp": (z // 2) * 2 + 1})

        @pl.when(alone)
        def _():
            rz1[...] = own

        consts1 = constants(1)
        wait_recv(gb.at[pl.ds(0, 7)], GAIN)
        low1 = low_half(1)
        gains = [jnp.where(low1, gb[2 * q], roll(gb[2 * q + 1], 64)) for q in range(4)]
        wait_near(2, wi.at[0])
        win_t = jnp.concatenate(
            [unfold(wi[q, 0].astype(F32), wi[q, 1].astype(F32)).astype(BF16) for q in range(4)], axis=1
        )

        wait_recv(r4.at[pl.ds(0, 7)], PH4)
        tiles = []
        sq = jnp.zeros((64, 1), F32)
        for q in range(4):
            cur = unfold(r4[2 * q].astype(F32), r4[2 * q + 1].astype(F32))
            sq = sq + jnp.sum(cur * cur, axis=1, keepdims=True)
            tiles.append((cur * gains[q]).astype(BF16))
        part = lax.dot_general(jnp.concatenate(tiles, axis=1), win_t, NT, preferred_element_type=F32)
        squares = [rows4(sq[32 * h : 32 * h + 32]) for h in range(2)]
        for q in range(2):
            for j in range(4):
                packed = []
                for h in range(2):
                    rows = [part[32 * h + 8 * i : 32 * h + 8 * i + 8, 128 * q : 128 * q + 128] for i in range(4)]
                    packed.append(pick4([roll(rows[i], 32 * (i - j)) for i in range(4)], group8))
                s5[4 * q + j] = jnp.concatenate(packed + squares, axis=0).astype(BF16)
        for k in FARTHEST:
            send(s5.at[lax.rem(y + k, 8)], r5.at[y], PH5, at_y(k))
        r5[pl.ds(y, 1)] = s5[pl.ds(y, 1)]
        wait_recv(r5.at[pl.ds(0, 7)], PH5)
        value = recurrence(1, consts1, jnp.sum(r5[...].astype(F32), axis=0))
        gather_readout(1, value, PH6)
        send(nsend.at[1], nrecv.at[1], NEW, at_x(0, 0))
        wait_near(1, w.at[1, 0])

        @pl.when(jnp.logical_not(alone))
        def _():
            wait_recv(rz1, RES1)

        wait_recv(r2.at[1, pl.ds(0, 7)], PH6)
        piece = unpack_readout(1)
        for k in range(8):
            s7[k] = project(1, piece, k)
        for k in (4, 5, 2, 3, 6, 7, 0, 1):
            to = lax.rem(2 * x + k, 8)
            zz = lax.rem(2 * x + to, 8)
            dev = {"tp": zz * 8 + y, "dp": (to // 2) * 2 + 1}
            if k > 1:
                send(s7.at[to], r7.at[z], PH7, dev)
            else:

                @pl.when(z != zz)
                def _(to=to, dev=dev):
                    send(s7.at[to], r7.at[z], PH7, dev)

                @pl.when(z == zz)
                def _(to=to):
                    r7[pl.ds(z, 1)] = s7[pl.ds(to, 1)]

        wait_sent(s1.at[pl.ds(0, 3)], PH1)
        for k in range(1, 8):
            wait_sent(ws.at[0, 0], FARN + k)
        for r in range(3):
            wait_sent(w.at[0, 0], NEAR + r)
            wait_sent(w.at[1, 0], NEAR + 3 + r)
            wait_sent(wi.at[0], NEAR + 6 + r)
        wait_sent(gb.at[pl.ds(0, 3)], GAIN)
        wait_sent(wis.at[pl.ds(0, 7)], STWN)
        wait_sent(ws.at[1, pl.ds(0, 7)], ST1N)
        wait_sent(r2.at[0, pl.ds(0, 7)], PH2)
        wait_sent(r2.at[1, pl.ds(0, 7)], PH6)
        wait_sent(s3.at[pl.ds(0, 7)], PH3)
        wait_sent(r4.at[pl.ds(0, 7)], PH4)
        wait_sent(s5.at[pl.ds(0, 7)], PH5)
        wait_sent(nsend, NEW)

        @pl.when(d == z)
        def _():
            wait_sent(rz.at[pl.ds(0, 3)], RES0)

        @pl.when(jnp.logical_not(alone))
        def _():
            wait_sent(m0, RES1)

        keeps = jnp.logical_or(z == lax.rem(4 * x, 8), z == lax.rem(4 * x + 1, 8))

        @pl.when(keeps)
        def _():
            wait_recv(r7.at[pl.ds(0, 7)], PH7)

        @pl.when(jnp.logical_not(keeps))
        def _():
            wait_recv(r7, PH7)

        own = gated(jnp.sum(r7[...].astype(F32), axis=0), rz1[...].astype(F32))

        odd = lax.rem(y + z, 2)
        core_a = 2 * x + lax.rem(y, 2)
        core_b = 2 * x + lax.rem(z, 2)

        def forward_a(zz):
            block = oa.at[y, zz // 2]
            for k in FARTHEST:
                send(block, block, PH9A, at_y(k, core_a))

            @pl.when(lax.rem(y, 2) == 0)
            def _():
                send(block, block, PH9A, at_x(0, 0))

        def forward_b(yy):
            block = ob.at[z, yy // 2]
            for k in FARTHEST:
                send(block, block, PH9B, at_z(k, core_b))

            @pl.when(lax.rem(z, 2) == 0)
            def _():
                send(block, block, PH9B, at_x(0, 0))

        def from_z(k):
            zz = lax.rem(z + 8 - k, 8)
            wait_recv(oa.at[y, zz // 2], LASTZ + k)
            forward_a(zz)

        def from_y(k):
            yy = lax.rem(y + 8 - k, 8)
            wait_recv(ob.at[z, yy // 2], LASTY + k)
            forward_b(yy)

        @pl.when(odd == 0)
        def _():
            oa[pl.ds(y, 1), pl.ds(z // 2, 1)] = own[None, None]
            for k in FARTHEST:
                send(oa.at[y, z // 2], oa.at[y, z // 2], LASTZ + k, at_z(k))
            forward_a(z)
            for k in NEAREST:
                (from_z if k % 2 == 0 else from_y)(k)

        @pl.when(odd == 1)
        def _():
            ob[pl.ds(z, 1), pl.ds(y // 2, 1)] = own[None, None]
            for k in FARTHEST:
                send(ob.at[z, y // 2], ob.at[z, y // 2], LASTY + k, at_y(k))
            forward_b(y)
            for k in NEAREST:
                (from_y if k % 2 == 0 else from_z)(k)

        def last_waits(buffer, sem, parity):
            @pl.when(parity == 0)
            def _():
                wait_recv(buffer.at[pl.ds(0, 4)], sem)

            @pl.when(parity == 1)
            def _():
                wait_recv(buffer.at[pl.ds(0, 3)], sem)

        last_waits(oa, PH9A, lax.rem(y, 2))
        last_waits(ob, PH9B, lax.rem(z, 2))
        assemble(1)

        def last_sent(buffer, sem, parity):
            @pl.when(parity == 0)
            def _():
                wait_sent(buffer, sem)

            @pl.when(parity == 1)
            def _():
                wait_sent(buffer.at[pl.ds(0, 7)], sem)

        last_sent(oa, PH9A, lax.rem(y, 2))
        last_sent(ob, PH9B, lax.rem(z, 2))

        @pl.when(odd == 0)
        def _():
            for k in FARTHEST:
                wait_sent(m0, LASTZ + k)

        @pl.when(odd == 1)
        def _():
            for k in FARTHEST:
                wait_sent(m0, LASTY + k)

        @pl.when(keeps)
        def _():
            wait_sent(s7.at[pl.ds(0, 7)], PH7)

        @pl.when(jnp.logical_not(keeps))
        def _():
            wait_sent(s7, PH7)


def body(tokens, lengths, norm_gain, w_in, log_step, eig_re, eig_im, in_mat, output_matrices, skip,
         w_glu, w_gate, state):
    args = (tokens, lengths.reshape(1, 32), norm_gain, w_in.swapaxes(1, 2), log_step, eig_re, eig_im,
            in_mat.swapaxes(3, 4), output_matrices, skip, w_glu, w_gate, state)
    return pl.pallas_call(
        kernel,
        name="decode",
        out_shape=(pltpu.VMEM((256, 512), BF16), pltpu.VMEM((2, 2, 32, 128), F32)),
        in_specs=[pl.BlockSpec(memory_space=pl.ANY)] * 13,
        out_specs=(pl.BlockSpec(memory_space=pltpu.VMEM),) * 2,
        scratch_shapes=[pltpu.VMEM(a.shape, a.dtype) for a in args]
        + [
            pltpu.VMEM((4, 32, 128), BF16),
            pltpu.VMEM((8, 32, 128), BF16),
            pltpu.VMEM((2, 8, 32, 128), BF16),
            pltpu.VMEM((2, 4, 8, 2, 32, 128), BF16),
            pltpu.VMEM((8, 16, 128), BF16),
            pltpu.VMEM((2, 8, 16, 128), BF16),
            pltpu.VMEM((4, 2, 128, 128), BF16),
            pltpu.VMEM((8, 1, 128), F32),
            pltpu.VMEM((5, 32, 128), BF16),
            pltpu.VMEM((32, 128), BF16),
            pltpu.VMEM((2, 16, 128), BF16),
            pltpu.VMEM((2, 8, 16, 128), BF16),
            pltpu.VMEM((8, 64, 128), BF16),
            pltpu.VMEM((8, 64, 128), BF16),
            pltpu.VMEM((8, 32, 128), BF16),
            pltpu.VMEM((32, 128), BF16),
            pltpu.VMEM((8, 32, 128), BF16),
            pltpu.VMEM((8, 32, 128), BF16),
            pltpu.VMEM((8, 64, 128), BF16),
            pltpu.VMEM((8, 64, 128), BF16),
            pltpu.VMEM((8, 4, 32, 128), BF16),
            pltpu.VMEM((8, 4, 32, 128), BF16),
            pltpu.VMEM((2, 1, 32), F32),
            pltpu.VMEM((2, 2, 32, 128), F32),
            pltpu.VMEM((2, 2, 32, 128), F32),
            pltpu.VMEM((2, 2, 32, 128), F32),
            pltpu.SemaphoreType.DMA((13,)),
            pltpu.SemaphoreType.DMA((COUNT,)),
            pltpu.SemaphoreType.DMA((COUNT,)),
        ],
        compiler_params=pltpu.CompilerParams(collective_id=0, has_side_effects=True),
    )(*args)


def solution(mesh):
    placed = (
        P(None, "dp"),
        P("dp"),
        P(None, "dp"),
        P(None, "dp", "tp"),
        P(None, "tp"),
        P(None, "tp", None),
        P(None, "tp", None),
        P(None, None, "tp", None, None),
        P(None, None, "tp", None, None),
        P(None, "tp"),
        P(None, "tp", "dp"),
        P(None, "tp", "dp"),
        P(None, None, "dp", "tp"),
    )
    return jax.shard_map(
        body,
        mesh=mesh,
        in_specs=placed,
        out_specs=(P(None, "dp"), P(None, None, "dp", "tp")),
        check_vma=False,
    )
```

```python
import jax
import jax.numpy as jnp
from jax import lax
from jax.experimental import pallas as pl
from jax.experimental.pallas import tpu as pltpu
from jax.sharding import PartitionSpec as P

D = 4096
LEN_MAX = 4096
BLOCK_LEN = 256
NORM_EPS = 1e-06
MESH = pl.DeviceIdType.MESH
NT = (((1,), (1,)), ((), ()))
F32 = jnp.float32
BF16 = jnp.bfloat16

(PH1, RES0, PH2, ST1, STW, PH3, PH4, RES1, PH5, PH6, PH7, PH9A, PH9B, GAIN, STATE, COUNTS, NEW, NEAR, NEAR1, NEARW) = range(20)
FAR = 20
LAST = FAR + 5
RECV = LAST + 4
BULK, SMALL, READ = range(3)
SENT_ON = {NEAR: BULK, NEAR1: BULK, NEARW: BULK, NEW: BULK, STATE: READ, COUNTS: 3, PH3: SMALL, PH4: SMALL, PH5: SMALL,
           PH2: READ, PH6: READ, STW: 4, PH1: 5, GAIN: 6, RES0: 7, RES1: 8, PH7: 9, PH9A: 10, PH9B: 10}
SENT_LAST, SENT_A, SENT_B, SENT = 3, 11, 12, 13
NEAREST = ((1, 7), (2, 6), (3, 5), (4,))
FARTHEST = (4, 3, 5, 2, 6, 1, 7)


def roll(x, amount):
    amount = amount % 128
    return x if amount == 0 else pltpu.roll(x, amount, 1)


def groups4(rows):
    return lax.broadcasted_iota(jnp.int32, (rows, 128), 1) // 32


def low_half(rows):
    return lax.broadcasted_iota(jnp.int32, (rows, 128), 1) < 64


def pick4(parts, group):
    out = parts[3]
    for i in (2, 1, 0):
        out = jnp.where(group == i, parts[i], out)
    return out


def split2(x):
    hi = x.astype(BF16)
    lo = (x - hi.astype(F32)).astype(BF16)
    return hi, lo


def kernel(
    tok_h, len_h, gain_h, win_h, ls_h, er_h, ei_h, im_h, om_h, skip_h, glu_h, gate_h, st_h,
    mixed_ref, ns_ref,
    tok, lens, gain, win, ls, er, ei, im, om, skip, glu, gate, st,
    s1, r1, ws, w, wis, pk, wi, gb, rz, rz1, s2, r2, s3, r3, r4, m0, s5, r5, s7, r7, oa, ob,
    counts, st2, nsend, nrecv,
    lsem, ss, rs,
):
    tp = lax.axis_index("tp")
    d = lax.axis_index("dp")
    z = tp // 8
    y = lax.rem(tp, 8)
    x = d // 2
    core = lax.rem(d, 2)
    one = 2 * x + 1

    def at_y(k, dp=None):
        return {"tp": z * 8 + lax.rem(y + k, 8), "dp": one if dp is None else dp}

    def at_z(k, dp=None):
        return {"tp": lax.rem(z + k, 8) * 8 + y, "dp": one if dp is None else dp}

    def far(k):
        return FAR + min(k, 8 - k)

    def last(k):
        return LAST + min(k, 8 - k) - 1

    def at_x(k, c=1):
        return {"tp": tp, "dp": 2 * lax.rem(x + k, 4) + c}

    def send(src, dst, sem, dev, sent=None):
        if sent is None:
            sent = SENT_LAST if sem >= LAST else SMALL if sem >= FAR or sem == ST1 else SENT_ON[sem]
        pltpu.make_async_remote_copy(
            src_ref=src,
            dst_ref=dst,
            send_sem=ss.at[sent],
            recv_sem=rs.at[sem],
            device_id=dev,
            device_id_type=MESH,
        ).start()

    def wait_recv(ref, sem):
        with jax.named_scope(f"recv{sem}"):
            pltpu.make_async_copy(ref, ref, rs.at[sem]).wait()

    def wait_sent(ref, sem):
        pltpu.make_async_copy(ref, ref, ss.at[sem]).wait()

    def fold_low(t):
        n = t.shape[0] // 2
        return jnp.where(low_half(n), t[0:n], roll(t[n : 2 * n], 64))

    def fold_high(t):
        n = t.shape[0] // 2
        return jnp.where(low_half(n), roll(t[0:n], 64), t[n : 2 * n])

    def unfold(a, b):
        low = low_half(a.shape[0])
        return jnp.concatenate([jnp.where(low, a, roll(b, 64)), jnp.where(low, roll(a, 64), b)], axis=0)

    hbm = (tok_h, win_h, gain_h, glu_h, gate_h, len_h, st_h, ls_h, er_h, ei_h, im_h, om_h, skip_h)
    vmem = (tok, win, gain, glu, gate, lens, st, ls, er, ei, im, om, skip)
    group = (0, 0, 1, 2, 2, 3, 4, 5, 6, 7, 8, 9, 10)
    loads = [pltpu.make_async_copy(a, b, lsem.at[i]) for i, a, b in zip(group, hbm, vmem)]

    def wait_loaded(i):
        ref = (w.at[0, pl.ds(0, 4), pl.ds(0, 5)], gain, w.at[0, 0], lens, st, ls, er, ei, im, om, skip)[i]
        pltpu.make_async_copy(ref, ref, lsem.at[i]).wait()

    for copy in loads[:3]:
        copy.start()

    barrier = pltpu.get_barrier_semaphore()

    def greet(dev):
        pl.semaphore_signal(barrier, inc=1, device_id=dev, device_id_type=MESH)

    @pl.when(core == 1)
    def _():
        for k in FARTHEST:
            greet(at_y(k, 2 * x))
            greet(at_y(k))
            greet(at_z(k))
        for k in (2, 3, 1):
            greet(at_x(k, 0))
            greet(at_x(k))
        greet(at_x(0, 0))

    @pl.when(core == 0)
    def _():
        greet(at_x(0))

    for copy in loads[3:]:
        copy.start()
    group8 = groups4(8)

    def rows4(t):
        return pick4([jnp.broadcast_to(t[8 * i : 8 * i + 8], (8, 128)) for i in range(4)], group8)

    with jax.named_scope("load0"):
        wait_loaded(0)
        wait_loaded(1)
    for xx in range(4):
        t = tok[64 * xx : 64 * xx + 64, :].astype(F32)
        scaled = (t * gain[0:1, :]).astype(BF16)
        part = lax.dot_general(scaled, win[0], NT, preferred_element_type=F32)
        sq = jnp.sum(t * t, axis=1, keepdims=True)
        packed = [
            jnp.concatenate([part[32 * h + 8 * i : 32 * h + 8 * i + 8, :] for i in range(4)], axis=1)
            for h in range(2)
        ]
        spread = [rows4(sq[32 * h : 32 * h + 32]) for h in range(2)]
        s1[xx] = jnp.concatenate(packed + spread, axis=0).astype(BF16)

    wait_loaded(2)
    low32 = low_half(32)

    def pack_projection(layer):
        for q in range(4):
            g = glu[layer, :, 128 * q : 128 * q + 128].astype(F32)
            t = gate[layer, :, 128 * q : 128 * q + 128].astype(F32)
            ws[layer, 2 * q] = jnp.where(low32, g, roll(t, 64)).astype(BF16)
            ws[layer, 2 * q + 1] = jnp.where(low32, roll(g, 64), t).astype(BF16)

    pack_projection(0)

    half = lax.rem(y, 2)
    column = pl.ds(pl.multiple_of((y // 2) * 128, 128), 128)

    def pack_residual():
        for xx in range(4):
            t = tok[64 * xx : 64 * xx + 64, column].astype(F32)
            rz[xx] = fold_low(jnp.where(half == 1, roll(t, 64), t)).astype(BF16)

    def pack_input_weights():
        for q in range(4):
            t = win[1, :, 128 * q : 128 * q + 128].astype(F32)
            wis[2 * q] = fold_low(t).astype(BF16)
            wis[2 * q + 1] = fold_high(t).astype(BF16)

    def pack_gain():
        t = gain[1:2, column]
        return jnp.where(half == 1, roll(t, 64), t)[None]

    def assemble(g):
        for m in range(4):
            rows = pl.ds(pl.multiple_of((lax.rem(2 * m + g + 8 - 2 * x, 8) // 2) * 64, 64), 64)
            for q in range(4):
                a, b = (oa[2 * q, m], ob[2 * m, q]) if g == 0 else (ob[2 * m + 1, q], oa[2 * q + 1, m])
                mixed_ref[rows, 128 * q : 128 * q + 128] = unfold(a.astype(F32), b.astype(F32)).astype(BF16)

    @pl.when(core == 0)
    def _():
        with jax.named_scope("entry"):
            pl.semaphore_wait(barrier, 11)
        for k in (2, 3, 1, 0):
            send(s1.at[lax.rem(x + k, 4)], r1.at[d], PH1, at_x(k))
        for k in (0, *FARTHEST):
            send(ws.at[0, lax.rem(y + k, 8)], w.at[0, x, y, 0], far(k), at_y(k))
        wait_loaded(3)
        counts[0] = (lens[...] // BLOCK_LEN).astype(F32)
        send(counts.at[0], counts.at[0], COUNTS, at_x(0))
        wait_loaded(4)
        send(st, st2, STATE, at_x(0))

        @pl.when(d == z)
        def _():
            pack_residual()
            for k in range(4):
                send(rz.at[lax.rem(x + k, 4)], rz.at[4], RES0, at_x(k))

        pack_input_weights()
        for k in (0, *FARTHEST):
            send(wis.at[lax.rem(y + k, 8)], pk.at[0, y], STW, at_y(k))
        gb[pl.ds(d, 1)] = pack_gain()
        for k in range(4):
            send(gb.at[d], gb.at[d], GAIN, at_x(k))
        pack_projection(1)
        for k in (0, *FARTHEST):
            send(ws.at[1, lax.rem(y + k, 8)], w.at[1, x, y, 0], ST1, at_y(k))
        for i in range(5, 11):
            wait_loaded(i)

        wait_sent(s1, SENT_ON[PH1])
        wait_sent(w.at[0, 0], SMALL)
        wait_sent(counts.at[0], SENT_ON[COUNTS])
        wait_sent(st, READ)

        @pl.when(d == z)
        def _():
            wait_sent(rz.at[pl.ds(0, 4)], SENT_ON[RES0])

        wait_sent(wis, SENT_ON[STW])
        wait_sent(gb.at[pl.ds(0, 4)], SENT_ON[GAIN])

        wait_recv(nrecv, NEW)
        ns_ref[...] = nrecv[...]
        wait_recv(oa.at[pl.ds(0, 4)], PH9A)
        wait_recv(ob.at[pl.ds(0, 4)], PH9B)
        assemble(0)

    @pl.when(core == 1)
    def _():
        r1[pl.ds(d, 1)] = s1[pl.ds(x, 1)]
        w[0, pl.ds(x, 1), pl.ds(y, 1), 1] = ws[0, pl.ds(y, 1)][None]

        @pl.when(d == z)
        def _():
            pack_residual()
            rz[4] = rz[pl.ds(x, 1)][0]

        with jax.named_scope("entry"):
            pl.semaphore_wait(barrier, 18)
        for k in (2, 3, 1):
            send(s1.at[lax.rem(x + k, 4)], r1.at[d], PH1, at_x(k))
        for k in FARTHEST:
            send(ws.at[0, lax.rem(y + k, 8)], w.at[0, x, y, 1], far(k), at_y(k))

        def pass_on(*distances):
            if distances == (0,):
                wait_recv(w.at[0, x, y, 0], FAR)
            else:
                wait_recv(w.at[0, 0, pl.ds(0, len(distances))], far(distances[0]))
            for k in distances:
                block = w.at[0, x, lax.rem(y + 8 - k, 8)]
                for r in (2, 3, 1):
                    send(block, block, NEAR, at_x(r))

        @pl.when(d == z)
        def _():
            for k in (2, 3, 1):
                send(rz.at[lax.rem(x + k, 4)], rz.at[4], RES0, at_x(k))

        wait_loaded(3)
        counts[1] = (lens[...] // BLOCK_LEN).astype(F32)
        for i in range(4, 11):
            wait_loaded(i)
        wait_recv(counts.at[0], COUNTS)
        wait_recv(st2, STATE)
        eye = lax.broadcasted_iota(jnp.int32, (32, 32), 0) == lax.broadcasted_iota(jnp.int32, (32, 32), 1)
        blocks = jnp.concatenate(
            [
                jnp.sum(jnp.where(eye, jnp.broadcast_to(counts[h], (32, 32)), 0.0), axis=1, keepdims=True)
                for h in range(2)
            ],
            axis=0,
        )
        factor = 2.0 / (1.0 + blocks * (4.0 * BLOCK_LEN / LEN_MAX))

        def by_group(slabs, sign):
            zero = jnp.zeros((16, 64), F32)
            cols = []
            for c in range(2):
                top = jnp.concatenate([slabs[2 * c], zero], axis=1)
                low = jnp.concatenate([zero, slabs[2 * c + 1]], axis=1)
                both = jnp.concatenate([top, low], axis=0)
                cols.append(both if c == 0 else sign * both)
            return jnp.concatenate([jnp.concatenate(cols, axis=1)] * 4, axis=0)

        def constants(layer):
            def row(ref):
                return jnp.concatenate([ref[layer, 0:1, :], ref[layer, 1:2, :]], axis=1)

            e_re, e_im = row(er), row(ei)
            rate = jnp.exp(ls[layer : layer + 1, :])
            rate = jnp.concatenate(
                [jnp.broadcast_to(rate[:, 0:1], (1, 64)), jnp.broadcast_to(rate[:, 1:2], (1, 64))], axis=1
            )
            step = rate * factor
            magnitude = jnp.exp(e_re * step)
            turned = e_im * step
            a_re = magnitude * jnp.cos(turned)
            a_im = magnitude * jnp.sin(turned)
            modulus = e_re * e_re + e_im * e_im
            b_re = ((a_re - 1.0) * e_re + a_im * e_im) / modulus
            b_im = (a_im * e_re - (a_re - 1.0) * e_im) / modulus
            u = jnp.concatenate([st2[layer, 0], st[layer, 0]], axis=0)
            v = jnp.concatenate([st2[layer, 1], st[layer, 1]], axis=0)
            k_re = a_re * u - a_im * v
            k_im = a_re * v + a_im * u
            hi, lo = split2(by_group([im[layer, c, g] for c in range(2) for g in range(2)], 1.0))
            in_cat = jnp.concatenate([hi, lo], axis=0)
            hi, lo = split2(by_group([om[layer, c, g] for c in range(2) for g in range(2)], -1.0))
            out_cat = jnp.concatenate([hi, lo, hi], axis=1)
            direct = jnp.concatenate([skip[layer : layer + 1, :]] * 4, axis=1)
            return k_re, k_im, b_re, b_im, in_cat, out_cat, direct

        def recurrence(layer, consts, total):
            k_re, k_im, b_re, b_im, in_cat, out_cat, direct = consts
            driven = (total[0:16] * lax.rsqrt(total[16:32] / D + NORM_EPS)).astype(BF16).astype(F32)
            spread = jnp.concatenate(
                [jnp.where(group8 == i, driven[8 * h : 8 * h + 8], 0.0) for h in range(2) for i in range(4)],
                axis=0,
            ).astype(BF16)
            drive = lax.dot_general(
                jnp.concatenate([spread, spread], axis=1), in_cat, (((1,), (0,)), ((), ())),
                preferred_element_type=F32,
            )
            d_re, d_im = drive[:, 0:128], drive[:, 128:256]
            n_re = k_re + b_re * d_re - b_im * d_im
            n_im = k_im + b_re * d_im + b_im * d_re
            for part, new in ((0, n_re), (1, n_im)):
                nsend[layer, part] = new[0:32]
                ns_ref[layer, part] = new[32:64]
            hi, lo = split2(jnp.concatenate([n_re, n_im], axis=1))
            full = lax.dot_general(
                jnp.concatenate([hi, hi, lo], axis=1), out_cat, NT, preferred_element_type=F32
            )
            value = jnp.concatenate([rows4(full[32 * h : 32 * h + 32]) for h in range(2)], axis=0)
            value = value + direct * driven
            inner = 0.7978845608028654 * (value + 0.044715 * (value * value * value))
            return (value * (0.5 * (1.0 + jnp.tanh(inner)))).astype(BF16)

        def gather_readout(layer, value, sem):
            s2[layer] = value
            r2[layer, pl.ds(y, 1)] = value[None]
            for k in FARTHEST:
                send(s2.at[layer], r2.at[layer, y], sem, at_y(k))

        def unpack_readout(layer):
            got = [r2[layer, j].astype(F32) for j in range(8)]
            tiles = []
            for h in range(2):
                for i in range(4):
                    cols = []
                    for q in range(2):
                        parts = [got[4 * q + j][8 * h : 8 * h + 8] for j in range(4)]
                        cols.append(pick4([roll(parts[j], 32 * (j - i)) for j in range(4)], group8))
                    tiles.append(jnp.concatenate(cols, axis=1))
            return jnp.concatenate(tiles, axis=0).astype(BF16)

        def project(layer, piece, k):
            return jnp.dot(
                piece, w[layer, k // 2, :, k % 2].reshape(256, 128), preferred_element_type=F32
            ).astype(BF16)

        def near(sem, block):
            for r in (2, 3, 1):
                send(block, block, sem, at_x(r))

        pass_on(0)
        consts0 = constants(0)
        for distances in NEAREST[:2]:
            pass_on(*distances)
        wait_recv(r1.at[pl.ds(0, 7)], PH1)
        value = recurrence(0, consts0, jnp.sum(r1[...].astype(F32), axis=0))
        gather_readout(0, value, PH2)
        for distances in NEAREST[2:]:
            pass_on(*distances)

        pack_input_weights()
        pk[1, pl.ds(y, 1)] = wis[pl.ds(y, 1)]
        for k in FARTHEST:
            send(wis.at[lax.rem(y + k, 8)], pk.at[1, y], STW, at_y(k))
        gb[pl.ds(d, 1)] = pack_gain()
        for k in range(1, 4):
            send(gb.at[d], gb.at[d], GAIN, at_x(k))
        pack_projection(1)
        w[1, pl.ds(x, 1), pl.ds(y, 1), 1] = ws[1, pl.ds(y, 1)][None]
        for k in FARTHEST:
            send(ws.at[1, lax.rem(y + k, 8)], w.at[1, x, y, 1], ST1, at_y(k))

        wait_recv(r2.at[0, pl.ds(0, 7)], PH2)
        piece = unpack_readout(0)
        wait_recv(w.at[0, pl.ds(0, 3)], NEAR)
        for k in range(8):
            s3[k] = project(0, piece, k)
        for k in FARTHEST:
            send(s3.at[lax.rem(z + k, 8)], r3.at[z], PH3, at_z(k))
        r3[pl.ds(z, 1)] = s3[pl.ds(z, 1)]

        wait_recv(w.at[0, pl.ds(0, 3), pl.ds(0, 5), 0, pl.ds(0, 16)], STW)
        for h in range(2):
            for j in range(4):
                rows = unfold(pk[h, j].astype(F32), pk[h, 4 + j].astype(F32)).astype(BF16)
                wi[pl.ds(x, 1), h, 32 * j : 32 * j + 32, :] = rows[None]
        near(NEARW, wi.at[x])
        wait_recv(w.at[0, pl.ds(0, 3), pl.ds(0, 5), 0], ST1)
        near(NEAR1, w.at[1, x])
        send(nsend.at[0], nrecv.at[0], NEW, at_x(0, 0))

        @pl.when(d != z)
        def _():
            wait_recv(rz.at[4], RES0)

        def gated(parts, residual):
            linear, gate_sum = fold_low(parts), fold_high(parts)
            return (residual + linear * (1.0 / (1.0 + jnp.exp(-gate_sum)))).astype(BF16)

        residual0 = rz[4].astype(F32)
        wait_recv(r3.at[pl.ds(0, 7)], PH3)
        own = gated(jnp.sum(r3[...].astype(F32), axis=0), residual0)
        m0[...] = own
        r4[pl.ds(z, 1)] = own[None]
        for k in FARTHEST:
            send(m0, r4.at[z], PH4, at_z(k))

        alone = jnp.logical_and(x == 0, z < 2)

        @pl.when(jnp.logical_not(alone))
        def _():
            send(m0, rz1, RES1, {"tp": lax.rem(2 * x + z, 8) * 8 + y, "dp": (z // 2) * 2 + 1})

        @pl.when(alone)
        def _():
            rz1[...] = own

        consts1 = constants(1)
        wait_recv(gb.at[pl.ds(0, 7)], GAIN)
        low1 = low_half(1)
        gains = [jnp.where(low1, gb[2 * q], roll(gb[2 * q + 1], 64)) for q in range(4)]
        wait_recv(wi.at[pl.ds(0, 3)], NEARW)
        win_t = jnp.concatenate(
            [unfold(wi[q, 0].astype(F32), wi[q, 1].astype(F32)).astype(BF16) for q in range(4)], axis=1
        )

        wait_recv(r4.at[pl.ds(0, 7)], PH4)
        tiles = []
        sq = jnp.zeros((64, 1), F32)
        for q in range(4):
            cur = unfold(r4[2 * q].astype(F32), r4[2 * q + 1].astype(F32))
            sq = sq + jnp.sum(cur * cur, axis=1, keepdims=True)
            tiles.append((cur * gains[q]).astype(BF16))
        part = lax.dot_general(jnp.concatenate(tiles, axis=1), win_t, NT, preferred_element_type=F32)
        squares = [rows4(sq[32 * h : 32 * h + 32]) for h in range(2)]
        for q in range(2):
            for j in range(4):
                packed = []
                for h in range(2):
                    rows = [part[32 * h + 8 * i : 32 * h + 8 * i + 8, 128 * q : 128 * q + 128] for i in range(4)]
                    packed.append(pick4([roll(rows[i], 32 * (i - j)) for i in range(4)], group8))
                s5[4 * q + j] = jnp.concatenate(packed + squares, axis=0).astype(BF16)
        for k in FARTHEST:
            send(s5.at[lax.rem(y + k, 8)], r5.at[y], PH5, at_y(k))
        r5[pl.ds(y, 1)] = s5[pl.ds(y, 1)]
        wait_recv(r5.at[pl.ds(0, 7)], PH5)
        value = recurrence(1, consts1, jnp.sum(r5[...].astype(F32), axis=0))
        gather_readout(1, value, PH6)
        send(nsend.at[1], nrecv.at[1], NEW, at_x(0, 0))
        wait_recv(w.at[1, pl.ds(0, 3)], NEAR1)

        @pl.when(jnp.logical_not(alone))
        def _():
            wait_recv(rz1, RES1)

        wait_recv(r2.at[1, pl.ds(0, 7)], PH6)
        piece = unpack_readout(1)
        for k in range(8):
            s7[k] = project(1, piece, k)
        for k in (4, 5, 2, 3, 6, 7, 0, 1):
            to = lax.rem(2 * x + k, 8)
            zz = lax.rem(2 * x + to, 8)
            dev = {"tp": zz * 8 + y, "dp": (to // 2) * 2 + 1}
            if k > 1:
                send(s7.at[to], r7.at[z], PH7, dev)
            else:

                @pl.when(z != zz)
                def _(to=to, dev=dev):
                    send(s7.at[to], r7.at[z], PH7, dev)

                @pl.when(z == zz)
                def _(to=to):
                    r7[pl.ds(z, 1)] = s7[pl.ds(to, 1)]

        wait_sent(s1.at[pl.ds(0, 3)], SENT_ON[PH1])
        wait_sent(w, BULK)
        wait_sent(w.at[0, pl.ds(0, 3), pl.ds(0, 7)], SMALL)
        wait_sent(r4.at[pl.ds(0, 7)], READ)
        wait_sent(gb.at[pl.ds(0, 3)], SENT_ON[GAIN])
        wait_sent(wis.at[pl.ds(0, 7)], SENT_ON[STW])

        @pl.when(d == z)
        def _():
            wait_sent(rz.at[pl.ds(0, 3)], SENT_ON[RES0])

        @pl.when(jnp.logical_not(alone))
        def _():
            wait_sent(m0, SENT_ON[RES1])

        keeps = jnp.logical_or(z == lax.rem(4 * x, 8), z == lax.rem(4 * x + 1, 8))

        @pl.when(keeps)
        def _():
            wait_recv(r7.at[pl.ds(0, 7)], PH7)

        @pl.when(jnp.logical_not(keeps))
        def _():
            wait_recv(r7, PH7)

        own = gated(jnp.sum(r7[...].astype(F32), axis=0), rz1[...].astype(F32))

        odd = lax.rem(y + z, 2)
        core_a = 2 * x + lax.rem(y, 2)
        core_b = 2 * x + lax.rem(z, 2)

        def forward_a(zz):
            block = oa.at[y, zz // 2]
            for k in FARTHEST:
                send(block, block, PH9A, at_y(k, core_a))

            @pl.when(lax.rem(y, 2) == 0)
            def _():
                send(block, block, PH9A, at_x(0, 0), SENT_A)

        def forward_b(yy):
            block = ob.at[z, yy // 2]
            for k in FARTHEST:
                send(block, block, PH9B, at_z(k, core_b))

            @pl.when(lax.rem(z, 2) == 0)
            def _():
                send(block, block, PH9B, at_x(0, 0), SENT_B)

        def from_z(distances):
            wait_recv(r4.at[pl.ds(0, len(distances))], last(distances[0]))
            for k in distances:
                forward_a(lax.rem(z + 8 - k, 8))

        def from_y(distances):
            wait_recv(r4.at[pl.ds(0, len(distances))], last(distances[0]))
            for k in distances:
                forward_b(lax.rem(y + 8 - k, 8))

        @pl.when(odd == 0)
        def _():
            block = oa.at[y, z // 2]
            oa[pl.ds(y, 1), pl.ds(z // 2, 1)] = own[None, None]
            for k in FARTHEST:
                send(block, block, last(k), at_z(k))
            forward_a(z)
            for distances in NEAREST:
                (from_z if distances[0] % 2 == 0 else from_y)(distances)

        @pl.when(odd == 1)
        def _():
            block = ob.at[z, y // 2]
            ob[pl.ds(z, 1), pl.ds(y // 2, 1)] = own[None, None]
            for k in FARTHEST:
                send(block, block, last(k), at_y(k))
            forward_b(y)
            for distances in NEAREST:
                (from_y if distances[0] % 2 == 0 else from_z)(distances)

        def last_waits(buffer, sem, parity):
            @pl.when(parity == 0)
            def _():
                wait_recv(buffer.at[pl.ds(0, 4)], sem)

            @pl.when(parity == 1)
            def _():
                wait_recv(buffer.at[pl.ds(0, 3)], sem)

        last_waits(oa, PH9A, lax.rem(y, 2))
        last_waits(ob, PH9B, lax.rem(z, 2))
        with jax.named_scope("assemble"):
            assemble(1)

        with jax.named_scope("sent"):
            wait_sent(w.at[0, pl.ds(0, 4), pl.ds(0, 7)], SENT_ON[PH9A])

            @pl.when(lax.rem(y, 2) == 0)
            def _():
                wait_sent(oa.at[0], SENT_A)

            @pl.when(lax.rem(z, 2) == 0)
            def _():
                wait_sent(ob.at[0], SENT_B)

        wait_sent(r4.at[pl.ds(0, 7)], SENT_LAST)

        @pl.when(keeps)
        def _():
            wait_sent(s7.at[pl.ds(0, 7)], SENT_ON[PH7])

        @pl.when(jnp.logical_not(keeps))
        def _():
            wait_sent(s7, SENT_ON[PH7])


def hand_over(mixed, state, mixed_h, state_h, sems):
    copies = [
        pltpu.make_async_copy(mixed, mixed_h, sems.at[0]),
        pltpu.make_async_copy(state, state_h, sems.at[1]),
    ]
    for copy in copies:
        copy.start()
    for copy in copies:
        copy.wait()


def body(tokens, lengths, norm_gain, w_in, log_step, eig_re, eig_im, in_mat, output_matrices, skip,
         w_glu, w_gate, state):
    args = (tokens, lengths.reshape(1, 32), norm_gain, w_in.swapaxes(1, 2), log_step, eig_re, eig_im,
            in_mat.swapaxes(3, 4), output_matrices, skip, w_glu, w_gate, state)
    mixed, new_state = pl.pallas_call(
        kernel,
        name="decode",
        out_shape=(pltpu.VMEM((256, 512), BF16), pltpu.VMEM((2, 2, 32, 128), F32)),
        in_specs=[pl.BlockSpec(memory_space=pl.ANY)] * 13,
        out_specs=(pl.BlockSpec(memory_space=pltpu.VMEM),) * 2,
        scratch_shapes=[pltpu.VMEM(a.shape, a.dtype) for a in args]
        + [
            pltpu.VMEM((4, 32, 128), BF16),
            pltpu.VMEM((8, 32, 128), BF16),
            pltpu.VMEM((2, 8, 32, 128), BF16),
            pltpu.VMEM((2, 4, 8, 2, 32, 128), BF16),
            pltpu.VMEM((8, 16, 128), BF16),
            pltpu.VMEM((2, 8, 16, 128), BF16),
            pltpu.VMEM((4, 2, 128, 128), BF16),
            pltpu.VMEM((8, 1, 128), F32),
            pltpu.VMEM((5, 32, 128), BF16),
            pltpu.VMEM((32, 128), BF16),
            pltpu.VMEM((2, 16, 128), BF16),
            pltpu.VMEM((2, 8, 16, 128), BF16),
            pltpu.VMEM((8, 64, 128), BF16),
            pltpu.VMEM((8, 64, 128), BF16),
            pltpu.VMEM((8, 32, 128), BF16),
            pltpu.VMEM((32, 128), BF16),
            pltpu.VMEM((8, 32, 128), BF16),
            pltpu.VMEM((8, 32, 128), BF16),
            pltpu.VMEM((8, 64, 128), BF16),
            pltpu.VMEM((8, 64, 128), BF16),
            pltpu.VMEM((8, 4, 32, 128), BF16),
            pltpu.VMEM((8, 4, 32, 128), BF16),
            pltpu.VMEM((2, 1, 32), F32),
            pltpu.VMEM((2, 2, 32, 128), F32),
            pltpu.VMEM((2, 2, 32, 128), F32),
            pltpu.VMEM((2, 2, 32, 128), F32),
            pltpu.SemaphoreType.DMA((11,)),
            pltpu.SemaphoreType.DMA((SENT,)),
            pltpu.SemaphoreType.DMA((RECV,)),
        ],
        compiler_params=pltpu.CompilerParams(collective_id=0, has_side_effects=True),
    )(*args)
    inside = [pltpu.with_memory_space_constraint(a, pltpu.VMEM) for a in (mixed, new_state)]
    return pl.pallas_call(
        hand_over,
        name="hand_over",
        out_shape=(jax.ShapeDtypeStruct((256, 512), BF16), jax.ShapeDtypeStruct((2, 2, 32, 128), F32)),
        in_specs=[pl.BlockSpec(memory_space=pltpu.VMEM)] * 2,
        out_specs=(pl.BlockSpec(memory_space=pl.ANY),) * 2,
        scratch_shapes=[pltpu.SemaphoreType.DMA((2,))],
    )(*inside)


def solution(mesh):
    placed = (
        P(None, "dp"),
        P("dp"),
        P(None, "dp"),
        P(None, "dp", "tp"),
        P(None, "tp"),
        P(None, "tp", None),
        P(None, "tp", None),
        P(None, None, "tp", None, None),
        P(None, None, "tp", None, None),
        P(None, "tp"),
        P(None, "tp", "dp"),
        P(None, "tp", "dp"),
        P(None, None, "dp", "tp"),
    )
    return jax.shard_map(
        body,
        mesh=mesh,
        in_specs=placed,
        out_specs=(P(None, "dp"), P(None, None, "dp", "tp")),
        check_vma=False,
    )
```

```python
import jax
import jax.numpy as jnp
from jax import lax
from jax.experimental import pallas as pl
from jax.experimental.pallas import tpu as pltpu
from jax.sharding import PartitionSpec as P

D = 4096
LEN_MAX = 4096
BLOCK_LEN = 256
NORM_EPS = 1e-06
MESH = pl.DeviceIdType.MESH
NT = (((1,), (1,)), ((), ()))
F32 = jnp.float32
BF16 = jnp.bfloat16

(PH1, RES0, PH2, ST1, STW, PH3, PH4, RES1, PH5, PH6, PH7, PH9A, PH9B, GAIN, STATE, COUNTS, NEW, NEAR, NEAR1, NEARW) = range(20)
FAR = 20
LAST = FAR + 5
RECV = LAST + 4
BULK, SMALL, READ = range(3)
SENT_ON = {NEAR: BULK, NEAR1: BULK, NEARW: BULK, NEW: BULK, STATE: READ, COUNTS: 3, PH3: SMALL, PH4: SMALL, PH5: SMALL,
           PH2: READ, PH6: READ, STW: 4, PH1: 5, GAIN: 6, RES0: 7, RES1: 8, PH7: 9, PH9A: 10, PH9B: 10}
SENT_LAST, SENT_A, SENT_B, SENT = 3, 11, 12, 13
NEAREST = ((1, 7), (2, 6), (3, 5), (4,))
FARTHEST = (4, 3, 5, 2, 6, 1, 7)


def roll(x, amount):
    amount = amount % 128
    return x if amount == 0 else pltpu.roll(x, amount, 1)


def groups4(rows):
    return lax.broadcasted_iota(jnp.int32, (rows, 128), 1) // 32


def low_half(rows):
    return lax.broadcasted_iota(jnp.int32, (rows, 128), 1) < 64


def pick4(parts, group):
    out = parts[3]
    for i in (2, 1, 0):
        out = jnp.where(group == i, parts[i], out)
    return out


def split2(x):
    hi = x.astype(BF16)
    lo = (x - hi.astype(F32)).astype(BF16)
    return hi, lo


def kernel(
    tok_h, len_h, gain_h, win_h, ls_h, er_h, ei_h, im_h, om_h, skip_h, glu_h, gate_h, st_h,
    mixed_ref, ns_ref,
    tok, lens, gain, win, ls, er, ei, im, om, skip, glu, gate, st,
    s1, r1, ws, w, wis, pk, wi, gb, rz, rz1, s2, r2, s3, r3, r4, m0, s5, r5, s7, r7, oa, ob,
    counts, st2, nsend, nrecv,
    lsem, ss, rs,
):
    tp = lax.axis_index("tp")
    d = lax.axis_index("dp")
    z = tp // 8
    y = lax.rem(tp, 8)
    x = d // 2
    core = lax.rem(d, 2)
    one = 2 * x + 1

    def at_y(k, dp=None):
        return {"tp": z * 8 + lax.rem(y + k, 8), "dp": one if dp is None else dp}

    def at_z(k, dp=None):
        return {"tp": lax.rem(z + k, 8) * 8 + y, "dp": one if dp is None else dp}

    def far(k):
        return FAR + min(k, 8 - k)

    def last(k):
        return LAST + min(k, 8 - k) - 1

    def at_x(k, c=1):
        return {"tp": tp, "dp": 2 * lax.rem(x + k, 4) + c}

    def send(src, dst, sem, dev, sent=None):
        if sent is None:
            sent = SENT_LAST if sem >= LAST else SMALL if sem >= FAR or sem == ST1 else SENT_ON[sem]
        pltpu.make_async_remote_copy(
            src_ref=src,
            dst_ref=dst,
            send_sem=ss.at[sent],
            recv_sem=rs.at[sem],
            device_id=dev,
            device_id_type=MESH,
        ).start()

    def wait_recv(ref, sem):
        with jax.named_scope(f"recv{sem}"):
            pltpu.make_async_copy(ref, ref, rs.at[sem]).wait()

    def wait_sent(ref, sem):
        pltpu.make_async_copy(ref, ref, ss.at[sem]).wait()

    def fold_low(t):
        n = t.shape[0] // 2
        return jnp.where(low_half(n), t[0:n], roll(t[n : 2 * n], 64))

    def fold_high(t):
        n = t.shape[0] // 2
        return jnp.where(low_half(n), roll(t[0:n], 64), t[n : 2 * n])

    def unfold(a, b):
        low = low_half(a.shape[0])
        return jnp.concatenate([jnp.where(low, a, roll(b, 64)), jnp.where(low, roll(a, 64), b)], axis=0)

    hbm = (tok_h, win_h, gain_h, glu_h, gate_h, len_h, st_h, ls_h, er_h, ei_h, im_h, om_h, skip_h)
    vmem = (tok, win, gain, glu, gate, lens, st, ls, er, ei, im, om, skip)
    group = (0, 0, 1, 2, 2, 3, 4, 5, 6, 7, 8, 9, 10)
    loads = [pltpu.make_async_copy(a, b, lsem.at[i]) for i, a, b in zip(group, hbm, vmem)]

    def wait_loaded(i):
        ref = (w.at[0, pl.ds(0, 4), pl.ds(0, 5)], gain, w.at[0, 0], lens, st, ls, er, ei, im, om, skip)[i]
        pltpu.make_async_copy(ref, ref, lsem.at[i]).wait()

    for copy in loads[:3]:
        copy.start()

    barrier = pltpu.get_barrier_semaphore()

    def greet(dev):
        pl.semaphore_signal(barrier, inc=1, device_id=dev, device_id_type=MESH)

    @pl.when(core == 1)
    def _():
        for k in FARTHEST:
            greet(at_y(k))
            greet(at_y(k, 2 * x))
        for k in FARTHEST:
            greet(at_z(k))
        for k in (2, 3, 1):
            greet(at_x(k, 0))
            greet(at_x(k))
        greet(at_x(0, 0))

    @pl.when(core == 0)
    def _():
        greet(at_x(0))

    for copy in loads[3:]:
        copy.start()
    group8 = groups4(8)

    def rows4(t):
        return pick4([jnp.broadcast_to(t[8 * i : 8 * i + 8], (8, 128)) for i in range(4)], group8)

    with jax.named_scope("load0"):
        wait_loaded(0)
        wait_loaded(1)
    for xx in range(4):
        t = tok[64 * xx : 64 * xx + 64, :].astype(F32)
        scaled = (t * gain[0:1, :]).astype(BF16)
        part = lax.dot_general(scaled, win[0], NT, preferred_element_type=F32)
        sq = jnp.sum(t * t, axis=1, keepdims=True)
        packed = [
            jnp.concatenate([part[32 * h + 8 * i : 32 * h + 8 * i + 8, :] for i in range(4)], axis=1)
            for h in range(2)
        ]
        spread = [rows4(sq[32 * h : 32 * h + 32]) for h in range(2)]
        s1[xx] = jnp.concatenate(packed + spread, axis=0).astype(BF16)

    wait_loaded(2)
    low32 = low_half(32)

    def pack_projection(layer):
        for q in range(4):
            g = glu[layer, :, 128 * q : 128 * q + 128].astype(F32)
            t = gate[layer, :, 128 * q : 128 * q + 128].astype(F32)
            ws[layer, 2 * q] = jnp.where(low32, g, roll(t, 64)).astype(BF16)
            ws[layer, 2 * q + 1] = jnp.where(low32, roll(g, 64), t).astype(BF16)

    pack_projection(0)

    half = lax.rem(y, 2)
    column = pl.ds(pl.multiple_of((y // 2) * 128, 128), 128)

    def pack_residual():
        for xx in range(4):
            t = tok[64 * xx : 64 * xx + 64, column].astype(F32)
            rz[xx] = fold_low(jnp.where(half == 1, roll(t, 64), t)).astype(BF16)

    def pack_input_weights():
        for q in range(4):
            t = win[1, :, 128 * q : 128 * q + 128].astype(F32)
            wis[2 * q] = fold_low(t).astype(BF16)
            wis[2 * q + 1] = fold_high(t).astype(BF16)

    def pack_gain():
        t = gain[1:2, column]
        return jnp.where(half == 1, roll(t, 64), t)[None]

    def assemble(g):
        for m in range(4):
            rows = pl.ds(pl.multiple_of((lax.rem(2 * m + g + 8 - 2 * x, 8) // 2) * 64, 64), 64)
            for q in range(4):
                a, b = (oa[2 * q, m], ob[2 * m, q]) if g == 0 else (ob[2 * m + 1, q], oa[2 * q + 1, m])
                mixed_ref[rows, 128 * q : 128 * q + 128] = unfold(a.astype(F32), b.astype(F32)).astype(BF16)

    @pl.when(core == 0)
    def _():
        with jax.named_scope("entry"):
            pl.semaphore_wait(barrier, 11)
        for k in (2, 3, 1, 0):
            send(s1.at[lax.rem(x + k, 4)], r1.at[d], PH1, at_x(k))
        for k in (0, *FARTHEST):
            send(ws.at[0, lax.rem(y + k, 8)], w.at[0, x, y, 0], far(k), at_y(k))
        wait_loaded(3)
        counts[0] = (lens[...] // BLOCK_LEN).astype(F32)
        send(counts.at[0], counts.at[0], COUNTS, at_x(0))
        wait_loaded(4)
        send(st, st2, STATE, at_x(0))

        @pl.when(d == z)
        def _():
            pack_residual()
            for k in range(4):
                send(rz.at[lax.rem(x + k, 4)], rz.at[4], RES0, at_x(k))

        pack_input_weights()
        for k in (0, *FARTHEST):
            send(wis.at[lax.rem(y + k, 8)], pk.at[0, y], STW, at_y(k))
        gb[pl.ds(d, 1)] = pack_gain()
        for k in range(4):
            send(gb.at[d], gb.at[d], GAIN, at_x(k))
        pack_projection(1)
        for k in (0, *FARTHEST):
            send(ws.at[1, lax.rem(y + k, 8)], w.at[1, x, y, 0], ST1, at_y(k))
        for i in range(5, 11):
            wait_loaded(i)

        wait_sent(s1, SENT_ON[PH1])
        wait_sent(w.at[0, 0], SMALL)
        wait_sent(counts.at[0], SENT_ON[COUNTS])
        wait_sent(st, READ)

        @pl.when(d == z)
        def _():
            wait_sent(rz.at[pl.ds(0, 4)], SENT_ON[RES0])

        wait_sent(wis, SENT_ON[STW])
        wait_sent(gb.at[pl.ds(0, 4)], SENT_ON[GAIN])

        wait_recv(nrecv, NEW)
        ns_ref[...] = nrecv[...]
        wait_recv(oa.at[pl.ds(0, 4)], PH9A)
        wait_recv(ob.at[pl.ds(0, 4)], PH9B)
        assemble(0)

    @pl.when(core == 1)
    def _():
        r1[pl.ds(d, 1)] = s1[pl.ds(x, 1)]
        w[0, pl.ds(x, 1), pl.ds(y, 1), 1] = ws[0, pl.ds(y, 1)][None]

        @pl.when(d == z)
        def _():
            pack_residual()
            rz[4] = rz[pl.ds(x, 1)][0]

        with jax.named_scope("entry"):
            pl.semaphore_wait(barrier, 18)
        for k in (2, 3, 1):
            send(s1.at[lax.rem(x + k, 4)], r1.at[d], PH1, at_x(k))
        for k in FARTHEST:
            send(ws.at[0, lax.rem(y + k, 8)], w.at[0, x, y, 1], far(k), at_y(k))

        def pass_on(*distances):
            if distances == (0,):
                wait_recv(w.at[0, x, y, 0], FAR)
            else:
                wait_recv(w.at[0, 0, pl.ds(0, len(distances))], far(distances[0]))
            for k in distances:
                block = w.at[0, x, lax.rem(y + 8 - k, 8)]
                for r in (2, 3, 1):
                    send(block, block, NEAR, at_x(r))

        @pl.when(d == z)
        def _():
            for k in (2, 3, 1):
                send(rz.at[lax.rem(x + k, 4)], rz.at[4], RES0, at_x(k))

        wait_loaded(3)
        counts[1] = (lens[...] // BLOCK_LEN).astype(F32)
        for i in range(4, 11):
            wait_loaded(i)
        wait_recv(counts.at[0], COUNTS)
        wait_recv(st2, STATE)
        eye = lax.broadcasted_iota(jnp.int32, (32, 32), 0) == lax.broadcasted_iota(jnp.int32, (32, 32), 1)
        blocks = jnp.concatenate(
            [
                jnp.sum(jnp.where(eye, jnp.broadcast_to(counts[h], (32, 32)), 0.0), axis=1, keepdims=True)
                for h in range(2)
            ],
            axis=0,
        )
        factor = 2.0 / (1.0 + blocks * (4.0 * BLOCK_LEN / LEN_MAX))

        def by_group(slabs, sign):
            zero = jnp.zeros((16, 64), F32)
            cols = []
            for c in range(2):
                top = jnp.concatenate([slabs[2 * c], zero], axis=1)
                low = jnp.concatenate([zero, slabs[2 * c + 1]], axis=1)
                both = jnp.concatenate([top, low], axis=0)
                cols.append(both if c == 0 else sign * both)
            return jnp.concatenate([jnp.concatenate(cols, axis=1)] * 4, axis=0)

        def constants(layer):
            def row(ref):
                return jnp.concatenate([ref[layer, 0:1, :], ref[layer, 1:2, :]], axis=1)

            e_re, e_im = row(er), row(ei)
            rate = jnp.exp(ls[layer : layer + 1, :])
            rate = jnp.concatenate(
                [jnp.broadcast_to(rate[:, 0:1], (1, 64)), jnp.broadcast_to(rate[:, 1:2], (1, 64))], axis=1
            )
            step = rate * factor
            magnitude = jnp.exp(e_re * step)
            turned = e_im * step
            a_re = magnitude * jnp.cos(turned)
            a_im = magnitude * jnp.sin(turned)
            modulus = e_re * e_re + e_im * e_im
            b_re = ((a_re - 1.0) * e_re + a_im * e_im) / modulus
            b_im = (a_im * e_re - (a_re - 1.0) * e_im) / modulus
            u = jnp.concatenate([st2[layer, 0], st[layer, 0]], axis=0)
            v = jnp.concatenate([st2[layer, 1], st[layer, 1]], axis=0)
            k_re = a_re * u - a_im * v
            k_im = a_re * v + a_im * u
            hi, lo = split2(by_group([im[layer, c, g] for c in range(2) for g in range(2)], 1.0))
            in_cat = jnp.concatenate([hi, lo], axis=0)
            hi, lo = split2(by_group([om[layer, c, g] for c in range(2) for g in range(2)], -1.0).T)
            out_cat = jnp.concatenate([hi, lo, hi], axis=0)
            direct = jnp.concatenate([skip[layer : layer + 1, :]] * 4, axis=1)
            return k_re, k_im, b_re, b_im, in_cat, out_cat, direct

        def recurrence(layer, consts, total):
            k_re, k_im, b_re, b_im, in_cat, out_cat, direct = consts
            driven = (total[0:16] * lax.rsqrt(total[16:32] / D + NORM_EPS)).astype(BF16).astype(F32)
            spread = jnp.concatenate(
                [jnp.where(group8 == i, driven[8 * h : 8 * h + 8], 0.0) for h in range(2) for i in range(4)],
                axis=0,
            ).astype(BF16)
            drive = lax.dot_general(
                jnp.concatenate([spread, spread], axis=1), in_cat, (((1,), (0,)), ((), ())),
                preferred_element_type=F32,
            )
            d_re, d_im = drive[:, 0:128], drive[:, 128:256]
            n_re = k_re + b_re * d_re - b_im * d_im
            n_im = k_im + b_re * d_im + b_im * d_re
            for part, new in ((0, n_re), (1, n_im)):
                nsend[layer, part] = new[0:32]
                ns_ref[layer, part] = new[32:64]
            hi, lo = split2(jnp.concatenate([n_re, n_im], axis=1))
            full = lax.dot_general(
                jnp.concatenate([hi, hi, lo], axis=1), out_cat, (((1,), (0,)), ((), ())),
                preferred_element_type=F32,
            )
            value = jnp.concatenate([rows4(full[32 * h : 32 * h + 32]) for h in range(2)], axis=0)
            value = value + direct * driven
            inner = 0.7978845608028654 * (value + 0.044715 * (value * value * value))
            return (value * (0.5 * (1.0 + jnp.tanh(inner)))).astype(BF16)

        def gather_readout(layer, value, sem):
            s2[layer] = value
            r2[layer, pl.ds(y, 1)] = value[None]
            for k in FARTHEST:
                send(s2.at[layer], r2.at[layer, y], sem, at_y(k))

        def unpack_readout(layer):
            got = [r2[layer, j].astype(F32) for j in range(8)]
            tiles = []
            for h in range(2):
                for i in range(4):
                    cols = []
                    for q in range(2):
                        parts = [got[4 * q + j][8 * h : 8 * h + 8] for j in range(4)]
                        cols.append(pick4([roll(parts[j], 32 * (j - i)) for j in range(4)], group8))
                    tiles.append(jnp.concatenate(cols, axis=1))
            return jnp.concatenate(tiles, axis=0).astype(BF16)

        def project(layer, piece, xx, out):
            rhs = jnp.concatenate([w[layer, xx, :, h].reshape(256, 128) for h in range(2)], axis=1)
            both = jnp.dot(piece, rhs, preferred_element_type=F32).astype(BF16)
            out[2 * xx] = both[:, 0:128]
            out[2 * xx + 1] = both[:, 128:256]

        def near(sem, block):
            for r in (2, 3, 1):
                send(block, block, sem, at_x(r))

        pass_on(0)
        consts0 = constants(0)
        for distances in NEAREST[:2]:
            pass_on(*distances)
        wait_recv(r1.at[pl.ds(0, 7)], PH1)
        value = recurrence(0, consts0, jnp.sum(r1[...].astype(F32), axis=0))
        gather_readout(0, value, PH2)
        for distances in NEAREST[2:]:
            pass_on(*distances)

        pack_input_weights()
        pk[1, pl.ds(y, 1)] = wis[pl.ds(y, 1)]
        for k in FARTHEST:
            send(wis.at[lax.rem(y + k, 8)], pk.at[1, y], STW, at_y(k))
        gb[pl.ds(d, 1)] = pack_gain()
        for k in range(1, 4):
            send(gb.at[d], gb.at[d], GAIN, at_x(k))
        pack_projection(1)
        w[1, pl.ds(x, 1), pl.ds(y, 1), 1] = ws[1, pl.ds(y, 1)][None]
        for k in FARTHEST:
            send(ws.at[1, lax.rem(y + k, 8)], w.at[1, x, y, 1], ST1, at_y(k))

        wait_recv(r2.at[0, pl.ds(0, 7)], PH2)
        piece = unpack_readout(0)
        wait_recv(w.at[0, pl.ds(0, 3)], NEAR)
        for xx in range(4):
            project(0, piece, xx, s3)
        for k in FARTHEST:
            send(s3.at[lax.rem(z + k, 8)], r3.at[z], PH3, at_z(k))
        r3[pl.ds(z, 1)] = s3[pl.ds(z, 1)]

        wait_recv(w.at[0, pl.ds(0, 3), pl.ds(0, 5), 0, pl.ds(0, 16)], STW)
        for h in range(2):
            for j in range(4):
                rows = unfold(pk[h, j].astype(F32), pk[h, 4 + j].astype(F32)).astype(BF16)
                wi[pl.ds(x, 1), h, 32 * j : 32 * j + 32, :] = rows[None]
        near(NEARW, wi.at[x])
        wait_recv(w.at[0, pl.ds(0, 3), pl.ds(0, 5), 0], ST1)
        near(NEAR1, w.at[1, x])
        send(nsend.at[0], nrecv.at[0], NEW, at_x(0, 0))

        @pl.when(d != z)
        def _():
            wait_recv(rz.at[4], RES0)

        def gated(parts, residual):
            linear, gate_sum = fold_low(parts), fold_high(parts)
            return (residual + linear * (1.0 / (1.0 + jnp.exp(-gate_sum)))).astype(BF16)

        residual0 = rz[4].astype(F32)
        wait_recv(r3.at[pl.ds(0, 7)], PH3)
        own = gated(jnp.sum(r3[...].astype(F32), axis=0), residual0)
        m0[...] = own
        r4[pl.ds(z, 1)] = own[None]
        for k in FARTHEST:
            send(m0, r4.at[z], PH4, at_z(k))

        alone = jnp.logical_and(x == 0, z < 2)

        @pl.when(jnp.logical_not(alone))
        def _():
            send(m0, rz1, RES1, {"tp": lax.rem(2 * x + z, 8) * 8 + y, "dp": (z // 2) * 2 + 1})

        @pl.when(alone)
        def _():
            rz1[...] = own

        consts1 = constants(1)
        wait_recv(gb.at[pl.ds(0, 7)], GAIN)
        low1 = low_half(1)
        gains = [jnp.where(low1, gb[2 * q], roll(gb[2 * q + 1], 64)) for q in range(4)]
        wait_recv(wi.at[pl.ds(0, 3)], NEARW)
        win_t = jnp.concatenate(
            [unfold(wi[q, 0].astype(F32), wi[q, 1].astype(F32)).T.astype(BF16) for q in range(4)], axis=0
        )

        wait_recv(r4.at[pl.ds(0, 7)], PH4)
        tiles = []
        sq = jnp.zeros((64, 1), F32)
        for q in range(4):
            cur = unfold(r4[2 * q].astype(F32), r4[2 * q + 1].astype(F32))
            sq = sq + jnp.sum(cur * cur, axis=1, keepdims=True)
            tiles.append((cur * gains[q]).astype(BF16))
        part = jnp.dot(jnp.concatenate(tiles, axis=1), win_t, preferred_element_type=F32)
        squares = [rows4(sq[32 * h : 32 * h + 32]) for h in range(2)]
        for q in range(2):
            for j in range(4):
                packed = []
                for h in range(2):
                    rows = [part[32 * h + 8 * i : 32 * h + 8 * i + 8, 128 * q : 128 * q + 128] for i in range(4)]
                    packed.append(pick4([roll(rows[i], 32 * (i - j)) for i in range(4)], group8))
                s5[4 * q + j] = jnp.concatenate(packed + squares, axis=0).astype(BF16)
        for k in FARTHEST:
            send(s5.at[lax.rem(y + k, 8)], r5.at[y], PH5, at_y(k))
        r5[pl.ds(y, 1)] = s5[pl.ds(y, 1)]
        wait_recv(r5.at[pl.ds(0, 7)], PH5)
        value = recurrence(1, consts1, jnp.sum(r5[...].astype(F32), axis=0))
        gather_readout(1, value, PH6)
        send(nsend.at[1], nrecv.at[1], NEW, at_x(0, 0))
        wait_recv(w.at[1, pl.ds(0, 3)], NEAR1)

        @pl.when(jnp.logical_not(alone))
        def _():
            wait_recv(rz1, RES1)

        wait_recv(r2.at[1, pl.ds(0, 7)], PH6)
        piece = unpack_readout(1)
        for xx in range(4):
            project(1, piece, xx, s7)
        for k in (4, 5, 2, 3, 6, 7, 0, 1):
            to = lax.rem(2 * x + k, 8)
            zz = lax.rem(2 * x + to, 8)
            dev = {"tp": zz * 8 + y, "dp": (to // 2) * 2 + 1}
            if k > 1:
                send(s7.at[to], r7.at[z], PH7, dev)
            else:

                @pl.when(z != zz)
                def _(to=to, dev=dev):
                    send(s7.at[to], r7.at[z], PH7, dev)

                @pl.when(z == zz)
                def _(to=to):
                    r7[pl.ds(z, 1)] = s7[pl.ds(to, 1)]

        wait_sent(s1.at[pl.ds(0, 3)], SENT_ON[PH1])
        wait_sent(w, BULK)
        wait_sent(w.at[0, pl.ds(0, 3), pl.ds(0, 7)], SMALL)
        wait_sent(r4.at[pl.ds(0, 7)], READ)
        wait_sent(gb.at[pl.ds(0, 3)], SENT_ON[GAIN])
        wait_sent(wis.at[pl.ds(0, 7)], SENT_ON[STW])

        @pl.when(d == z)
        def _():
            wait_sent(rz.at[pl.ds(0, 3)], SENT_ON[RES0])

        @pl.when(jnp.logical_not(alone))
        def _():
            wait_sent(m0, SENT_ON[RES1])

        keeps = jnp.logical_or(z == lax.rem(4 * x, 8), z == lax.rem(4 * x + 1, 8))

        @pl.when(keeps)
        def _():
            wait_recv(r7.at[pl.ds(0, 7)], PH7)

        @pl.when(jnp.logical_not(keeps))
        def _():
            wait_recv(r7, PH7)

        own = gated(jnp.sum(r7[...].astype(F32), axis=0), rz1[...].astype(F32))

        odd = lax.rem(y + z, 2)
        core_a = 2 * x + lax.rem(y, 2)
        core_b = 2 * x + lax.rem(z, 2)

        def others(mine, serve):
            for t in (0, 1, 2, 7, 3, 6, 5, 4):

                @pl.when(mine != t)
                def _(t=t):
                    serve(t)

        def apart(a, b):
            k = lax.rem(a + 8 - b, 8)
            return jnp.minimum(k, 8 - k)

        def forward_a(zz):
            block = oa.at[y, zz // 2]
            others(y, lambda t: send(block, block, PH9A, {"tp": z * 8 + t, "dp": core_a}))

            @pl.when(lax.rem(y, 2) == 0)
            def _():
                send(block, block, PH9A, at_x(0, 0), SENT_A)

        def forward_b(yy):
            block = ob.at[z, yy // 2]
            others(z, lambda t: send(block, block, PH9B, {"tp": t * 8 + y, "dp": core_b}))

            @pl.when(lax.rem(z, 2) == 0)
            def _():
                send(block, block, PH9B, at_x(0, 0), SENT_B)

        def from_z(distances):
            wait_recv(r4.at[pl.ds(0, len(distances))], last(distances[0]))
            for k in distances:
                forward_a(lax.rem(z + 8 - k, 8))

        def from_y(distances):
            wait_recv(r4.at[pl.ds(0, len(distances))], last(distances[0]))
            for k in distances:
                forward_b(lax.rem(y + 8 - k, 8))

        @pl.when(odd == 0)
        def _():
            block = oa.at[y, z // 2]
            oa[pl.ds(y, 1), pl.ds(z // 2, 1)] = own[None, None]
            others(z, lambda t: send(block, block, LAST + apart(t, z) - 1, {"tp": t * 8 + y, "dp": one}, SENT_LAST))
            forward_a(z)
            for distances in NEAREST:
                (from_z if distances[0] % 2 == 0 else from_y)(distances)

        @pl.when(odd == 1)
        def _():
            block = ob.at[z, y // 2]
            ob[pl.ds(z, 1), pl.ds(y // 2, 1)] = own[None, None]
            others(y, lambda t: send(block, block, LAST + apart(t, y) - 1, {"tp": z * 8 + t, "dp": one}, SENT_LAST))
            forward_b(y)
            for distances in NEAREST:
                (from_y if distances[0] % 2 == 0 else from_z)(distances)

        def last_waits(buffer, sem, parity):
            @pl.when(parity == 0)
            def _():
                wait_recv(buffer.at[pl.ds(0, 4)], sem)

            @pl.when(parity == 1)
            def _():
                wait_recv(buffer.at[pl.ds(0, 3)], sem)

        last_waits(oa, PH9A, lax.rem(y, 2))
        last_waits(ob, PH9B, lax.rem(z, 2))
        with jax.named_scope("assemble"):
            assemble(1)

        with jax.named_scope("sent"):
            wait_sent(w.at[0, pl.ds(0, 4), pl.ds(0, 7)], SENT_ON[PH9A])

            @pl.when(lax.rem(y, 2) == 0)
            def _():
                wait_sent(oa.at[0], SENT_A)

            @pl.when(lax.rem(z, 2) == 0)
            def _():
                wait_sent(ob.at[0], SENT_B)

        wait_sent(r4.at[pl.ds(0, 7)], SENT_LAST)

        @pl.when(keeps)
        def _():
            wait_sent(s7.at[pl.ds(0, 7)], SENT_ON[PH7])

        @pl.when(jnp.logical_not(keeps))
        def _():
            wait_sent(s7, SENT_ON[PH7])


def hand_over(mixed, state, mixed_h, state_h, sems):
    copies = [
        pltpu.make_async_copy(mixed, mixed_h, sems.at[0]),
        pltpu.make_async_copy(state, state_h, sems.at[1]),
    ]
    for copy in copies:
        copy.start()
    for copy in copies:
        copy.wait()


def body(tokens, lengths, norm_gain, w_in, log_step, eig_re, eig_im, in_mat, output_matrices, skip,
         w_glu, w_gate, state):
    args = (tokens, lengths.reshape(1, 32), norm_gain, w_in.swapaxes(1, 2), log_step, eig_re, eig_im,
            in_mat.swapaxes(3, 4), output_matrices, skip, w_glu, w_gate, state)
    mixed, new_state = pl.pallas_call(
        kernel,
        name="decode",
        out_shape=(pltpu.VMEM((256, 512), BF16), pltpu.VMEM((2, 2, 32, 128), F32)),
        in_specs=[pl.BlockSpec(memory_space=pl.ANY)] * 13,
        out_specs=(pl.BlockSpec(memory_space=pltpu.VMEM),) * 2,
        scratch_shapes=[pltpu.VMEM(a.shape, a.dtype) for a in args]
        + [
            pltpu.VMEM((4, 32, 128), BF16),
            pltpu.VMEM((8, 32, 128), BF16),
            pltpu.VMEM((2, 8, 32, 128), BF16),
            pltpu.VMEM((2, 4, 8, 2, 32, 128), BF16),
            pltpu.VMEM((8, 16, 128), BF16),
            pltpu.VMEM((2, 8, 16, 128), BF16),
            pltpu.VMEM((4, 2, 128, 128), BF16),
            pltpu.VMEM((8, 1, 128), F32),
            pltpu.VMEM((5, 32, 128), BF16),
            pltpu.VMEM((32, 128), BF16),
            pltpu.VMEM((2, 16, 128), BF16),
            pltpu.VMEM((2, 8, 16, 128), BF16),
            pltpu.VMEM((8, 64, 128), BF16),
            pltpu.VMEM((8, 64, 128), BF16),
            pltpu.VMEM((8, 32, 128), BF16),
            pltpu.VMEM((32, 128), BF16),
            pltpu.VMEM((8, 32, 128), BF16),
            pltpu.VMEM((8, 32, 128), BF16),
            pltpu.VMEM((8, 64, 128), BF16),
            pltpu.VMEM((8, 64, 128), BF16),
            pltpu.VMEM((8, 4, 32, 128), BF16),
            pltpu.VMEM((8, 4, 32, 128), BF16),
            pltpu.VMEM((2, 1, 32), F32),
            pltpu.VMEM((2, 2, 32, 128), F32),
            pltpu.VMEM((2, 2, 32, 128), F32),
            pltpu.VMEM((2, 2, 32, 128), F32),
            pltpu.SemaphoreType.DMA((11,)),
            pltpu.SemaphoreType.DMA((SENT,)),
            pltpu.SemaphoreType.DMA((RECV,)),
        ],
        compiler_params=pltpu.CompilerParams(collective_id=0, has_side_effects=True),
    )(*args)
    inside = [pltpu.with_memory_space_constraint(a, pltpu.VMEM) for a in (mixed, new_state)]
    return pl.pallas_call(
        hand_over,
        name="hand_over",
        out_shape=(jax.ShapeDtypeStruct((256, 512), BF16), jax.ShapeDtypeStruct((2, 2, 32, 128), F32)),
        in_specs=[pl.BlockSpec(memory_space=pltpu.VMEM)] * 2,
        out_specs=(pl.BlockSpec(memory_space=pl.ANY),) * 2,
        scratch_shapes=[pltpu.SemaphoreType.DMA((2,))],
    )(*inside)


def solution(mesh):
    placed = (
        P(None, "dp"),
        P("dp"),
        P(None, "dp"),
        P(None, "dp", "tp"),
        P(None, "tp"),
        P(None, "tp", None),
        P(None, "tp", None),
        P(None, None, "tp", None, None),
        P(None, None, "tp", None, None),
        P(None, "tp"),
        P(None, "tp", "dp"),
        P(None, "tp", "dp"),
        P(None, None, "dp", "tp"),
    )
    return jax.shard_map(
        body,
        mesh=mesh,
        in_specs=placed,
        out_specs=(P(None, "dp"), P(None, None, "dp", "tp")),
        check_vma=False,
    )
```

```python
import jax
import jax.numpy as jnp
from jax import lax
from jax.experimental import pallas as pl
from jax.experimental.pallas import tpu as pltpu
from jax.sharding import PartitionSpec as P

D = 4096
LEN_MAX = 4096
BLOCK_LEN = 256
NORM_EPS = 1e-06
MESH = pl.DeviceIdType.MESH
NT = (((1,), (1,)), ((), ()))
F32 = jnp.float32
BF16 = jnp.bfloat16

(PH1, RES0, PH2, ST1, STW, PH3, PH4, RES1, PH5, PH6, PH7, PH9A, PH9B, GAIN, STATE, COUNTS, NEW, NEAR, NEAR1, NEARW) = range(20)
FAR = 20
LAST = FAR + 5
RECV = LAST + 4
BULK, SMALL, READ = range(3)
SENT_ON = {NEAR: BULK, NEAR1: BULK, NEARW: BULK, NEW: BULK, STATE: READ, COUNTS: 3, PH3: SMALL, PH4: SMALL, PH5: SMALL,
           PH2: READ, PH6: READ, STW: 4, PH1: 5, GAIN: 6, RES0: 7, RES1: 8, PH7: 9, PH9A: 10, PH9B: 10}
SENT_LAST, SENT_A, SENT_B, RELAY_A, RELAY_B, LOW, SENT = 3, 11, 12, 13, 14, 15, 17
NEAREST = ((1, 7), (2, 6), (3, 5), (4,))
FARTHEST = (4, 3, 5, 2, 6, 1, 7)


def roll(x, amount):
    amount = amount % 128
    return x if amount == 0 else pltpu.roll(x, amount, 1)


def groups4(rows):
    return lax.broadcasted_iota(jnp.int32, (rows, 128), 1) // 32


def low_half(rows):
    return lax.broadcasted_iota(jnp.int32, (rows, 128), 1) < 64


def pick4(parts, group):
    out = parts[3]
    for i in (2, 1, 0):
        out = jnp.where(group == i, parts[i], out)
    return out


def split2(x):
    hi = x.astype(BF16)
    lo = (x - hi.astype(F32)).astype(BF16)
    return hi, lo


def kernel(
    tok_h, len_h, gain_h, win_h, ls_h, er_h, ei_h, im_h, om_h, skip_h, glu_h, gate_h, st_h,
    mixed_ref, ns_ref,
    tok, lens, gain, win, ls, er, ei, im, om, skip, glu, gate, st,
    s1, r1, ws, w, wis, pk, wi, gb, rz, rz1, s2, r2, s3, r3, r4, m0, s5, r5, s7, r7, oa, ob,
    counts, st2, nsend, nrecv,
    lsem, ss, rs,
):
    tp = lax.axis_index("tp")
    d = lax.axis_index("dp")
    z = tp // 8
    y = lax.rem(tp, 8)
    x = d // 2
    core = lax.rem(d, 2)
    one = 2 * x + 1

    def at_y(k, dp=None):
        return {"tp": z * 8 + lax.rem(y + k, 8), "dp": one if dp is None else dp}

    def at_z(k, dp=None):
        return {"tp": lax.rem(z + k, 8) * 8 + y, "dp": one if dp is None else dp}

    def far(k):
        return FAR + min(k, 8 - k)

    def last(k):
        return LAST + min(k, 8 - k) - 1

    def at_x(k, c=1):
        return {"tp": tp, "dp": 2 * lax.rem(x + k, 4) + c}

    def send(src, dst, sem, dev, sent=None):
        if sent is None:
            sent = SENT_LAST if sem >= LAST else SMALL if sem >= FAR or sem == ST1 else SENT_ON[sem]
        pltpu.make_async_remote_copy(
            src_ref=src,
            dst_ref=dst,
            send_sem=ss.at[sent],
            recv_sem=rs.at[sem],
            device_id=dev,
            device_id_type=MESH,
        ).start()

    def wait_recv(ref, sem):
        with jax.named_scope(f"recv{sem}"):
            pltpu.make_async_copy(ref, ref, rs.at[sem]).wait()

    def wait_sent(ref, sem):
        pltpu.make_async_copy(ref, ref, ss.at[sem]).wait()

    def fold_low(t):
        n = t.shape[0] // 2
        return jnp.where(low_half(n), t[0:n], roll(t[n : 2 * n], 64))

    def fold_high(t):
        n = t.shape[0] // 2
        return jnp.where(low_half(n), roll(t[0:n], 64), t[n : 2 * n])

    def unfold(a, b):
        low = low_half(a.shape[0])
        return jnp.concatenate([jnp.where(low, a, roll(b, 64)), jnp.where(low, roll(a, 64), b)], axis=0)

    hbm = (tok_h, win_h, gain_h, glu_h, gate_h, len_h, st_h, ls_h, er_h, ei_h, im_h, om_h, skip_h)
    vmem = (tok, win, gain, glu, gate, lens, st, ls, er, ei, im, om, skip)
    group = (0, 0, 1, 2, 2, 3, 4, 5, 6, 7, 8, 9, 10)
    loads = [pltpu.make_async_copy(a, b, lsem.at[i]) for i, a, b in zip(group, hbm, vmem)]

    def wait_loaded(i):
        ref = (w.at[0, pl.ds(0, 4), pl.ds(0, 5)], gain, w.at[0, 0], lens, st, ls, er, ei, im, om, skip)[i]
        pltpu.make_async_copy(ref, ref, lsem.at[i]).wait()

    for copy in loads[:3]:
        copy.start()

    barrier = pltpu.get_barrier_semaphore()

    def greet(dev):
        pl.semaphore_signal(barrier, inc=1, device_id=dev, device_id_type=MESH)

    @pl.when(core == 1)
    def _():
        for k in FARTHEST:
            greet(at_y(k))
            greet(at_y(k, 2 * x))
        for k in FARTHEST:
            greet(at_z(k))
        for k in (2, 3, 1):
            greet(at_x(k, 0))
            greet(at_x(k))
        greet(at_x(0, 0))

    @pl.when(core == 0)
    def _():
        greet(at_x(0))

    for copy in loads[3:]:
        copy.start()
    group8 = groups4(8)

    def rows4(t):
        return pick4([jnp.broadcast_to(t[8 * i : 8 * i + 8], (8, 128)) for i in range(4)], group8)

    with jax.named_scope("load0"):
        wait_loaded(0)
        wait_loaded(1)
    for xx in range(4):
        t = tok[64 * xx : 64 * xx + 64, :].astype(F32)
        scaled = (t * gain[0:1, :]).astype(BF16)
        part = lax.dot_general(scaled, win[0], NT, preferred_element_type=F32)
        sq = jnp.sum(t * t, axis=1, keepdims=True)
        packed = [
            jnp.concatenate([part[32 * h + 8 * i : 32 * h + 8 * i + 8, :] for i in range(4)], axis=1)
            for h in range(2)
        ]
        spread = [rows4(sq[32 * h : 32 * h + 32]) for h in range(2)]
        s1[xx] = jnp.concatenate(packed + spread, axis=0).astype(BF16)

    wait_loaded(2)
    low32 = low_half(32)

    def pack_projection(layer):
        for q in range(4):
            g = glu[layer, :, 128 * q : 128 * q + 128].astype(F32)
            t = gate[layer, :, 128 * q : 128 * q + 128].astype(F32)
            ws[layer, 2 * q] = jnp.where(low32, g, roll(t, 64)).astype(BF16)
            ws[layer, 2 * q + 1] = jnp.where(low32, roll(g, 64), t).astype(BF16)

    pack_projection(0)

    half = lax.rem(y, 2)
    column = pl.ds(pl.multiple_of((y // 2) * 128, 128), 128)

    def pack_residual():
        for xx in range(4):
            t = tok[64 * xx : 64 * xx + 64, column].astype(F32)
            rz[xx] = fold_low(jnp.where(half == 1, roll(t, 64), t)).astype(BF16)

    def pack_input_weights():
        for q in range(4):
            t = win[1, :, 128 * q : 128 * q + 128].astype(F32)
            wis[2 * q] = fold_low(t).astype(BF16)
            wis[2 * q + 1] = fold_high(t).astype(BF16)

    def pack_gain():
        t = gain[1:2, column]
        return jnp.where(half == 1, roll(t, 64), t)[None]

    def assemble(g):
        for m in range(4):
            rows = pl.ds(pl.multiple_of((lax.rem(2 * m + g + 8 - 2 * x, 8) // 2) * 64, 64), 64)
            for q in range(4):
                a, b = (oa[2 * q, m], ob[2 * m, q]) if g == 0 else (ob[2 * m + 1, q], oa[2 * q + 1, m])
                mixed_ref[rows, 128 * q : 128 * q + 128] = unfold(a.astype(F32), b.astype(F32)).astype(BF16)

    @pl.when(core == 0)
    def _():
        with jax.named_scope("entry"):
            pl.semaphore_wait(barrier, 11)
        for k in (2, 3, 1, 0):
            send(s1.at[lax.rem(x + k, 4)], r1.at[d], PH1, at_x(k))
        for k in (0, *FARTHEST):
            send(ws.at[0, lax.rem(y + k, 8)], w.at[0, x, y, 0], far(k), at_y(k))
        wait_loaded(3)
        counts[0] = (lens[...] // BLOCK_LEN).astype(F32)
        send(counts.at[0], counts.at[0], COUNTS, at_x(0))
        wait_loaded(4)
        send(st, st2, STATE, at_x(0))

        @pl.when(d == z)
        def _():
            pack_residual()
            for k in range(4):
                send(rz.at[lax.rem(x + k, 4)], rz.at[4], RES0, at_x(k))

        pack_input_weights()
        for k in (0, *FARTHEST):
            send(wis.at[lax.rem(y + k, 8)], pk.at[0, y], STW, at_y(k))
        gb[pl.ds(d, 1)] = pack_gain()
        for k in range(4):
            send(gb.at[d], gb.at[d], GAIN, at_x(k))
        pack_projection(1)
        for k in (0, *FARTHEST):
            send(ws.at[1, lax.rem(y + k, 8)], w.at[1, x, y, 0], ST1, at_y(k))
        for i in range(5, 11):
            wait_loaded(i)

        wait_sent(s1, SENT_ON[PH1])
        wait_sent(w.at[0, 0], SMALL)
        wait_sent(counts.at[0], SENT_ON[COUNTS])
        wait_sent(st, READ)

        @pl.when(d == z)
        def _():
            wait_sent(rz.at[pl.ds(0, 4)], SENT_ON[RES0])

        wait_sent(wis, SENT_ON[STW])
        wait_sent(gb.at[pl.ds(0, 4)], SENT_ON[GAIN])

        wait_recv(nrecv, NEW)
        ns_ref[...] = nrecv[...]
        wait_recv(oa.at[pl.ds(0, 4)], PH9A)
        wait_recv(ob.at[pl.ds(0, 4)], PH9B)
        assemble(0)

    @pl.when(core == 1)
    def _():
        r1[pl.ds(d, 1)] = s1[pl.ds(x, 1)]
        w[0, pl.ds(x, 1), pl.ds(y, 1), 1] = ws[0, pl.ds(y, 1)][None]

        @pl.when(d == z)
        def _():
            pack_residual()
            rz[4] = rz[pl.ds(x, 1)][0]

        with jax.named_scope("entry"):
            pl.semaphore_wait(barrier, 18)
        for k in (2, 3, 1):
            send(s1.at[lax.rem(x + k, 4)], r1.at[d], PH1, at_x(k))
        for k in FARTHEST:
            send(ws.at[0, lax.rem(y + k, 8)], w.at[0, x, y, 1], far(k), at_y(k))

        def pass_on(*distances):
            if distances == (0,):
                wait_recv(w.at[0, x, y, 0], FAR)
            else:
                wait_recv(w.at[0, 0, pl.ds(0, len(distances))], far(distances[0]))
            for k in distances:
                block = w.at[0, x, lax.rem(y + 8 - k, 8)]
                for r in (2, 3, 1):
                    send(block, block, NEAR, at_x(r))

        @pl.when(d == z)
        def _():
            for k in (2, 3, 1):
                send(rz.at[lax.rem(x + k, 4)], rz.at[4], RES0, at_x(k))

        wait_loaded(3)
        counts[1] = (lens[...] // BLOCK_LEN).astype(F32)
        for i in range(4, 11):
            wait_loaded(i)
        wait_recv(counts.at[0], COUNTS)
        wait_recv(st2, STATE)
        eye = lax.broadcasted_iota(jnp.int32, (32, 32), 0) == lax.broadcasted_iota(jnp.int32, (32, 32), 1)
        blocks = jnp.concatenate(
            [
                jnp.sum(jnp.where(eye, jnp.broadcast_to(counts[h], (32, 32)), 0.0), axis=1, keepdims=True)
                for h in range(2)
            ],
            axis=0,
        )
        factor = 2.0 / (1.0 + blocks * (4.0 * BLOCK_LEN / LEN_MAX))

        def by_group(slabs, sign):
            zero = jnp.zeros((16, 64), F32)
            cols = []
            for c in range(2):
                top = jnp.concatenate([slabs[2 * c], zero], axis=1)
                low = jnp.concatenate([zero, slabs[2 * c + 1]], axis=1)
                both = jnp.concatenate([top, low], axis=0)
                cols.append(both if c == 0 else sign * both)
            return jnp.concatenate([jnp.concatenate(cols, axis=1)] * 4, axis=0)

        def constants(layer):
            def row(ref):
                return jnp.concatenate([ref[layer, 0:1, :], ref[layer, 1:2, :]], axis=1)

            e_re, e_im = row(er), row(ei)
            rate = jnp.exp(ls[layer : layer + 1, :])
            rate = jnp.concatenate(
                [jnp.broadcast_to(rate[:, 0:1], (1, 64)), jnp.broadcast_to(rate[:, 1:2], (1, 64))], axis=1
            )
            step = rate * factor
            magnitude = jnp.exp(e_re * step)
            turned = e_im * step
            a_re = magnitude * jnp.cos(turned)
            a_im = magnitude * jnp.sin(turned)
            modulus = e_re * e_re + e_im * e_im
            b_re = ((a_re - 1.0) * e_re + a_im * e_im) / modulus
            b_im = (a_im * e_re - (a_re - 1.0) * e_im) / modulus
            u = jnp.concatenate([st2[layer, 0], st[layer, 0]], axis=0)
            v = jnp.concatenate([st2[layer, 1], st[layer, 1]], axis=0)
            k_re = a_re * u - a_im * v
            k_im = a_re * v + a_im * u
            hi, lo = split2(by_group([im[layer, c, g] for c in range(2) for g in range(2)], 1.0))
            in_cat = jnp.concatenate([hi, lo], axis=0)
            hi, lo = split2(by_group([om[layer, c, g] for c in range(2) for g in range(2)], -1.0).T)
            out_cat = jnp.concatenate([hi, lo, hi], axis=0)
            direct = jnp.concatenate([skip[layer : layer + 1, :]] * 4, axis=1)
            return k_re, k_im, b_re, b_im, in_cat, out_cat, direct

        def recurrence(layer, consts, total):
            k_re, k_im, b_re, b_im, in_cat, out_cat, direct = consts
            driven = (total[0:16] * lax.rsqrt(total[16:32] / D + NORM_EPS)).astype(BF16).astype(F32)
            spread = jnp.concatenate(
                [jnp.where(group8 == i, driven[8 * h : 8 * h + 8], 0.0) for h in range(2) for i in range(4)],
                axis=0,
            ).astype(BF16)
            drive = lax.dot_general(
                jnp.concatenate([spread, spread], axis=1), in_cat, (((1,), (0,)), ((), ())),
                preferred_element_type=F32,
            )
            d_re, d_im = drive[:, 0:128], drive[:, 128:256]
            n_re = k_re + b_re * d_re - b_im * d_im
            n_im = k_im + b_re * d_im + b_im * d_re
            for part, new in ((0, n_re), (1, n_im)):
                nsend[layer, part] = new[0:32]
                ns_ref[layer, part] = new[32:64]
            hi, lo = split2(jnp.concatenate([n_re, n_im], axis=1))
            full = lax.dot_general(
                jnp.concatenate([hi, hi, lo], axis=1), out_cat, (((1,), (0,)), ((), ())),
                preferred_element_type=F32,
            )
            value = jnp.concatenate([rows4(full[32 * h : 32 * h + 32]) for h in range(2)], axis=0)
            value = value + direct * driven
            inner = 0.7978845608028654 * (value + 0.044715 * (value * value * value))
            return (value * (0.5 * (1.0 + jnp.tanh(inner)))).astype(BF16)

        def gather_readout(layer, value, sem):
            s2[layer] = value
            r2[layer, pl.ds(y, 1)] = value[None]
            for k in FARTHEST:
                send(s2.at[layer], r2.at[layer, y], sem, at_y(k))

        def unpack_readout(layer):
            got = [r2[layer, j].astype(F32) for j in range(8)]
            tiles = []
            for h in range(2):
                for i in range(4):
                    cols = []
                    for q in range(2):
                        parts = [got[4 * q + j][8 * h : 8 * h + 8] for j in range(4)]
                        cols.append(pick4([roll(parts[j], 32 * (j - i)) for j in range(4)], group8))
                    tiles.append(jnp.concatenate(cols, axis=1))
            return jnp.concatenate(tiles, axis=0).astype(BF16)

        def project(layer, piece, xx, out):
            rhs = jnp.concatenate([w[layer, xx, :, h].reshape(256, 128) for h in range(2)], axis=1)
            both = jnp.dot(piece, rhs, preferred_element_type=F32).astype(BF16)
            out[2 * xx] = both[:, 0:128]
            out[2 * xx + 1] = both[:, 128:256]

        def near(sem, block):
            for r in (2, 3, 1):
                send(block, block, sem, at_x(r))

        pass_on(0)
        consts0 = constants(0)
        for distances in NEAREST[:2]:
            pass_on(*distances)
        wait_recv(r1.at[pl.ds(0, 7)], PH1)
        value = recurrence(0, consts0, jnp.sum(r1[...].astype(F32), axis=0))
        gather_readout(0, value, PH2)
        for distances in NEAREST[2:]:
            pass_on(*distances)

        pack_input_weights()
        pk[1, pl.ds(y, 1)] = wis[pl.ds(y, 1)]
        for k in FARTHEST:
            send(wis.at[lax.rem(y + k, 8)], pk.at[1, y], STW, at_y(k))
        gb[pl.ds(d, 1)] = pack_gain()
        for k in range(1, 4):
            send(gb.at[d], gb.at[d], GAIN, at_x(k))
        pack_projection(1)
        w[1, pl.ds(x, 1), pl.ds(y, 1), 1] = ws[1, pl.ds(y, 1)][None]
        for k in FARTHEST:
            send(ws.at[1, lax.rem(y + k, 8)], w.at[1, x, y, 1], ST1, at_y(k))

        wait_recv(r2.at[0, pl.ds(0, 7)], PH2)
        piece = unpack_readout(0)
        wait_recv(w.at[0, pl.ds(0, 3)], NEAR)
        for xx in range(4):
            project(0, piece, xx, s3)
        for k in FARTHEST:
            send(s3.at[lax.rem(z + k, 8)], r3.at[z], PH3, at_z(k))
        r3[pl.ds(z, 1)] = s3[pl.ds(z, 1)]

        wait_recv(w.at[0, pl.ds(0, 3), pl.ds(0, 5), 0, pl.ds(0, 16)], STW)
        for h in range(2):
            for j in range(4):
                rows = unfold(pk[h, j].astype(F32), pk[h, 4 + j].astype(F32)).astype(BF16)
                wi[pl.ds(x, 1), h, 32 * j : 32 * j + 32, :] = rows[None]
        near(NEARW, wi.at[x])
        wait_recv(w.at[0, pl.ds(0, 3), pl.ds(0, 5), 0], ST1)
        near(NEAR1, w.at[1, x])
        send(nsend.at[0], nrecv.at[0], NEW, at_x(0, 0))

        @pl.when(d != z)
        def _():
            wait_recv(rz.at[4], RES0)

        def gated(parts, residual):
            linear, gate_sum = fold_low(parts), fold_high(parts)
            return (residual + linear * (1.0 / (1.0 + jnp.exp(-gate_sum)))).astype(BF16)

        residual0 = rz[4].astype(F32)
        wait_recv(r3.at[pl.ds(0, 7)], PH3)
        own = gated(jnp.sum(r3[...].astype(F32), axis=0), residual0)
        m0[...] = own
        r4[pl.ds(z, 1)] = own[None]
        for k in FARTHEST:
            send(m0, r4.at[z], PH4, at_z(k))

        alone = jnp.logical_and(x == 0, z < 2)

        @pl.when(jnp.logical_not(alone))
        def _():
            send(m0, rz1, RES1, {"tp": lax.rem(2 * x + z, 8) * 8 + y, "dp": (z // 2) * 2 + 1})

        @pl.when(alone)
        def _():
            rz1[...] = own

        consts1 = constants(1)
        wait_recv(gb.at[pl.ds(0, 7)], GAIN)
        low1 = low_half(1)
        gains = [jnp.where(low1, gb[2 * q], roll(gb[2 * q + 1], 64)) for q in range(4)]
        wait_recv(wi.at[pl.ds(0, 3)], NEARW)
        win_t = jnp.concatenate(
            [unfold(wi[q, 0].astype(F32), wi[q, 1].astype(F32)).T.astype(BF16) for q in range(4)], axis=0
        )

        wait_recv(r4.at[pl.ds(0, 7)], PH4)
        tiles = []
        sq = jnp.zeros((64, 1), F32)
        for q in range(4):
            cur = unfold(r4[2 * q].astype(F32), r4[2 * q + 1].astype(F32))
            sq = sq + jnp.sum(cur * cur, axis=1, keepdims=True)
            tiles.append((cur * gains[q]).astype(BF16))
        part = jnp.dot(jnp.concatenate(tiles, axis=1), win_t, preferred_element_type=F32)
        squares = [rows4(sq[32 * h : 32 * h + 32]) for h in range(2)]
        for q in range(2):
            for j in range(4):
                packed = []
                for h in range(2):
                    rows = [part[32 * h + 8 * i : 32 * h + 8 * i + 8, 128 * q : 128 * q + 128] for i in range(4)]
                    packed.append(pick4([roll(rows[i], 32 * (i - j)) for i in range(4)], group8))
                s5[4 * q + j] = jnp.concatenate(packed + squares, axis=0).astype(BF16)
        for k in FARTHEST:
            send(s5.at[lax.rem(y + k, 8)], r5.at[y], PH5, at_y(k))
        r5[pl.ds(y, 1)] = s5[pl.ds(y, 1)]
        wait_recv(r5.at[pl.ds(0, 7)], PH5)
        value = recurrence(1, consts1, jnp.sum(r5[...].astype(F32), axis=0))
        gather_readout(1, value, PH6)
        send(nsend.at[1], nrecv.at[1], NEW, at_x(0, 0))
        wait_recv(w.at[1, pl.ds(0, 3)], NEAR1)

        @pl.when(jnp.logical_not(alone))
        def _():
            wait_recv(rz1, RES1)

        wait_recv(r2.at[1, pl.ds(0, 7)], PH6)
        piece = unpack_readout(1)
        for xx in range(4):
            project(1, piece, xx, s7)
        for k in (4, 5, 2, 3, 6, 7, 0, 1):
            to = lax.rem(2 * x + k, 8)
            zz = lax.rem(2 * x + to, 8)
            dev = {"tp": zz * 8 + y, "dp": (to // 2) * 2 + 1}
            if k > 1:
                send(s7.at[to], r7.at[z], PH7, dev)
            else:

                @pl.when(z != zz)
                def _(to=to, dev=dev):
                    send(s7.at[to], r7.at[z], PH7, dev)

                @pl.when(z == zz)
                def _(to=to):
                    r7[pl.ds(z, 1)] = s7[pl.ds(to, 1)]

        wait_sent(s1.at[pl.ds(0, 3)], SENT_ON[PH1])
        wait_sent(w, BULK)
        wait_sent(w.at[0, pl.ds(0, 3), pl.ds(0, 7)], SMALL)
        wait_sent(r4.at[pl.ds(0, 7)], READ)
        wait_sent(gb.at[pl.ds(0, 3)], SENT_ON[GAIN])
        wait_sent(wis.at[pl.ds(0, 7)], SENT_ON[STW])

        @pl.when(d == z)
        def _():
            wait_sent(rz.at[pl.ds(0, 3)], SENT_ON[RES0])

        @pl.when(jnp.logical_not(alone))
        def _():
            wait_sent(m0, SENT_ON[RES1])

        keeps = jnp.logical_or(z == lax.rem(4 * x, 8), z == lax.rem(4 * x + 1, 8))

        @pl.when(keeps)
        def _():
            wait_recv(r7.at[pl.ds(0, 7)], PH7)

        @pl.when(jnp.logical_not(keeps))
        def _():
            wait_recv(r7, PH7)

        own = gated(jnp.sum(r7[...].astype(F32), axis=0), rz1[...].astype(F32))

        odd = lax.rem(y + z, 2)
        core_a = 2 * x + lax.rem(y, 2)
        core_b = 2 * x + lax.rem(z, 2)

        ORDER = (0, 1, 2, 7, 3, 6, 5, 4)

        def others(mine, serve, first=0):
            for t in ORDER:
                if t >= first:

                    @pl.when(mine != t)
                    def _(t=t):
                        serve(t)

        def apart(a, b):
            k = lax.rem(a + 8 - b, 8)
            return jnp.minimum(k, 8 - k)

        def across(block, sent):
            others(y, lambda t: send(block, block, PH9A, {"tp": z * 8 + t, "dp": core_a}, sent))

        def along(block, sent, first=0):
            others(z, lambda t: send(block, block, PH9B, {"tp": t * 8 + y, "dp": core_b}, sent), first)

        def to_own_a(block):
            @pl.when(lax.rem(y, 2) == 0)
            def _():
                send(block, block, PH9A, at_x(0, 0), SENT_A)

        def to_own_b(block):
            @pl.when(lax.rem(z, 2) == 0)
            def _():
                send(block, block, PH9B, at_x(0, 0), SENT_B)

        def from_z(distances):
            wait_recv(r4.at[pl.ds(0, len(distances))], last(distances[0]))
            for k in distances:
                block = oa.at[y, lax.rem(z + 8 - k, 8) // 2]
                if distances[0] < 3:
                    across(block, RELAY_A)
                else:

                    @pl.when(z > 1)
                    def _(block=block):
                        across(block, RELAY_A)

                to_own_a(block)

        def from_y(distances):
            wait_recv(r4.at[pl.ds(0, len(distances))], last(distances[0]))
            for k in distances:
                block = ob.at[z, lax.rem(y + 8 - k, 8) // 2]
                along(block, RELAY_B, 2)
                to_own_b(block)

        def straight(t, block, sem, parity):
            for k in FARTHEST:
                send(block, block, sem, {"tp": t * 8 + lax.rem(y + k, 8), "dp": 2 * x + parity}, LOW + t)

        @pl.when(odd == 0)
        def _():
            block = oa.at[y, z // 2]
            oa[pl.ds(y, 1), pl.ds(z // 2, 1)] = own[None, None]
            for t in (0, 1):

                @pl.when(apart(z, t) > 2)
                def _(t=t):
                    straight(t, block, PH9A, lax.rem(y, 2))

            others(z, lambda t: send(block, block, LAST + apart(t, z) - 1, {"tp": t * 8 + y, "dp": one}, SENT_LAST))
            across(block, SENT_ON[PH9A])
            to_own_a(block)
            for distances in NEAREST:
                (from_z if distances[0] % 2 == 0 else from_y)(distances)

        @pl.when(odd == 1)
        def _():
            block = ob.at[z, y // 2]
            ob[pl.ds(z, 1), pl.ds(y // 2, 1)] = own[None, None]
            for t in (0, 1):

                @pl.when(z != t)
                def _(t=t):
                    straight(t, block, PH9B, lax.rem(z, 2))

            others(y, lambda t: send(block, block, LAST + apart(t, y) - 1, {"tp": z * 8 + t, "dp": one}, SENT_LAST))
            along(block, SENT_ON[PH9B])
            to_own_b(block)
            for distances in NEAREST:
                (from_y if distances[0] % 2 == 0 else from_z)(distances)

        def last_waits(buffer, sem, parity):
            @pl.when(parity == 0)
            def _():
                wait_recv(buffer.at[pl.ds(0, 4)], sem)

            @pl.when(parity == 1)
            def _():
                wait_recv(buffer.at[pl.ds(0, 3)], sem)

        last_waits(oa, PH9A, lax.rem(y, 2))
        last_waits(ob, PH9B, lax.rem(z, 2))
        with jax.named_scope("assemble"):
            assemble(1)

        with jax.named_scope("sent"):
            wait_sent(r4.at[pl.ds(0, 7)], SENT_ON[PH9A])
            for parity in range(2):
                for low in range(2):

                    @pl.when(jnp.logical_and(odd == parity, (z < 2) if low else (z > 1)))
                    def _(parity=parity, low=low):
                        wait_sent(oa.at[pl.ds(0, 5 + low), pl.ds(0, 4 - parity)], RELAY_B)
                        wait_sent(oa.at[pl.ds(0, 7), pl.ds(0, 2 if low else 3 + parity)], RELAY_A)

            for t in (0, 1):

                @pl.when(jnp.where(odd == 0, apart(z, t) > 2, z != t))
                def _(t=t):
                    wait_sent(r4.at[pl.ds(0, 7)], LOW + t)

            @pl.when(lax.rem(y, 2) == 0)
            def _():
                wait_sent(oa.at[0], SENT_A)

            @pl.when(lax.rem(z, 2) == 0)
            def _():
                wait_sent(ob.at[0], SENT_B)

        wait_sent(r4.at[pl.ds(0, 7)], SENT_LAST)

        @pl.when(keeps)
        def _():
            wait_sent(s7.at[pl.ds(0, 7)], SENT_ON[PH7])

        @pl.when(jnp.logical_not(keeps))
        def _():
            wait_sent(s7, SENT_ON[PH7])


def hand_over(mixed, state, mixed_h, state_h, sems):
    copies = [
        pltpu.make_async_copy(mixed, mixed_h, sems.at[0]),
        pltpu.make_async_copy(state, state_h, sems.at[1]),
    ]
    for copy in copies:
        copy.start()
    for copy in copies:
        copy.wait()


def body(tokens, lengths, norm_gain, w_in, log_step, eig_re, eig_im, in_mat, output_matrices, skip,
         w_glu, w_gate, state):
    args = (tokens, lengths.reshape(1, 32), norm_gain, w_in.swapaxes(1, 2), log_step, eig_re, eig_im,
            in_mat.swapaxes(3, 4), output_matrices, skip, w_glu, w_gate, state)
    mixed, new_state = pl.pallas_call(
        kernel,
        name="decode",
        out_shape=(pltpu.VMEM((256, 512), BF16), pltpu.VMEM((2, 2, 32, 128), F32)),
        in_specs=[pl.BlockSpec(memory_space=pl.ANY)] * 13,
        out_specs=(pl.BlockSpec(memory_space=pltpu.VMEM),) * 2,
        scratch_shapes=[pltpu.VMEM(a.shape, a.dtype) for a in args]
        + [
            pltpu.VMEM((4, 32, 128), BF16),
            pltpu.VMEM((8, 32, 128), BF16),
            pltpu.VMEM((2, 8, 32, 128), BF16),
            pltpu.VMEM((2, 4, 8, 2, 32, 128), BF16),
            pltpu.VMEM((8, 16, 128), BF16),
            pltpu.VMEM((2, 8, 16, 128), BF16),
            pltpu.VMEM((4, 2, 128, 128), BF16),
            pltpu.VMEM((8, 1, 128), F32),
            pltpu.VMEM((5, 32, 128), BF16),
            pltpu.VMEM((32, 128), BF16),
            pltpu.VMEM((2, 16, 128), BF16),
            pltpu.VMEM((2, 8, 16, 128), BF16),
            pltpu.VMEM((8, 64, 128), BF16),
            pltpu.VMEM((8, 64, 128), BF16),
            pltpu.VMEM((8, 32, 128), BF16),
            pltpu.VMEM((32, 128), BF16),
            pltpu.VMEM((8, 32, 128), BF16),
            pltpu.VMEM((8, 32, 128), BF16),
            pltpu.VMEM((8, 64, 128), BF16),
            pltpu.VMEM((8, 64, 128), BF16),
            pltpu.VMEM((8, 4, 32, 128), BF16),
            pltpu.VMEM((8, 4, 32, 128), BF16),
            pltpu.VMEM((2, 1, 32), F32),
            pltpu.VMEM((2, 2, 32, 128), F32),
            pltpu.VMEM((2, 2, 32, 128), F32),
            pltpu.VMEM((2, 2, 32, 128), F32),
            pltpu.SemaphoreType.DMA((11,)),
            pltpu.SemaphoreType.DMA((SENT,)),
            pltpu.SemaphoreType.DMA((RECV,)),
        ],
        compiler_params=pltpu.CompilerParams(collective_id=0, has_side_effects=True),
    )(*args)
    inside = [pltpu.with_memory_space_constraint(a, pltpu.VMEM) for a in (mixed, new_state)]
    return pl.pallas_call(
        hand_over,
        name="hand_over",
        out_shape=(jax.ShapeDtypeStruct((256, 512), BF16), jax.ShapeDtypeStruct((2, 2, 32, 128), F32)),
        in_specs=[pl.BlockSpec(memory_space=pltpu.VMEM)] * 2,
        out_specs=(pl.BlockSpec(memory_space=pl.ANY),) * 2,
        scratch_shapes=[pltpu.SemaphoreType.DMA((2,))],
    )(*inside)


def solution(mesh):
    placed = (
        P(None, "dp"),
        P("dp"),
        P(None, "dp"),
        P(None, "dp", "tp"),
        P(None, "tp"),
        P(None, "tp", None),
        P(None, "tp", None),
        P(None, None, "tp", None, None),
        P(None, None, "tp", None, None),
        P(None, "tp"),
        P(None, "tp", "dp"),
        P(None, "tp", "dp"),
        P(None, None, "dp", "tp"),
    )
    return jax.shard_map(
        body,
        mesh=mesh,
        in_specs=placed,
        out_specs=(P(None, "dp"), P(None, None, "dp", "tp")),
        check_vma=False,
    )
```

```python
import jax
import jax.numpy as jnp
from jax import lax
from jax.experimental import pallas as pl
from jax.experimental.pallas import tpu as pltpu
from jax.sharding import PartitionSpec as P

D = 4096
LEN_MAX = 4096
BLOCK_LEN = 256
NORM_EPS = 1e-06
MESH = pl.DeviceIdType.MESH
NT = (((1,), (1,)), ((), ()))
F32 = jnp.float32
BF16 = jnp.bfloat16

(PH1, RES0, PH2, ST1, STW, PH3, PH4, RES1, PH5, PH6, PH7, PH9A, PH9B, GAIN, STATE, COUNTS, NEW, NEAR, NEAR1, NEARW) = range(20)
FAR = 20
LAST = FAR + 5
RECV = LAST + 4
BULK, SMALL, READ = range(3)
SENT_ON = {NEAR: BULK, NEAR1: BULK, NEARW: BULK, NEW: BULK, STATE: READ, COUNTS: 3, PH3: SMALL, PH4: SMALL, PH5: SMALL,
           PH2: READ, PH6: READ, STW: 4, PH1: 5, GAIN: 6, RES0: 7, RES1: 8, PH7: 9, PH9A: 10, PH9B: 10}
SENT_LAST, SENT_A, SENT_B, RELAY_A, RELAY_B, LOW, SENT = 3, 11, 12, 13, 14, 15, 17
NEAREST = ((1, 7), (2, 6), (3, 5), (4,))
FARTHEST = (4, 3, 5, 2, 6, 1, 7)


def roll(x, amount):
    amount = amount % 128
    return x if amount == 0 else pltpu.roll(x, amount, 1)


def groups4(rows):
    return lax.broadcasted_iota(jnp.int32, (rows, 128), 1) // 32


def low_half(rows):
    return lax.broadcasted_iota(jnp.int32, (rows, 128), 1) < 64


def pick4(parts, group):
    out = parts[3]
    for i in (2, 1, 0):
        out = jnp.where(group == i, parts[i], out)
    return out


def split2(x):
    hi = x.astype(BF16)
    lo = (x - hi.astype(F32)).astype(BF16)
    return hi, lo


def kernel(
    tok_h, len_h, gain_h, win_h, ls_h, er_h, ei_h, im_h, om_h, skip_h, glu_h, gate_h, st_h,
    mixed_ref, ns_ref,
    tok, lens, gain, win, ls, er, ei, im, om, skip, glu, gate, st,
    s1, r1, ws, w, wis, pk, wi, gb, rz, rz1, s2, r2, s3, r3, r4, m0, s5, r5, s7, r7, oa, ob,
    counts, st2, nsend, nrecv,
    lsem, ss, rs,
):
    tp = lax.axis_index("tp")
    d = lax.axis_index("dp")
    z = tp // 8
    y = lax.rem(tp, 8)
    x = d // 2
    core = lax.rem(d, 2)
    one = 2 * x + 1

    def at_y(k, dp=None):
        return {"tp": z * 8 + lax.rem(y + k, 8), "dp": one if dp is None else dp}

    def at_z(k, dp=None):
        return {"tp": lax.rem(z + k, 8) * 8 + y, "dp": one if dp is None else dp}

    def far(k):
        return FAR + min(k, 8 - k)

    def last(k):
        return LAST + min(k, 8 - k) - 1

    def at_x(k, c=1):
        return {"tp": tp, "dp": 2 * lax.rem(x + k, 4) + c}

    def send(src, dst, sem, dev, sent=None):
        if sent is None:
            sent = SENT_LAST if sem >= LAST else SMALL if sem >= FAR or sem == ST1 else SENT_ON[sem]
        pltpu.make_async_remote_copy(
            src_ref=src,
            dst_ref=dst,
            send_sem=ss.at[sent],
            recv_sem=rs.at[sem],
            device_id=dev,
            device_id_type=MESH,
        ).start()

    def wait_recv(ref, sem):
        with jax.named_scope(f"recv{sem}"):
            pltpu.make_async_copy(ref, ref, rs.at[sem]).wait()

    def wait_sent(ref, sem):
        pltpu.make_async_copy(ref, ref, ss.at[sem]).wait()

    def fold_low(t):
        n = t.shape[0] // 2
        return jnp.where(low_half(n), t[0:n], roll(t[n : 2 * n], 64))

    def fold_high(t):
        n = t.shape[0] // 2
        return jnp.where(low_half(n), roll(t[0:n], 64), t[n : 2 * n])

    def unfold(a, b):
        low = low_half(a.shape[0])
        return jnp.concatenate([jnp.where(low, a, roll(b, 64)), jnp.where(low, roll(a, 64), b)], axis=0)

    hbm = (tok_h, win_h, gain_h, glu_h, gate_h, len_h, st_h, ls_h, er_h, ei_h, im_h, om_h, skip_h)
    vmem = (tok, win, gain, glu, gate, lens, st, ls, er, ei, im, om, skip)
    group = (0, 0, 1, 2, 2, 3, 4, 5, 6, 7, 8, 9, 10)
    loads = [pltpu.make_async_copy(a, b, lsem.at[i]) for i, a, b in zip(group, hbm, vmem)]

    def wait_loaded(i):
        ref = (w.at[0, pl.ds(0, 4), pl.ds(0, 5)], gain, w.at[0, 0], lens, st, ls, er, ei, im, om, skip)[i]
        pltpu.make_async_copy(ref, ref, lsem.at[i]).wait()

    for copy in loads[:3]:
        copy.start()

    barrier = pltpu.get_barrier_semaphore()

    def greet(dev):
        pl.semaphore_signal(barrier, inc=1, device_id=dev, device_id_type=MESH)

    @pl.when(core == 1)
    def _():
        for k in FARTHEST:
            greet(at_y(k))
            greet(at_y(k, 2 * x))
        for k in FARTHEST:
            greet(at_z(k))
        for k in (2, 3, 1):
            greet(at_x(k, 0))
            greet(at_x(k))
        greet(at_x(0, 0))

    @pl.when(core == 0)
    def _():
        greet(at_x(0))

    for copy in loads[3:]:
        copy.start()
    group8 = groups4(8)

    def rows4(t):
        return pick4([jnp.broadcast_to(t[8 * i : 8 * i + 8], (8, 128)) for i in range(4)], group8)

    with jax.named_scope("load0"):
        wait_loaded(0)
        wait_loaded(1)
    for xx in range(4):
        t = tok[64 * xx : 64 * xx + 64, :].astype(F32)
        scaled = (t * gain[0:1, :]).astype(BF16)
        part = lax.dot_general(scaled, win[0], NT, preferred_element_type=F32)
        sq = jnp.sum(t * t, axis=1, keepdims=True)
        packed = [
            jnp.concatenate([part[32 * h + 8 * i : 32 * h + 8 * i + 8, :] for i in range(4)], axis=1)
            for h in range(2)
        ]
        spread = [rows4(sq[32 * h : 32 * h + 32]) for h in range(2)]
        s1[xx] = jnp.concatenate(packed + spread, axis=0).astype(BF16)

    wait_loaded(2)
    low32 = low_half(32)

    def pack_projection(layer):
        for q in range(4):
            g = glu[layer, :, 128 * q : 128 * q + 128].astype(F32)
            t = gate[layer, :, 128 * q : 128 * q + 128].astype(F32)
            ws[layer, 2 * q] = jnp.where(low32, g, roll(t, 64)).astype(BF16)
            ws[layer, 2 * q + 1] = jnp.where(low32, roll(g, 64), t).astype(BF16)

    pack_projection(0)

    half = lax.rem(y, 2)
    column = pl.ds(pl.multiple_of((y // 2) * 128, 128), 128)

    def pack_residual():
        for xx in range(4):
            t = tok[64 * xx : 64 * xx + 64, column].astype(F32)
            rz[xx] = fold_low(jnp.where(half == 1, roll(t, 64), t)).astype(BF16)

    def pack_input_weights():
        for q in range(4):
            t = win[1, :, 128 * q : 128 * q + 128].astype(F32)
            wis[2 * q] = fold_low(t).astype(BF16)
            wis[2 * q + 1] = fold_high(t).astype(BF16)

    def pack_gain():
        t = gain[1:2, column]
        return jnp.where(half == 1, roll(t, 64), t)[None]

    def assemble(g):
        for m in range(4):
            rows = pl.ds(pl.multiple_of((lax.rem(2 * m + g + 8 - 2 * x, 8) // 2) * 64, 64), 64)
            for q in range(4):
                a, b = (oa[2 * q, m], ob[2 * m, q]) if g == 0 else (ob[2 * m + 1, q], oa[2 * q + 1, m])
                mixed_ref[rows, 128 * q : 128 * q + 128] = unfold(a.astype(F32), b.astype(F32)).astype(BF16)

    @pl.when(core == 0)
    def _():
        with jax.named_scope("entry"):
            pl.semaphore_wait(barrier, 11)
        for k in (2, 3, 1, 0):
            send(s1.at[lax.rem(x + k, 4)], r1.at[d], PH1, at_x(k))
        for k in (0, *FARTHEST):
            send(ws.at[0, lax.rem(y + k, 8)], w.at[0, x, y, 0], far(k), at_y(k))
        wait_loaded(3)
        counts[0] = (lens[...] // BLOCK_LEN).astype(F32)
        send(counts.at[0], counts.at[0], COUNTS, at_x(0))
        wait_loaded(4)
        send(st, st2, STATE, at_x(0))

        @pl.when(d == z)
        def _():
            pack_residual()
            for k in range(4):
                send(rz.at[lax.rem(x + k, 4)], rz.at[4], RES0, at_x(k))

        pack_input_weights()
        for k in (0, *FARTHEST):
            send(wis.at[lax.rem(y + k, 8)], pk.at[0, y], STW, at_y(k))
        gb[pl.ds(d, 1)] = pack_gain()
        for k in range(4):
            send(gb.at[d], gb.at[d], GAIN, at_x(k))
        pack_projection(1)
        for k in (0, *FARTHEST):
            send(ws.at[1, lax.rem(y + k, 8)], w.at[1, x, y, 0], ST1, at_y(k))
        for i in range(5, 11):
            wait_loaded(i)

        wait_sent(s1, SENT_ON[PH1])
        wait_sent(w.at[0, 0], SMALL)
        wait_sent(counts.at[0], SENT_ON[COUNTS])
        wait_sent(st, READ)

        @pl.when(d == z)
        def _():
            wait_sent(rz.at[pl.ds(0, 4)], SENT_ON[RES0])

        wait_sent(wis, SENT_ON[STW])
        wait_sent(gb.at[pl.ds(0, 4)], SENT_ON[GAIN])

        wait_recv(nrecv, NEW)
        ns_ref[...] = nrecv[...]
        wait_recv(oa.at[pl.ds(0, 4)], PH9A)
        wait_recv(ob.at[pl.ds(0, 4)], PH9B)
        assemble(0)

    @pl.when(core == 1)
    def _():
        r1[pl.ds(d, 1)] = s1[pl.ds(x, 1)]
        w[0, pl.ds(x, 1), pl.ds(y, 1), 1] = ws[0, pl.ds(y, 1)][None]

        @pl.when(d == z)
        def _():
            pack_residual()
            rz[4] = rz[pl.ds(x, 1)][0]

        with jax.named_scope("entry"):
            pl.semaphore_wait(barrier, 18)
        for k in (2, 3, 1):
            send(s1.at[lax.rem(x + k, 4)], r1.at[d], PH1, at_x(k))
        for k in FARTHEST:
            send(ws.at[0, lax.rem(y + k, 8)], w.at[0, x, y, 1], far(k), at_y(k))

        def pass_on(*distances):
            if distances == (0,):
                wait_recv(w.at[0, x, y, 0], FAR)
            else:
                wait_recv(w.at[0, 0, pl.ds(0, len(distances))], far(distances[0]))
            for k in distances:
                block = w.at[0, x, lax.rem(y + 8 - k, 8)]
                for r in (2, 3, 1):
                    send(block, block, NEAR, at_x(r))

        @pl.when(d == z)
        def _():
            for k in (2, 3, 1):
                send(rz.at[lax.rem(x + k, 4)], rz.at[4], RES0, at_x(k))

        wait_loaded(3)
        counts[1] = (lens[...] // BLOCK_LEN).astype(F32)
        for i in range(4, 11):
            wait_loaded(i)
        wait_recv(counts.at[0], COUNTS)
        wait_recv(st2, STATE)
        eye = lax.broadcasted_iota(jnp.int32, (32, 32), 0) == lax.broadcasted_iota(jnp.int32, (32, 32), 1)
        blocks = jnp.concatenate(
            [
                jnp.sum(jnp.where(eye, jnp.broadcast_to(counts[h], (32, 32)), 0.0), axis=1, keepdims=True)
                for h in range(2)
            ],
            axis=0,
        )
        factor = 2.0 / (1.0 + blocks * (4.0 * BLOCK_LEN / LEN_MAX))

        def by_group(slabs, sign):
            zero = jnp.zeros((16, 64), F32)
            cols = []
            for c in range(2):
                top = jnp.concatenate([slabs[2 * c], zero], axis=1)
                low = jnp.concatenate([zero, slabs[2 * c + 1]], axis=1)
                both = jnp.concatenate([top, low], axis=0)
                cols.append(both if c == 0 else sign * both)
            return jnp.concatenate([jnp.concatenate(cols, axis=1)] * 4, axis=0)

        def constants(layer):
            def row(ref):
                return jnp.concatenate([ref[layer, 0:1, :], ref[layer, 1:2, :]], axis=1)

            e_re, e_im = row(er), row(ei)
            rate = jnp.exp(ls[layer : layer + 1, :])
            rate = jnp.concatenate(
                [jnp.broadcast_to(rate[:, 0:1], (1, 64)), jnp.broadcast_to(rate[:, 1:2], (1, 64))], axis=1
            )
            step = rate * factor
            magnitude = jnp.exp(e_re * step)
            turned = e_im * step
            a_re = magnitude * jnp.cos(turned)
            a_im = magnitude * jnp.sin(turned)
            modulus = e_re * e_re + e_im * e_im
            b_re = ((a_re - 1.0) * e_re + a_im * e_im) / modulus
            b_im = (a_im * e_re - (a_re - 1.0) * e_im) / modulus
            u = jnp.concatenate([st2[layer, 0], st[layer, 0]], axis=0)
            v = jnp.concatenate([st2[layer, 1], st[layer, 1]], axis=0)
            k_re = a_re * u - a_im * v
            k_im = a_re * v + a_im * u
            hi, lo = split2(by_group([im[layer, c, g] for c in range(2) for g in range(2)], 1.0))
            in_cat = jnp.concatenate([hi, lo], axis=0)
            hi, lo = split2(by_group([om[layer, c, g] for c in range(2) for g in range(2)], -1.0).T)
            out_cat = jnp.concatenate([hi, lo, hi], axis=0)
            direct = jnp.concatenate([skip[layer : layer + 1, :]] * 4, axis=1)
            return k_re, k_im, b_re, b_im, in_cat, out_cat, direct

        def recurrence(layer, consts, total):
            k_re, k_im, b_re, b_im, in_cat, out_cat, direct = consts
            driven = (total[0:16] * lax.rsqrt(total[16:32] / D + NORM_EPS)).astype(BF16).astype(F32)
            spread = jnp.concatenate(
                [jnp.where(group8 == i, driven[8 * h : 8 * h + 8], 0.0) for h in range(2) for i in range(4)],
                axis=0,
            ).astype(BF16)
            drive = lax.dot_general(
                jnp.concatenate([spread, spread], axis=1), in_cat, (((1,), (0,)), ((), ())),
                preferred_element_type=F32,
            )
            d_re, d_im = drive[:, 0:128], drive[:, 128:256]
            n_re = k_re + b_re * d_re - b_im * d_im
            n_im = k_im + b_re * d_im + b_im * d_re
            for part, new in ((0, n_re), (1, n_im)):
                nsend[layer, part] = new[0:32]
                ns_ref[layer, part] = new[32:64]
            hi, lo = split2(jnp.concatenate([n_re, n_im], axis=1))
            full = lax.dot_general(
                jnp.concatenate([hi, hi, lo], axis=1), out_cat, (((1,), (0,)), ((), ())),
                preferred_element_type=F32,
            )
            value = jnp.concatenate([rows4(full[32 * h : 32 * h + 32]) for h in range(2)], axis=0)
            value = value + direct * driven
            inner = 0.7978845608028654 * (value + 0.044715 * (value * value * value))
            return (value * (0.5 * (1.0 + jnp.tanh(inner)))).astype(BF16)

        def gather_readout(layer, value, sem):
            s2[layer] = value
            r2[layer, pl.ds(y, 1)] = value[None]
            for k in FARTHEST:
                send(s2.at[layer], r2.at[layer, y], sem, at_y(k))

        def unpack_readout(layer):
            got = [r2[layer, j].astype(F32) for j in range(8)]
            tiles = []
            for h in range(2):
                for i in range(4):
                    cols = []
                    for q in range(2):
                        parts = [got[4 * q + j][8 * h : 8 * h + 8] for j in range(4)]
                        cols.append(pick4([roll(parts[j], 32 * (j - i)) for j in range(4)], group8))
                    tiles.append(jnp.concatenate(cols, axis=1))
            return jnp.concatenate(tiles, axis=0).astype(BF16)

        def project(layer, piece, xx, out):
            rhs = jnp.concatenate([w[layer, xx, :, h].reshape(256, 128) for h in range(2)], axis=1)
            both = jnp.dot(piece, rhs, preferred_element_type=F32).astype(BF16)
            out[2 * xx] = both[:, 0:128]
            out[2 * xx + 1] = both[:, 128:256]

        def near(sem, block):
            for r in (2, 3, 1):
                send(block, block, sem, at_x(r))

        pass_on(0)
        consts0 = constants(0)
        for distances in NEAREST[:2]:
            pass_on(*distances)
        wait_recv(r1.at[pl.ds(0, 7)], PH1)
        value = recurrence(0, consts0, jnp.sum(r1[...].astype(F32), axis=0))
        gather_readout(0, value, PH2)
        for distances in NEAREST[2:]:
            pass_on(*distances)

        pack_input_weights()
        pk[1, pl.ds(y, 1)] = wis[pl.ds(y, 1)]
        for k in FARTHEST:
            send(wis.at[lax.rem(y + k, 8)], pk.at[1, y], STW, at_y(k))
        gb[pl.ds(d, 1)] = pack_gain()
        for k in range(1, 4):
            send(gb.at[d], gb.at[d], GAIN, at_x(k))
        pack_projection(1)
        w[1, pl.ds(x, 1), pl.ds(y, 1), 1] = ws[1, pl.ds(y, 1)][None]
        for k in FARTHEST:
            send(ws.at[1, lax.rem(y + k, 8)], w.at[1, x, y, 1], ST1, at_y(k))

        wait_recv(r2.at[0, pl.ds(0, 7)], PH2)
        piece = unpack_readout(0)
        wait_recv(w.at[0, pl.ds(0, 3)], NEAR)
        for xx in range(4):
            project(0, piece, xx, s3)
        for k in FARTHEST:
            send(s3.at[lax.rem(z + k, 8)], r3.at[z], PH3, at_z(k))
        r3[pl.ds(z, 1)] = s3[pl.ds(z, 1)]

        wait_recv(w.at[0, pl.ds(0, 3), pl.ds(0, 5), 0, pl.ds(0, 16)], STW)
        for h in range(2):
            for j in range(4):
                rows = unfold(pk[h, j].astype(F32), pk[h, 4 + j].astype(F32)).astype(BF16)
                wi[pl.ds(x, 1), h, 32 * j : 32 * j + 32, :] = rows[None]
        near(NEARW, wi.at[x])
        wait_recv(w.at[0, pl.ds(0, 3), pl.ds(0, 5), 0], ST1)
        near(NEAR1, w.at[1, x])
        send(nsend.at[0], nrecv.at[0], NEW, at_x(0, 0))

        @pl.when(d != z)
        def _():
            wait_recv(rz.at[4], RES0)

        def gated(parts, residual):
            linear, gate_sum = fold_low(parts), fold_high(parts)
            return (residual + linear * (1.0 / (1.0 + jnp.exp(-gate_sum)))).astype(BF16)

        residual0 = rz[4].astype(F32)
        wait_recv(r3.at[pl.ds(0, 7)], PH3)
        own = gated(jnp.sum(r3[...].astype(F32), axis=0), residual0)
        m0[...] = own
        r4[pl.ds(z, 1)] = own[None]
        for k in FARTHEST:
            send(m0, r4.at[z], PH4, at_z(k))

        alone = jnp.logical_and(x == 0, z < 2)

        @pl.when(jnp.logical_not(alone))
        def _():
            send(m0, rz1, RES1, {"tp": lax.rem(2 * x + z, 8) * 8 + y, "dp": (z // 2) * 2 + 1})

        @pl.when(alone)
        def _():
            rz1[...] = own

        consts1 = constants(1)
        wait_recv(gb.at[pl.ds(0, 7)], GAIN)
        low1 = low_half(1)
        gains = [jnp.where(low1, gb[2 * q], roll(gb[2 * q + 1], 64)) for q in range(4)]
        wait_recv(wi.at[pl.ds(0, 3)], NEARW)
        win_t = jnp.concatenate(
            [unfold(wi[q, 0].astype(F32), wi[q, 1].astype(F32)).T.astype(BF16) for q in range(4)], axis=0
        )

        wait_recv(r4.at[pl.ds(0, 7)], PH4)
        tiles = []
        sq = jnp.zeros((64, 1), F32)
        for q in range(4):
            cur = unfold(r4[2 * q].astype(F32), r4[2 * q + 1].astype(F32))
            sq = sq + jnp.sum(cur * cur, axis=1, keepdims=True)
            tiles.append((cur * gains[q]).astype(BF16))
        part = jnp.dot(jnp.concatenate(tiles, axis=1), win_t, preferred_element_type=F32)
        squares = [rows4(sq[32 * h : 32 * h + 32]) for h in range(2)]
        for q in range(2):
            for j in range(4):
                packed = []
                for h in range(2):
                    rows = [part[32 * h + 8 * i : 32 * h + 8 * i + 8, 128 * q : 128 * q + 128] for i in range(4)]
                    packed.append(pick4([roll(rows[i], 32 * (i - j)) for i in range(4)], group8))
                s5[4 * q + j] = jnp.concatenate(packed + squares, axis=0).astype(BF16)
        for k in FARTHEST:
            send(s5.at[lax.rem(y + k, 8)], r5.at[y], PH5, at_y(k))
        r5[pl.ds(y, 1)] = s5[pl.ds(y, 1)]
        wait_recv(r5.at[pl.ds(0, 7)], PH5)
        value = recurrence(1, consts1, jnp.sum(r5[...].astype(F32), axis=0))
        gather_readout(1, value, PH6)
        send(nsend.at[1], nrecv.at[1], NEW, at_x(0, 0))
        wait_recv(w.at[1, pl.ds(0, 3)], NEAR1)

        @pl.when(jnp.logical_not(alone))
        def _():
            wait_recv(rz1, RES1)

        wait_recv(r2.at[1, pl.ds(0, 7)], PH6)
        piece = unpack_readout(1)
        for xx in range(4):
            project(1, piece, xx, s7)
        for k in (4, 5, 2, 3, 6, 7, 0, 1):
            to = lax.rem(2 * x + k, 8)
            zz = lax.rem(2 * x + to, 8)
            dev = {"tp": zz * 8 + y, "dp": (to // 2) * 2 + 1}
            if k > 1:
                send(s7.at[to], r7.at[z], PH7, dev)
            else:

                @pl.when(z != zz)
                def _(to=to, dev=dev):
                    send(s7.at[to], r7.at[z], PH7, dev)

                @pl.when(z == zz)
                def _(to=to):
                    r7[pl.ds(z, 1)] = s7[pl.ds(to, 1)]

        wait_sent(s1.at[pl.ds(0, 3)], SENT_ON[PH1])
        wait_sent(w, BULK)
        wait_sent(w.at[0, pl.ds(0, 3), pl.ds(0, 7)], SMALL)
        wait_sent(r4.at[pl.ds(0, 7)], READ)
        wait_sent(gb.at[pl.ds(0, 3)], SENT_ON[GAIN])
        wait_sent(wis.at[pl.ds(0, 7)], SENT_ON[STW])

        @pl.when(d == z)
        def _():
            wait_sent(rz.at[pl.ds(0, 3)], SENT_ON[RES0])

        @pl.when(jnp.logical_not(alone))
        def _():
            wait_sent(m0, SENT_ON[RES1])

        keeps = jnp.logical_or(z == lax.rem(4 * x, 8), z == lax.rem(4 * x + 1, 8))

        @pl.when(keeps)
        def _():
            wait_recv(r7.at[pl.ds(0, 7)], PH7)

        @pl.when(jnp.logical_not(keeps))
        def _():
            wait_recv(r7, PH7)

        own = gated(jnp.sum(r7[...].astype(F32), axis=0), rz1[...].astype(F32))

        odd = lax.rem(y + z, 2)
        core_a = 2 * x + lax.rem(y, 2)
        core_b = 2 * x + lax.rem(z, 2)

        ORDER = (0, 1, 2, 7, 3, 6, 5, 4)

        def others(mine, serve, first=0):
            for t in ORDER:
                if t >= first:

                    @pl.when(mine != t)
                    def _(t=t):
                        serve(t)

        def apart(a, b):
            k = lax.rem(a + 8 - b, 8)
            return jnp.minimum(k, 8 - k)

        def across(block, sent):
            others(y, lambda t: send(block, block, PH9A, {"tp": z * 8 + t, "dp": core_a}, sent))

        def along(block, sent, first=0):
            others(z, lambda t: send(block, block, PH9B, {"tp": t * 8 + y, "dp": core_b}, sent), first)

        def to_own_a(block):
            @pl.when(lax.rem(y, 2) == 0)
            def _():
                send(block, block, PH9A, at_x(0, 0), SENT_A)

        def to_own_b(block):
            @pl.when(lax.rem(z, 2) == 0)
            def _():
                send(block, block, PH9B, at_x(0, 0), SENT_B)

        def from_z(distances):
            wait_recv(r4.at[pl.ds(0, len(distances))], last(distances[0]))
            for k in distances:
                block = oa.at[y, lax.rem(z + 8 - k, 8) // 2]
                if distances[0] < 3:
                    across(block, RELAY_A)
                else:

                    @pl.when(z > 1)
                    def _(block=block):
                        across(block, RELAY_A)

                to_own_a(block)

        def from_y(distances):
            wait_recv(r4.at[pl.ds(0, len(distances))], last(distances[0]))
            for k in distances:
                block = ob.at[z, lax.rem(y + 8 - k, 8) // 2]
                along(block, RELAY_B, 2)
                to_own_b(block)

        def straight(t, block, sem, parity):
            for k in FARTHEST:
                send(block, block, sem, {"tp": t * 8 + lax.rem(y + k, 8), "dp": 2 * x + parity}, LOW + t)

        @pl.when(odd == 0)
        def _():
            block = oa.at[y, z // 2]
            oa[pl.ds(y, 1), pl.ds(z // 2, 1)] = own[None, None]
            def far_row(t):
                @pl.when(apart(z, t) > 2)
                def _():
                    straight(t, block, PH9A, lax.rem(y, 2))

            far_row(0)
            others(z, lambda t: send(block, block, LAST + apart(t, z) - 1, {"tp": t * 8 + y, "dp": one}, SENT_LAST))
            far_row(1)
            across(block, SENT_ON[PH9A])
            to_own_a(block)
            for distances in NEAREST:
                (from_z if distances[0] % 2 == 0 else from_y)(distances)

        @pl.when(odd == 1)
        def _():
            block = ob.at[z, y // 2]
            ob[pl.ds(z, 1), pl.ds(y // 2, 1)] = own[None, None]
            def other_row(t):
                @pl.when(z != t)
                def _():
                    straight(t, block, PH9B, lax.rem(z, 2))

            other_row(0)
            others(y, lambda t: send(block, block, LAST + apart(t, y) - 1, {"tp": z * 8 + t, "dp": one}, SENT_LAST))
            other_row(1)
            along(block, SENT_ON[PH9B])
            to_own_b(block)
            for distances in NEAREST:
                (from_y if distances[0] % 2 == 0 else from_z)(distances)

        def last_waits(buffer, sem, parity):
            @pl.when(parity == 0)
            def _():
                wait_recv(buffer.at[pl.ds(0, 4)], sem)

            @pl.when(parity == 1)
            def _():
                wait_recv(buffer.at[pl.ds(0, 3)], sem)

        last_waits(oa, PH9A, lax.rem(y, 2))
        last_waits(ob, PH9B, lax.rem(z, 2))
        with jax.named_scope("assemble"):
            assemble(1)

        with jax.named_scope("sent"):
            wait_sent(r4.at[pl.ds(0, 7)], SENT_ON[PH9A])
            for parity in range(2):
                for low in range(2):

                    @pl.when(jnp.logical_and(odd == parity, (z < 2) if low else (z > 1)))
                    def _(parity=parity, low=low):
                        wait_sent(oa.at[pl.ds(0, 5 + low), pl.ds(0, 4 - parity)], RELAY_B)
                        wait_sent(oa.at[pl.ds(0, 7), pl.ds(0, 2 if low else 3 + parity)], RELAY_A)

            for t in (0, 1):

                @pl.when(jnp.where(odd == 0, apart(z, t) > 2, z != t))
                def _(t=t):
                    wait_sent(r4.at[pl.ds(0, 7)], LOW + t)

            @pl.when(lax.rem(y, 2) == 0)
            def _():
                wait_sent(oa.at[0], SENT_A)

            @pl.when(lax.rem(z, 2) == 0)
            def _():
                wait_sent(ob.at[0], SENT_B)

        wait_sent(r4.at[pl.ds(0, 7)], SENT_LAST)

        @pl.when(keeps)
        def _():
            wait_sent(s7.at[pl.ds(0, 7)], SENT_ON[PH7])

        @pl.when(jnp.logical_not(keeps))
        def _():
            wait_sent(s7, SENT_ON[PH7])


def hand_over(mixed, state, mixed_h, state_h, sems):
    copies = [
        pltpu.make_async_copy(mixed, mixed_h, sems.at[0]),
        pltpu.make_async_copy(state, state_h, sems.at[1]),
    ]
    for copy in copies:
        copy.start()
    for copy in copies:
        copy.wait()


def body(tokens, lengths, norm_gain, w_in, log_step, eig_re, eig_im, in_mat, output_matrices, skip,
         w_glu, w_gate, state):
    args = (tokens, lengths.reshape(1, 32), norm_gain, w_in.swapaxes(1, 2), log_step, eig_re, eig_im,
            in_mat.swapaxes(3, 4), output_matrices, skip, w_glu, w_gate, state)
    mixed, new_state = pl.pallas_call(
        kernel,
        name="decode",
        out_shape=(pltpu.VMEM((256, 512), BF16), pltpu.VMEM((2, 2, 32, 128), F32)),
        in_specs=[pl.BlockSpec(memory_space=pl.ANY)] * 13,
        out_specs=(pl.BlockSpec(memory_space=pltpu.VMEM),) * 2,
        scratch_shapes=[pltpu.VMEM(a.shape, a.dtype) for a in args]
        + [
            pltpu.VMEM((4, 32, 128), BF16),
            pltpu.VMEM((8, 32, 128), BF16),
            pltpu.VMEM((2, 8, 32, 128), BF16),
            pltpu.VMEM((2, 4, 8, 2, 32, 128), BF16),
            pltpu.VMEM((8, 16, 128), BF16),
            pltpu.VMEM((2, 8, 16, 128), BF16),
            pltpu.VMEM((4, 2, 128, 128), BF16),
            pltpu.VMEM((8, 1, 128), F32),
            pltpu.VMEM((5, 32, 128), BF16),
            pltpu.VMEM((32, 128), BF16),
            pltpu.VMEM((2, 16, 128), BF16),
            pltpu.VMEM((2, 8, 16, 128), BF16),
            pltpu.VMEM((8, 64, 128), BF16),
            pltpu.VMEM((8, 64, 128), BF16),
            pltpu.VMEM((8, 32, 128), BF16),
            pltpu.VMEM((32, 128), BF16),
            pltpu.VMEM((8, 32, 128), BF16),
            pltpu.VMEM((8, 32, 128), BF16),
            pltpu.VMEM((8, 64, 128), BF16),
            pltpu.VMEM((8, 64, 128), BF16),
            pltpu.VMEM((8, 4, 32, 128), BF16),
            pltpu.VMEM((8, 4, 32, 128), BF16),
            pltpu.VMEM((2, 1, 32), F32),
            pltpu.VMEM((2, 2, 32, 128), F32),
            pltpu.VMEM((2, 2, 32, 128), F32),
            pltpu.VMEM((2, 2, 32, 128), F32),
            pltpu.SemaphoreType.DMA((11,)),
            pltpu.SemaphoreType.DMA((SENT,)),
            pltpu.SemaphoreType.DMA((RECV,)),
        ],
        compiler_params=pltpu.CompilerParams(collective_id=0, has_side_effects=True),
    )(*args)
    inside = [pltpu.with_memory_space_constraint(a, pltpu.VMEM) for a in (mixed, new_state)]
    return pl.pallas_call(
        hand_over,
        name="hand_over",
        out_shape=(jax.ShapeDtypeStruct((256, 512), BF16), jax.ShapeDtypeStruct((2, 2, 32, 128), F32)),
        in_specs=[pl.BlockSpec(memory_space=pltpu.VMEM)] * 2,
        out_specs=(pl.BlockSpec(memory_space=pl.ANY),) * 2,
        scratch_shapes=[pltpu.SemaphoreType.DMA((2,))],
    )(*inside)


def solution(mesh):
    placed = (
        P(None, "dp"),
        P("dp"),
        P(None, "dp"),
        P(None, "dp", "tp"),
        P(None, "tp"),
        P(None, "tp", None),
        P(None, "tp", None),
        P(None, None, "tp", None, None),
        P(None, None, "tp", None, None),
        P(None, "tp"),
        P(None, "tp", "dp"),
        P(None, "tp", "dp"),
        P(None, None, "dp", "tp"),
    )
    return jax.shard_map(
        body,
        mesh=mesh,
        in_specs=placed,
        out_specs=(P(None, "dp"), P(None, None, "dp", "tp")),
        check_vma=False,
    )
```

```python
import jax
import jax.numpy as jnp
from jax import lax
from jax.experimental import pallas as pl
from jax.experimental.pallas import tpu as pltpu
from jax.sharding import PartitionSpec as P

D = 4096
LEN_MAX = 4096
BLOCK_LEN = 256
NORM_EPS = 1e-06
MESH = pl.DeviceIdType.MESH
NT = (((1,), (1,)), ((), ()))
F32 = jnp.float32
BF16 = jnp.bfloat16

(PH1, RES0, PH2, ST1, STW, PH3, PH4, RES1, PH5, PH6, PH7, PH9A, PH9B, GAIN, STATE, COUNTS, NEW, NEAR, NEAR1, NEARW) = range(20)
FAR = 20
LAST = FAR + 5
RECV = LAST + 4
BULK, SMALL, READ = range(3)
SENT_ON = {NEAR: BULK, NEAR1: BULK, NEARW: BULK, NEW: BULK, STATE: READ, COUNTS: 3, PH3: SMALL, PH4: SMALL, PH5: SMALL,
           PH2: READ, PH6: READ, STW: 4, PH1: 5, GAIN: 6, RES0: 7, RES1: 8, PH7: 9, PH9A: 10, PH9B: 10}
SENT_LAST, SENT_A, SENT_B, RELAY_A, RELAY_B, LOW, SENT = 3, 11, 12, 13, 14, 15, 17
NEAREST = ((1, 7), (2, 6), (3, 5), (4,))
FARTHEST = (4, 3, 5, 2, 6, 1, 7)


def roll(x, amount):
    amount = amount % 128
    return x if amount == 0 else pltpu.roll(x, amount, 1)


def groups4(rows):
    return lax.broadcasted_iota(jnp.int32, (rows, 128), 1) // 32


def low_half(rows):
    return lax.broadcasted_iota(jnp.int32, (rows, 128), 1) < 64


def pick4(parts, group):
    out = parts[3]
    for i in (2, 1, 0):
        out = jnp.where(group == i, parts[i], out)
    return out


def split2(x):
    hi = x.astype(BF16)
    lo = (x - hi.astype(F32)).astype(BF16)
    return hi, lo


def kernel(
    tok_h, len_h, gain_h, win_h, ls_h, er_h, ei_h, im_h, om_h, skip_h, glu_h, gate_h, st_h,
    mixed_ref, ns_ref,
    tok, lens, gain, win, ls, er, ei, im, om, skip, glu, gate, st,
    s1, r1, ws, w, wis, pk, wi, gb, rz, rz1, s2, r2, s3, r3, r4, m0, s5, r5, s7, r7, oa, ob,
    counts, st2, nsend, nrecv,
    lsem, ss, rs,
):
    tp = lax.axis_index("tp")
    d = lax.axis_index("dp")
    z = tp // 8
    y = lax.rem(tp, 8)
    x = d // 2
    core = lax.rem(d, 2)
    one = 2 * x + 1

    def at_y(k, dp=None):
        return {"tp": z * 8 + lax.rem(y + k, 8), "dp": one if dp is None else dp}

    def at_z(k, dp=None):
        return {"tp": lax.rem(z + k, 8) * 8 + y, "dp": one if dp is None else dp}

    def far(k):
        return FAR + min(k, 8 - k)

    def last(k):
        return LAST + min(k, 8 - k) - 1

    def at_x(k, c=1):
        return {"tp": tp, "dp": 2 * lax.rem(x + k, 4) + c}

    def send(src, dst, sem, dev, sent=None):
        if sent is None:
            sent = SENT_LAST if sem >= LAST else SMALL if sem >= FAR or sem == ST1 else SENT_ON[sem]
        pltpu.make_async_remote_copy(
            src_ref=src,
            dst_ref=dst,
            send_sem=ss.at[sent],
            recv_sem=rs.at[sem],
            device_id=dev,
            device_id_type=MESH,
        ).start()

    def wait_recv(ref, sem):
        with jax.named_scope(f"recv{sem}"):
            pltpu.make_async_copy(ref, ref, rs.at[sem]).wait()

    def wait_sent(ref, sem):
        pltpu.make_async_copy(ref, ref, ss.at[sem]).wait()

    def fold_low(t):
        n = t.shape[0] // 2
        return jnp.where(low_half(n), t[0:n], roll(t[n : 2 * n], 64))

    def fold_high(t):
        n = t.shape[0] // 2
        return jnp.where(low_half(n), roll(t[0:n], 64), t[n : 2 * n])

    def unfold(a, b):
        low = low_half(a.shape[0])
        return jnp.concatenate([jnp.where(low, a, roll(b, 64)), jnp.where(low, roll(a, 64), b)], axis=0)

    hbm = (tok_h, win_h, gain_h, glu_h, gate_h, len_h, st_h, ls_h, er_h, ei_h, im_h, om_h, skip_h)
    vmem = (tok, win, gain, glu, gate, lens, st, ls, er, ei, im, om, skip)
    group = (0, 0, 1, 2, 2, 3, 4, 5, 6, 7, 8, 9, 10)
    loads = [pltpu.make_async_copy(a, b, lsem.at[i]) for i, a, b in zip(group, hbm, vmem)]

    def wait_loaded(i):
        ref = (w.at[0, pl.ds(0, 4), pl.ds(0, 5)], gain, w.at[0, 0], lens, st, ls, er, ei, im, om, skip)[i]
        pltpu.make_async_copy(ref, ref, lsem.at[i]).wait()

    for copy in loads[:3]:
        copy.start()

    barrier = pltpu.get_barrier_semaphore()

    def greet(dev):
        pl.semaphore_signal(barrier, inc=1, device_id=dev, device_id_type=MESH)

    @pl.when(core == 1)
    def _():
        for k in FARTHEST:
            greet(at_y(k))
            greet(at_y(k, 2 * x))
        for k in FARTHEST:
            greet(at_z(k))
        for k in (2, 3, 1):
            greet(at_x(k, 0))
            greet(at_x(k))
        greet(at_x(0, 0))

    @pl.when(core == 0)
    def _():
        greet(at_x(0))

    for copy in loads[3:]:
        copy.start()
    group8 = groups4(8)

    def rows4(t):
        return pick4([jnp.broadcast_to(t[8 * i : 8 * i + 8], (8, 128)) for i in range(4)], group8)

    with jax.named_scope("load0"):
        wait_loaded(0)
        wait_loaded(1)
    for xx in range(4):
        t = tok[64 * xx : 64 * xx + 64, :].astype(F32)
        scaled = (t * gain[0:1, :]).astype(BF16)
        part = lax.dot_general(scaled, win[0], NT, preferred_element_type=F32)
        sq = jnp.sum(t * t, axis=1, keepdims=True)
        packed = [
            jnp.concatenate([part[32 * h + 8 * i : 32 * h + 8 * i + 8, :] for i in range(4)], axis=1)
            for h in range(2)
        ]
        spread = [rows4(sq[32 * h : 32 * h + 32]) for h in range(2)]
        s1[xx] = jnp.concatenate(packed + spread, axis=0).astype(BF16)

    wait_loaded(2)
    low32 = low_half(32)

    def pack_projection(layer):
        for q in range(4):
            g = glu[layer, :, 128 * q : 128 * q + 128].astype(F32)
            t = gate[layer, :, 128 * q : 128 * q + 128].astype(F32)
            ws[layer, 2 * q] = jnp.where(low32, g, roll(t, 64)).astype(BF16)
            ws[layer, 2 * q + 1] = jnp.where(low32, roll(g, 64), t).astype(BF16)

    pack_projection(0)

    half = lax.rem(y, 2)
    column = pl.ds(pl.multiple_of((y // 2) * 128, 128), 128)

    def pack_residual():
        for xx in range(4):
            t = tok[64 * xx : 64 * xx + 64, column].astype(F32)
            rz[xx] = fold_low(jnp.where(half == 1, roll(t, 64), t)).astype(BF16)

    def pack_input_weights():
        for q in range(4):
            t = win[1, :, 128 * q : 128 * q + 128].astype(F32)
            wis[2 * q] = fold_low(t).astype(BF16)
            wis[2 * q + 1] = fold_high(t).astype(BF16)

    def pack_gain():
        t = gain[1:2, column]
        return jnp.where(half == 1, roll(t, 64), t)[None]

    def assemble(g):
        for m in range(4):
            rows = pl.ds(pl.multiple_of((lax.rem(2 * m + g + 8 - 2 * x, 8) // 2) * 64, 64), 64)
            for q in range(4):
                a, b = (oa[2 * q, m], ob[2 * m, q]) if g == 0 else (ob[2 * m + 1, q], oa[2 * q + 1, m])
                mixed_ref[rows, 128 * q : 128 * q + 128] = unfold(a.astype(F32), b.astype(F32)).astype(BF16)

    @pl.when(core == 0)
    def _():
        with jax.named_scope("entry"):
            pl.semaphore_wait(barrier, 11)
        for k in (2, 3, 1, 0):
            send(s1.at[lax.rem(x + k, 4)], r1.at[d], PH1, at_x(k))
        for k in (0, *FARTHEST):
            send(ws.at[0, lax.rem(y + k, 8)], w.at[0, x, y, 0], far(k), at_y(k))
        wait_loaded(3)
        counts[0] = (lens[...] // BLOCK_LEN).astype(F32)
        send(counts.at[0], counts.at[0], COUNTS, at_x(0))
        wait_loaded(4)
        send(st, st2, STATE, at_x(0))

        @pl.when(d == z)
        def _():
            pack_residual()
            for k in range(4):
                send(rz.at[lax.rem(x + k, 4)], rz.at[4], RES0, at_x(k))

        pack_input_weights()
        for k in (0, *FARTHEST):
            send(wis.at[lax.rem(y + k, 8)], pk.at[0, y], STW, at_y(k))
        gb[pl.ds(d, 1)] = pack_gain()
        for k in range(4):
            send(gb.at[d], gb.at[d], GAIN, at_x(k))
        pack_projection(1)
        for k in (0, *FARTHEST):
            send(ws.at[1, lax.rem(y + k, 8)], w.at[1, x, y, 0], ST1, at_y(k))
        for i in range(5, 11):
            wait_loaded(i)

        wait_sent(s1, SENT_ON[PH1])
        wait_sent(w.at[0, 0], SMALL)
        wait_sent(counts.at[0], SENT_ON[COUNTS])
        wait_sent(st, READ)

        @pl.when(d == z)
        def _():
            wait_sent(rz.at[pl.ds(0, 4)], SENT_ON[RES0])

        wait_sent(wis, SENT_ON[STW])
        wait_sent(gb.at[pl.ds(0, 4)], SENT_ON[GAIN])

        wait_recv(nrecv, NEW)
        ns_ref[...] = nrecv[...]
        wait_recv(oa.at[pl.ds(0, 4)], PH9A)
        wait_recv(ob.at[pl.ds(0, 4)], PH9B)
        assemble(0)

    @pl.when(core == 1)
    def _():
        r1[pl.ds(d, 1)] = s1[pl.ds(x, 1)]
        w[0, pl.ds(x, 1), pl.ds(y, 1), 1] = ws[0, pl.ds(y, 1)][None]

        @pl.when(d == z)
        def _():
            pack_residual()
            rz[4] = rz[pl.ds(x, 1)][0]

        with jax.named_scope("entry"):
            pl.semaphore_wait(barrier, 18)
        for k in (2, 3, 1):
            send(s1.at[lax.rem(x + k, 4)], r1.at[d], PH1, at_x(k))
        for k in FARTHEST:
            send(ws.at[0, lax.rem(y + k, 8)], w.at[0, x, y, 1], far(k), at_y(k))

        def pass_on(*distances):
            if distances == (0,):
                wait_recv(w.at[0, x, y, 0], FAR)
            else:
                wait_recv(w.at[0, 0, pl.ds(0, len(distances))], far(distances[0]))
            for k in distances:
                block = w.at[0, x, lax.rem(y + 8 - k, 8)]
                for r in (2, 3, 1):
                    send(block, block, NEAR, at_x(r))

        @pl.when(d == z)
        def _():
            for k in (2, 3, 1):
                send(rz.at[lax.rem(x + k, 4)], rz.at[4], RES0, at_x(k))

        wait_loaded(3)
        counts[1] = (lens[...] // BLOCK_LEN).astype(F32)
        for i in range(4, 11):
            wait_loaded(i)
        wait_recv(counts.at[0], COUNTS)
        wait_recv(st2, STATE)
        eye = lax.broadcasted_iota(jnp.int32, (32, 32), 0) == lax.broadcasted_iota(jnp.int32, (32, 32), 1)
        blocks = jnp.concatenate(
            [
                jnp.sum(jnp.where(eye, jnp.broadcast_to(counts[h], (32, 32)), 0.0), axis=1, keepdims=True)
                for h in range(2)
            ],
            axis=0,
        )
        factor = 2.0 / (1.0 + blocks * (4.0 * BLOCK_LEN / LEN_MAX))

        def by_group(slabs, sign):
            zero = jnp.zeros((16, 64), F32)
            cols = []
            for c in range(2):
                top = jnp.concatenate([slabs[2 * c], zero], axis=1)
                low = jnp.concatenate([zero, slabs[2 * c + 1]], axis=1)
                both = jnp.concatenate([top, low], axis=0)
                cols.append(both if c == 0 else sign * both)
            return jnp.concatenate([jnp.concatenate(cols, axis=1)] * 4, axis=0)

        def constants(layer):
            def row(ref):
                return jnp.concatenate([ref[layer, 0:1, :], ref[layer, 1:2, :]], axis=1)

            e_re, e_im = row(er), row(ei)
            rate = jnp.exp(ls[layer : layer + 1, :])
            rate = jnp.concatenate(
                [jnp.broadcast_to(rate[:, 0:1], (1, 64)), jnp.broadcast_to(rate[:, 1:2], (1, 64))], axis=1
            )
            step = rate * factor
            magnitude = jnp.exp(e_re * step)
            turned = e_im * step
            a_re = magnitude * jnp.cos(turned)
            a_im = magnitude * jnp.sin(turned)
            modulus = e_re * e_re + e_im * e_im
            b_re = ((a_re - 1.0) * e_re + a_im * e_im) / modulus
            b_im = (a_im * e_re - (a_re - 1.0) * e_im) / modulus
            u = jnp.concatenate([st2[layer, 0], st[layer, 0]], axis=0)
            v = jnp.concatenate([st2[layer, 1], st[layer, 1]], axis=0)
            k_re = a_re * u - a_im * v
            k_im = a_re * v + a_im * u
            hi, lo = split2(by_group([im[layer, c, g] for c in range(2) for g in range(2)], 1.0))
            in_cat = jnp.concatenate([hi, lo], axis=0)
            hi, lo = split2(by_group([om[layer, c, g] for c in range(2) for g in range(2)], -1.0).T)
            out_cat = jnp.concatenate([hi, lo, hi], axis=0)
            direct = jnp.concatenate([skip[layer : layer + 1, :]] * 4, axis=1)
            return k_re, k_im, b_re, b_im, in_cat, out_cat, direct

        def recurrence(layer, consts, total):
            k_re, k_im, b_re, b_im, in_cat, out_cat, direct = consts
            driven = (total[0:16] * lax.rsqrt(total[16:32] / D + NORM_EPS)).astype(BF16).astype(F32)
            spread = jnp.concatenate(
                [jnp.where(group8 == i, driven[8 * h : 8 * h + 8], 0.0) for h in range(2) for i in range(4)],
                axis=0,
            ).astype(BF16)
            drive = lax.dot_general(
                jnp.concatenate([spread, spread], axis=1), in_cat, (((1,), (0,)), ((), ())),
                preferred_element_type=F32,
            )
            d_re, d_im = drive[:, 0:128], drive[:, 128:256]
            n_re = k_re + b_re * d_re - b_im * d_im
            n_im = k_im + b_re * d_im + b_im * d_re
            for part, new in ((0, n_re), (1, n_im)):
                nsend[layer, part] = new[0:32]
                ns_ref[layer, part] = new[32:64]
            hi, lo = split2(jnp.concatenate([n_re, n_im], axis=1))
            full = lax.dot_general(
                jnp.concatenate([hi, hi, lo], axis=1), out_cat, (((1,), (0,)), ((), ())),
                preferred_element_type=F32,
            )
            value = jnp.concatenate([rows4(full[32 * h : 32 * h + 32]) for h in range(2)], axis=0)
            value = value + direct * driven
            inner = 0.7978845608028654 * (value + 0.044715 * (value * value * value))
            return (value * (0.5 * (1.0 + jnp.tanh(inner)))).astype(BF16)

        def gather_readout(layer, value, sem):
            s2[layer] = value
            r2[layer, pl.ds(y, 1)] = value[None]
            for k in FARTHEST:
                send(s2.at[layer], r2.at[layer, y], sem, at_y(k))

        def unpack_readout(layer):
            got = [r2[layer, j].astype(F32) for j in range(8)]
            tiles = []
            for h in range(2):
                for i in range(4):
                    cols = []
                    for q in range(2):
                        parts = [got[4 * q + j][8 * h : 8 * h + 8] for j in range(4)]
                        cols.append(pick4([roll(parts[j], 32 * (j - i)) for j in range(4)], group8))
                    tiles.append(jnp.concatenate(cols, axis=1))
            return jnp.concatenate(tiles, axis=0).astype(BF16)

        def project(layer, piece, xx, out):
            rhs = jnp.concatenate([w[layer, xx, :, h].reshape(256, 128) for h in range(2)], axis=1)
            both = jnp.dot(piece, rhs, preferred_element_type=F32).astype(BF16)
            out[2 * xx] = both[:, 0:128]
            out[2 * xx + 1] = both[:, 128:256]

        def near(sem, block):
            for r in (2, 3, 1):
                send(block, block, sem, at_x(r))

        pass_on(0)
        consts0 = constants(0)
        for distances in NEAREST[:2]:
            pass_on(*distances)
        wait_recv(r1.at[pl.ds(0, 7)], PH1)
        value = recurrence(0, consts0, jnp.sum(r1[...].astype(F32), axis=0))
        gather_readout(0, value, PH2)
        for distances in NEAREST[2:]:
            pass_on(*distances)

        pack_input_weights()
        pk[1, pl.ds(y, 1)] = wis[pl.ds(y, 1)]
        for k in FARTHEST:
            send(wis.at[lax.rem(y + k, 8)], pk.at[1, y], STW, at_y(k))
        gb[pl.ds(d, 1)] = pack_gain()
        for k in range(1, 4):
            send(gb.at[d], gb.at[d], GAIN, at_x(k))
        pack_projection(1)
        w[1, pl.ds(x, 1), pl.ds(y, 1), 1] = ws[1, pl.ds(y, 1)][None]
        for k in FARTHEST:
            send(ws.at[1, lax.rem(y + k, 8)], w.at[1, x, y, 1], ST1, at_y(k))

        wait_recv(r2.at[0, pl.ds(0, 7)], PH2)
        piece = unpack_readout(0)
        wait_recv(w.at[0, pl.ds(0, 3)], NEAR)
        for xx in range(4):
            project(0, piece, xx, s3)
        for k in FARTHEST:
            send(s3.at[lax.rem(z + k, 8)], r3.at[z], PH3, at_z(k))
        r3[pl.ds(z, 1)] = s3[pl.ds(z, 1)]

        wait_recv(w.at[0, pl.ds(0, 3), pl.ds(0, 5), 0, pl.ds(0, 16)], STW)
        for h in range(2):
            for j in range(4):
                rows = unfold(pk[h, j].astype(F32), pk[h, 4 + j].astype(F32)).astype(BF16)
                wi[pl.ds(x, 1), h, 32 * j : 32 * j + 32, :] = rows[None]
        near(NEARW, wi.at[x])
        wait_recv(w.at[0, pl.ds(0, 3), pl.ds(0, 5), 0], ST1)
        near(NEAR1, w.at[1, x])
        send(nsend.at[0], nrecv.at[0], NEW, at_x(0, 0))

        @pl.when(d != z)
        def _():
            wait_recv(rz.at[4], RES0)

        def gated(parts, residual):
            linear, gate_sum = fold_low(parts), fold_high(parts)
            return (residual + linear * (1.0 / (1.0 + jnp.exp(-gate_sum)))).astype(BF16)

        residual0 = rz[4].astype(F32)
        wait_recv(r3.at[pl.ds(0, 7)], PH3)
        own = gated(jnp.sum(r3[...].astype(F32), axis=0), residual0)
        m0[...] = own
        r4[pl.ds(z, 1)] = own[None]
        for k in FARTHEST:
            send(m0, r4.at[z], PH4, at_z(k))

        alone = jnp.logical_and(x == 0, z < 2)

        @pl.when(jnp.logical_not(alone))
        def _():
            send(m0, rz1, RES1, {"tp": lax.rem(2 * x + z, 8) * 8 + y, "dp": (z // 2) * 2 + 1})

        @pl.when(alone)
        def _():
            rz1[...] = own

        consts1 = constants(1)
        wait_recv(gb.at[pl.ds(0, 7)], GAIN)
        low1 = low_half(1)
        gains = [jnp.where(low1, gb[2 * q], roll(gb[2 * q + 1], 64)) for q in range(4)]
        wait_recv(wi.at[pl.ds(0, 3)], NEARW)
        win_t = jnp.concatenate(
            [unfold(wi[q, 0].astype(F32), wi[q, 1].astype(F32)).T.astype(BF16) for q in range(4)], axis=0
        )

        wait_recv(r4.at[pl.ds(0, 7)], PH4)
        tiles = []
        sq = jnp.zeros((64, 1), F32)
        for q in range(4):
            cur = unfold(r4[2 * q].astype(F32), r4[2 * q + 1].astype(F32))
            sq = sq + jnp.sum(cur * cur, axis=1, keepdims=True)
            tiles.append((cur * gains[q]).astype(BF16))
        part = jnp.dot(jnp.concatenate(tiles, axis=1), win_t, preferred_element_type=F32)
        squares = [rows4(sq[32 * h : 32 * h + 32]) for h in range(2)]
        for q in range(2):
            for j in range(4):
                packed = []
                for h in range(2):
                    rows = [part[32 * h + 8 * i : 32 * h + 8 * i + 8, 128 * q : 128 * q + 128] for i in range(4)]
                    packed.append(pick4([roll(rows[i], 32 * (i - j)) for i in range(4)], group8))
                s5[4 * q + j] = jnp.concatenate(packed + squares, axis=0).astype(BF16)
        for k in FARTHEST:
            send(s5.at[lax.rem(y + k, 8)], r5.at[y], PH5, at_y(k))
        r5[pl.ds(y, 1)] = s5[pl.ds(y, 1)]
        wait_recv(r5.at[pl.ds(0, 7)], PH5)
        value = recurrence(1, consts1, jnp.sum(r5[...].astype(F32), axis=0))
        gather_readout(1, value, PH6)
        send(nsend.at[1], nrecv.at[1], NEW, at_x(0, 0))
        wait_recv(w.at[1, pl.ds(0, 3)], NEAR1)

        @pl.when(jnp.logical_not(alone))
        def _():
            wait_recv(rz1, RES1)

        wait_recv(r2.at[1, pl.ds(0, 7)], PH6)
        piece = unpack_readout(1)
        for xx in range(4):
            project(1, piece, xx, s7)
        for k in (4, 5, 2, 3, 6, 7, 0, 1):
            to = lax.rem(2 * x + k, 8)
            zz = lax.rem(2 * x + to, 8)
            dev = {"tp": zz * 8 + y, "dp": (to // 2) * 2 + 1}
            if k > 1:
                send(s7.at[to], r7.at[z], PH7, dev)
            else:

                @pl.when(z != zz)
                def _(to=to, dev=dev):
                    send(s7.at[to], r7.at[z], PH7, dev)

                @pl.when(z == zz)
                def _(to=to):
                    r7[pl.ds(z, 1)] = s7[pl.ds(to, 1)]

        wait_sent(s1.at[pl.ds(0, 3)], SENT_ON[PH1])
        wait_sent(w, BULK)
        wait_sent(w.at[0, pl.ds(0, 3), pl.ds(0, 7)], SMALL)
        wait_sent(r4.at[pl.ds(0, 7)], READ)
        wait_sent(gb.at[pl.ds(0, 3)], SENT_ON[GAIN])
        wait_sent(wis.at[pl.ds(0, 7)], SENT_ON[STW])

        @pl.when(d == z)
        def _():
            wait_sent(rz.at[pl.ds(0, 3)], SENT_ON[RES0])

        @pl.when(jnp.logical_not(alone))
        def _():
            wait_sent(m0, SENT_ON[RES1])

        keeps = jnp.logical_or(z == lax.rem(4 * x, 8), z == lax.rem(4 * x + 1, 8))

        @pl.when(keeps)
        def _():
            wait_recv(r7.at[pl.ds(0, 7)], PH7)

        @pl.when(jnp.logical_not(keeps))
        def _():
            wait_recv(r7, PH7)

        own = gated(jnp.sum(r7[...].astype(F32), axis=0), rz1[...].astype(F32))

        odd = lax.rem(y + z, 2)
        core_a = 2 * x + lax.rem(y, 2)
        core_b = 2 * x + lax.rem(z, 2)

        ORDER = (0, 2, 1, 7, 3, 6, 5, 4)

        def others(mine, serve, first=0):
            for t in ORDER:
                if t >= first:

                    @pl.when(mine != t)
                    def _(t=t):
                        serve(t)

        def apart(a, b):
            k = lax.rem(a + 8 - b, 8)
            return jnp.minimum(k, 8 - k)

        def across(block, sent):
            others(y, lambda t: send(block, block, PH9A, {"tp": z * 8 + t, "dp": core_a}, sent))

        def along(block, sent, first=0):
            others(z, lambda t: send(block, block, PH9B, {"tp": t * 8 + y, "dp": core_b}, sent), first)

        def to_own_a(block):
            @pl.when(lax.rem(y, 2) == 0)
            def _():
                send(block, block, PH9A, at_x(0, 0), SENT_A)

        def to_own_b(block):
            @pl.when(lax.rem(z, 2) == 0)
            def _():
                send(block, block, PH9B, at_x(0, 0), SENT_B)

        def from_z(distances):
            wait_recv(r4.at[pl.ds(0, len(distances))], last(distances[0]))
            for k in distances:
                block = oa.at[y, lax.rem(z + 8 - k, 8) // 2]
                if distances[0] < 3:
                    across(block, RELAY_A)
                else:

                    @pl.when(z > 1)
                    def _(block=block):
                        across(block, RELAY_A)

                to_own_a(block)

        def from_y(distances):
            wait_recv(r4.at[pl.ds(0, len(distances))], last(distances[0]))
            for k in distances:
                block = ob.at[z, lax.rem(y + 8 - k, 8) // 2]
                along(block, RELAY_B, 2)
                to_own_b(block)

        def straight(t, block, sem, parity):
            for k in FARTHEST:
                send(block, block, sem, {"tp": t * 8 + lax.rem(y + k, 8), "dp": 2 * x + parity}, LOW + t)

        @pl.when(odd == 0)
        def _():
            block = oa.at[y, z // 2]
            oa[pl.ds(y, 1), pl.ds(z // 2, 1)] = own[None, None]
            def far_row(t):
                @pl.when(apart(z, t) > 2)
                def _():
                    straight(t, block, PH9A, lax.rem(y, 2))

            far_row(0)
            others(z, lambda t: send(block, block, LAST + apart(t, z) - 1, {"tp": t * 8 + y, "dp": one}, SENT_LAST))
            far_row(1)
            across(block, SENT_ON[PH9A])
            to_own_a(block)
            for distances in NEAREST:
                (from_z if distances[0] % 2 == 0 else from_y)(distances)

        @pl.when(odd == 1)
        def _():
            block = ob.at[z, y // 2]
            ob[pl.ds(z, 1), pl.ds(y // 2, 1)] = own[None, None]
            def other_row(t):
                @pl.when(z != t)
                def _():
                    straight(t, block, PH9B, lax.rem(z, 2))

            other_row(0)
            others(y, lambda t: send(block, block, LAST + apart(t, y) - 1, {"tp": z * 8 + t, "dp": one}, SENT_LAST))
            other_row(1)
            along(block, SENT_ON[PH9B])
            to_own_b(block)
            for distances in NEAREST:
                (from_y if distances[0] % 2 == 0 else from_z)(distances)

        def last_waits(buffer, sem, parity):
            @pl.when(parity == 0)
            def _():
                wait_recv(buffer.at[pl.ds(0, 4)], sem)

            @pl.when(parity == 1)
            def _():
                wait_recv(buffer.at[pl.ds(0, 3)], sem)

        last_waits(oa, PH9A, lax.rem(y, 2))
        last_waits(ob, PH9B, lax.rem(z, 2))
        with jax.named_scope("assemble"):
            assemble(1)

        with jax.named_scope("sent"):
            wait_sent(r4.at[pl.ds(0, 7)], SENT_ON[PH9A])
            for parity in range(2):
                for low in range(2):

                    @pl.when(jnp.logical_and(odd == parity, (z < 2) if low else (z > 1)))
                    def _(parity=parity, low=low):
                        wait_sent(oa.at[pl.ds(0, 5 + low), pl.ds(0, 4 - parity)], RELAY_B)
                        wait_sent(oa.at[pl.ds(0, 7), pl.ds(0, 2 if low else 3 + parity)], RELAY_A)

            for t in (0, 1):

                @pl.when(jnp.where(odd == 0, apart(z, t) > 2, z != t))
                def _(t=t):
                    wait_sent(r4.at[pl.ds(0, 7)], LOW + t)

            @pl.when(lax.rem(y, 2) == 0)
            def _():
                wait_sent(oa.at[0], SENT_A)

            @pl.when(lax.rem(z, 2) == 0)
            def _():
                wait_sent(ob.at[0], SENT_B)

        wait_sent(r4.at[pl.ds(0, 7)], SENT_LAST)

        @pl.when(keeps)
        def _():
            wait_sent(s7.at[pl.ds(0, 7)], SENT_ON[PH7])

        @pl.when(jnp.logical_not(keeps))
        def _():
            wait_sent(s7, SENT_ON[PH7])


def hand_over(mixed, state, mixed_h, state_h, sems):
    copies = [
        pltpu.make_async_copy(mixed, mixed_h, sems.at[0]),
        pltpu.make_async_copy(state, state_h, sems.at[1]),
    ]
    for copy in copies:
        copy.start()
    for copy in copies:
        copy.wait()


def body(tokens, lengths, norm_gain, w_in, log_step, eig_re, eig_im, in_mat, output_matrices, skip,
         w_glu, w_gate, state):
    args = (tokens, lengths.reshape(1, 32), norm_gain, w_in.swapaxes(1, 2), log_step, eig_re, eig_im,
            in_mat.swapaxes(3, 4), output_matrices, skip, w_glu, w_gate, state)
    mixed, new_state = pl.pallas_call(
        kernel,
        name="decode",
        out_shape=(pltpu.VMEM((256, 512), BF16), pltpu.VMEM((2, 2, 32, 128), F32)),
        in_specs=[pl.BlockSpec(memory_space=pl.ANY)] * 13,
        out_specs=(pl.BlockSpec(memory_space=pltpu.VMEM),) * 2,
        scratch_shapes=[pltpu.VMEM(a.shape, a.dtype) for a in args]
        + [
            pltpu.VMEM((4, 32, 128), BF16),
            pltpu.VMEM((8, 32, 128), BF16),
            pltpu.VMEM((2, 8, 32, 128), BF16),
            pltpu.VMEM((2, 4, 8, 2, 32, 128), BF16),
            pltpu.VMEM((8, 16, 128), BF16),
            pltpu.VMEM((2, 8, 16, 128), BF16),
            pltpu.VMEM((4, 2, 128, 128), BF16),
            pltpu.VMEM((8, 1, 128), F32),
            pltpu.VMEM((5, 32, 128), BF16),
            pltpu.VMEM((32, 128), BF16),
            pltpu.VMEM((2, 16, 128), BF16),
            pltpu.VMEM((2, 8, 16, 128), BF16),
            pltpu.VMEM((8, 64, 128), BF16),
            pltpu.VMEM((8, 64, 128), BF16),
            pltpu.VMEM((8, 32, 128), BF16),
            pltpu.VMEM((32, 128), BF16),
            pltpu.VMEM((8, 32, 128), BF16),
            pltpu.VMEM((8, 32, 128), BF16),
            pltpu.VMEM((8, 64, 128), BF16),
            pltpu.VMEM((8, 64, 128), BF16),
            pltpu.VMEM((8, 4, 32, 128), BF16),
            pltpu.VMEM((8, 4, 32, 128), BF16),
            pltpu.VMEM((2, 1, 32), F32),
            pltpu.VMEM((2, 2, 32, 128), F32),
            pltpu.VMEM((2, 2, 32, 128), F32),
            pltpu.VMEM((2, 2, 32, 128), F32),
            pltpu.SemaphoreType.DMA((11,)),
            pltpu.SemaphoreType.DMA((SENT,)),
            pltpu.SemaphoreType.DMA((RECV,)),
        ],
        compiler_params=pltpu.CompilerParams(collective_id=0, has_side_effects=True),
    )(*args)
    inside = [pltpu.with_memory_space_constraint(a, pltpu.VMEM) for a in (mixed, new_state)]
    return pl.pallas_call(
        hand_over,
        name="hand_over",
        out_shape=(jax.ShapeDtypeStruct((256, 512), BF16), jax.ShapeDtypeStruct((2, 2, 32, 128), F32)),
        in_specs=[pl.BlockSpec(memory_space=pltpu.VMEM)] * 2,
        out_specs=(pl.BlockSpec(memory_space=pl.ANY),) * 2,
        scratch_shapes=[pltpu.SemaphoreType.DMA((2,))],
    )(*inside)


def solution(mesh):
    placed = (
        P(None, "dp"),
        P("dp"),
        P(None, "dp"),
        P(None, "dp", "tp"),
        P(None, "tp"),
        P(None, "tp", None),
        P(None, "tp", None),
        P(None, None, "tp", None, None),
        P(None, None, "tp", None, None),
        P(None, "tp"),
        P(None, "tp", "dp"),
        P(None, "tp", "dp"),
        P(None, None, "dp", "tp"),
    )
    return jax.shard_map(
        body,
        mesh=mesh,
        in_specs=placed,
        out_specs=(P(None, "dp"), P(None, None, "dp", "tp")),
        check_vma=False,
    )
```
